128 devices in a mesh: st: 64 (over z, y, x), tp: 2 (over core).
Axes of the slice: x: 4, y: 4, z: 4, core: 2. Of those that a mesh axis runs over, the one named last changes fastest.
Arguments:
- tokens: bfloat16 [65536, 2048], P('st', 'tp'), may hold values from -6 to 6
- passage_ids: int32 [1024, 2], P('st'), may hold values from 0 to 1023, as said below
- passage_store: bfloat16 [1024, 64, 2048], P('st'), may hold values from -6 to 6
- norm_gain: bfloat16 [2048], replicated, may hold values from 0.099609375 to 1.8984375
- conv_value_weight: bfloat16 [2048, 1536], P(None, 'tp'), may hold values from -0.125 to 0.125
- conv_gate_weight: bfloat16 [2048, 1536], P(None, 'tp'), may hold values from -0.125 to 0.125
- conv_weight: bfloat16 [31, 1536], P(None, 'tp'), may hold values from -1 to 1
- ln_gain: bfloat16 [1536], P('tp'), may hold values from 0.099609375 to 1.8984375
- query_weight: bfloat16 [2048, 512], P(None, 'tp'), may hold values from -0.125 to 0.125
- query_gain: bfloat16 [512], P('tp'), may hold values from 0.5 to 10
- passage_gain: bfloat16 [2048], replicated, may hold values from 0.099609375 to 1.8984375
- key_weight: bfloat16 [2048, 512], P(None, 'tp'), may hold values from -0.125 to 0.125
- value_weight: bfloat16 [2048, 512], P(None, 'tp'), may hold values from -0.125 to 0.125
- key_gain: bfloat16 [512], P('tp'), may hold values from 0.5 to 10
- memory_gate: bfloat16 [512], P('tp'), may hold values from 0.29882812 to 1.5
- conv_out_weight: bfloat16 [1536, 2048], P('tp'), may hold values from -0.125 to 0.125
- memory_out_weight: bfloat16 [512, 2048], P('tp'), may hold values from -0.125 to 0.125
Outputs:
- layer_out: bfloat16 [65536, 2048], P(('st', 'tp'))
The draws below stay inside these ranges and needn't reach their ends.
Inputs may be any that keep to these rules, and one draw needn't show every extreme that they name: The owner of passage p is p // 16. Among the 32 entries of the rows of passage_ids that lie on one index of st (aligned runs of 16 rows, that is the blocks of one index of st), no owner is named more than 1 times, and in every such run some owner is named exactly 1 times.
All inputs are finite; a program needn't handle non-finite values.
Results may differ from the reference program's by a relative error of at most 0.008.
The reference program's roundings to bfloat16 on the way count: a program that leaves them out, or rounds other values in their place, can miss the bound.
Values may be sent and summed in bfloat16 or wider, within the bound.
No kernel may reach another device: no remote copies, remote signals or barrier semaphores. Data moves between devices by JAX's collectives and lax.ppermute only.
A program may use at most 192 MiB of HBM per device.

```python
import jax
import jax.numpy as jnp
from jax import lax

D = 2048
C_A = 1536
MEM_HEADS = 8
MEM_HD = 64
MEM_W = 512
KW = 31
TOK_DEV = 1024
SEQS_DEV = 2
SEQ_LEN = 512
BLOCK = 64
PASS = 2
PLEN = 64
PASS_DEV = 16
TOKENS = 65536
BLOCKS = 1024
PASSAGES = 1024
N_ST = 64
N_TP = 2


def draw_passage_ids(key, part):
    owner_count = PASSAGES // PASS_DEV
    blocks_each = BLOCKS // owner_count
    request_count = blocks_each * PASS
    most_each = max(1, 2 * request_count // owner_count)
    slot_count = owner_count * most_each
    popular_key, hot_key, device_key = jax.random.split(jax.random.fold_in(key, 3), 3)
    popular = jax.random.randint(popular_key, (owner_count,), 0, 256)
    popular = popular * popular
    hot_owner = jax.random.randint(hot_key, (), 0, owner_count)
    slot_range = jnp.arange(slot_count, dtype=jnp.int32)
    slot_owner = slot_range // most_each
    first_slot = slot_range % most_each == 0

    def one_device(device):
        score_key, local_key, other_key, order_key = jax.random.split(jax.random.fold_in(device_key, device), 4)
        before = (device + owner_count - 1) % owner_count
        across = (device + owner_count // 2) % owner_count
        forced = (slot_owner == hot_owner) | first_slot & ((slot_owner == before) | (slot_owner == across))
        scores = jax.random.randint(score_key, (slot_count,), 0, 1 << 16) + popular[slot_owner] + jnp.where(forced, 1 << 18, 0)
        _, chosen = lax.top_k(scores * slot_count + slot_range, request_count)
        local_index = jnp.minimum(jax.random.randint(local_key, (request_count,), 0, PASS_DEV), jax.random.randint(other_key, (request_count,), 0, PASS_DEV))
        order = jax.random.permutation(order_key, request_count)
        picked = chosen // most_each * PASS_DEV + local_index
        return picked[order].reshape(blocks_each, PASS)
    return jax.vmap(one_device)(jnp.arange(owner_count, dtype=jnp.int32)).reshape(BLOCKS, PASS).astype(jnp.int32)


def gain_law(key):
    return jax.random.uniform(key, (MEM_W,), jnp.float32, 0.5, 2.5)


def draw_query_gain(key, part):
    return gain_law(jax.random.fold_in(key, 11)).astype(jnp.bfloat16)


def draw_key_gain(key, part):
    return gain_law(jax.random.fold_in(key, 17)).astype(jnp.bfloat16)


def draw_conv_weight(key, part):
    base = jax.random.truncated_normal(jax.random.fold_in(key, 23), -3.0, 3.0, (KW, C_A), jnp.float32)
    channel_scale = jnp.where(jnp.arange(C_A) < C_A // 2, 2.0, 0.6) * KW ** (-0.5)
    return jnp.clip(base * channel_scale[None, :], -1.0, 1.0).astype(jnp.bfloat16)


def shard_levels(key, shape, shards, low, largest):
    gain, own = 1.0, jax.random.fold_in(key, 6)
    for dim, blocks in shards:
        draws = jnp.exp(jax.random.uniform(jax.random.fold_in(own, dim), (blocks,), jnp.float32, low / len(shards), largest / len(shards)))
        gain = gain * jnp.repeat(draws, shape[dim] // blocks).reshape([-1 if axis == dim else 1 for axis in range(len(shape))])
    return gain


def gaussian(key, shape, spread, reach, shards=(), kind=jnp.bfloat16):
    array = jax.random.normal(key, shape, jnp.float32) * spread
    if len(shards) > 0:
        array = shard_levels(key, shape, shards, -0.22, 0.18) * array
    return jnp.clip(array, min=-reach, max=reach).astype(kind)


def setup_inputs(seed: int = 0) -> dict:
    streams_of = jax.random.split(jax.random.key(seed), 18)
    tokens = gaussian(streams_of[0], (TOKENS, D), 1.0, 6.0, ((0, 64), (1, 2)))
    passage_ids = draw_passage_ids(jax.random.fold_in(streams_of[17], 71), 0)
    passage_store = gaussian(streams_of[2], (PASSAGES, PLEN, D), 1.0, 6.0, ((0, 64),))
    norm_gain = jnp.clip(1.0 + 0.18 * jax.random.normal(streams_of[3], (D,), jnp.float32), 0.099609375, 1.8984375).astype(jnp.bfloat16)
    conv_value_weight = gaussian(streams_of[4], (D, C_A), D ** -0.5, 0.125, ((1, 2),))
    conv_gate_weight = gaussian(streams_of[5], (D, C_A), D ** -0.5, 0.125, ((1, 2),))
    conv_weight = draw_conv_weight(jax.random.fold_in(streams_of[17], 71), 0)
    ln_gain = jnp.clip(1.0 + 0.18 * jax.random.normal(streams_of[7], (C_A,), jnp.float32), 0.099609375, 1.8984375).astype(jnp.bfloat16)
    query_weight = gaussian(streams_of[8], (D, MEM_W), D ** -0.5, 0.125, ((1, 2),))
    query_gain = draw_query_gain(jax.random.fold_in(streams_of[17], 71), 0)
    passage_gain = jnp.clip(1.0 + 0.18 * jax.random.normal(streams_of[10], (D,), jnp.float32), 0.099609375, 1.8984375).astype(jnp.bfloat16)
    key_weight = gaussian(streams_of[11], (D, MEM_W), D ** -0.5, 0.125, ((1, 2),))
    value_weight = gaussian(streams_of[12], (D, MEM_W), D ** -0.5, 0.125, ((1, 2),))
    key_gain = draw_key_gain(jax.random.fold_in(streams_of[17], 71), 0)
    memory_gate = jnp.clip(0.29882812 + 1.2011719 * jax.random.uniform(streams_of[14], (MEM_W,), jnp.float32) ** shard_levels(streams_of[14], (MEM_W,), ((0, 2),), -0.2, 0.2), 0.29882812, 1.5).astype(jnp.bfloat16)
    conv_out_weight = gaussian(streams_of[15], (C_A, D), (C_A + MEM_W) ** -0.5, 0.125, ((0, 2),))
    memory_out_weight = gaussian(streams_of[16], (MEM_W, D), (C_A + MEM_W) ** -0.5, 0.125, ((0, 2),))
    return {"tokens": tokens, "passage_ids": passage_ids, "passage_store": passage_store, "norm_gain": norm_gain, "conv_value_weight": conv_value_weight, "conv_gate_weight": conv_gate_weight, "conv_weight": conv_weight, "ln_gain": ln_gain, "query_weight": query_weight, "query_gain": query_gain, "passage_gain": passage_gain, "key_weight": key_weight, "value_weight": value_weight, "key_gain": key_gain, "memory_gate": memory_gate, "conv_out_weight": conv_out_weight, "memory_out_weight": memory_out_weight}


NORM_EPS = 1e-06
LAYER_EPS = 1e-05

def row_norm(matrix, gain_row):
    widened = matrix.astype(jnp.float32)
    factor = lax.rsqrt(lax.optimization_barrier(jnp.mean(widened * widened, axis=-1, keepdims=True)) + NORM_EPS)
    return (widened * factor * gain_row.astype(jnp.float32)).astype(jnp.bfloat16)

def head_norm(product, gain_row, head_count):
    row_count = product.shape[0]
    split_heads = product.reshape(row_count, head_count, -1)
    factor = lax.rsqrt(lax.optimization_barrier(jnp.mean(split_heads * split_heads, axis=-1, keepdims=True)) + NORM_EPS)
    head_gains = gain_row.astype(jnp.float32).reshape(head_count, -1)
    return (split_heads * factor * head_gains).reshape(row_count, -1).astype(jnp.bfloat16)

def reference(tokens, passage_ids, passage_store, norm_gain, conv_value_weight, conv_gate_weight, conv_weight, ln_gain, query_weight, query_gain, passage_gain, key_weight, value_weight, key_gain, memory_gate, conv_out_weight, memory_out_weight):
    block_count = TOK_DEV // BLOCK
    token_groups = tokens.reshape(N_ST, TOK_DEV, D)
    id_groups = passage_ids.reshape(N_ST, block_count * PASS)
    taps = conv_weight.astype(jnp.float32)
    conv_part = C_A // N_TP
    head_part = MEM_W // N_TP

    def one_group(inputs):
        token_block, id_block = inputs
        normed_tokens = row_norm(token_block, norm_gain)
        up_value = jnp.dot(normed_tokens, conv_value_weight, preferred_element_type=jnp.float32)
        up_gate = jnp.dot(normed_tokens, conv_gate_weight, preferred_element_type=jnp.float32)
        gated_rows = (up_value * jax.nn.sigmoid(up_gate)).astype(jnp.bfloat16)
        sequences = gated_rows.astype(jnp.float32).reshape(SEQS_DEV, SEQ_LEN, C_A)
        padded = jnp.pad(sequences, ((0, 0), (KW - 1, 0), (0, 0)))
        filtered = jnp.zeros((SEQS_DEV, SEQ_LEN, C_A), jnp.float32)
        for tap in range(KW):
            filtered = filtered + taps[tap][None, None, :] * padded[:, tap:tap + SEQ_LEN, :]
        filtered = filtered.reshape(TOK_DEV, C_A)
        channel_mean = lax.optimization_barrier(jnp.sum(filtered, axis=-1, keepdims=True)) / C_A
        channel_var = lax.optimization_barrier(jnp.sum(filtered * filtered, axis=-1, keepdims=True)) / C_A - channel_mean * channel_mean
        scaled = (filtered - channel_mean) * lax.rsqrt(channel_var + LAYER_EPS) * ln_gain.astype(jnp.float32)
        conv_out = jax.nn.silu(scaled).astype(jnp.bfloat16)
        queries = head_norm(jnp.dot(normed_tokens, query_weight, preferred_element_type=jnp.float32), query_gain, MEM_HEADS)
        query_block = queries.reshape(block_count, BLOCK, MEM_HEADS, MEM_HD)
        fetched = passage_store[id_block].reshape(-1, D)
        normed_rows = row_norm(fetched, passage_gain)
        key_rows = head_norm(jnp.dot(normed_rows, key_weight, preferred_element_type=jnp.float32), key_gain, MEM_HEADS)
        value_rows = jnp.dot(normed_rows, value_weight, preferred_element_type=jnp.float32).astype(jnp.bfloat16)
        key_rows = key_rows.reshape(block_count, PASS * PLEN, MEM_HEADS, MEM_HD)
        value_rows = value_rows.reshape(block_count, PASS * PLEN, MEM_HEADS, MEM_HD)
        scores = jnp.einsum('nbhd,nkhd->nhbk', query_block.astype(jnp.float32), key_rows.astype(jnp.float32)) * MEM_HD ** (-0.5)
        row_max = lax.optimization_barrier(jnp.max(scores, axis=-1, keepdims=True))
        expanded = jnp.exp(scores - row_max)
        weights = (expanded / lax.optimization_barrier(jnp.sum(expanded, axis=-1, keepdims=True))).astype(jnp.bfloat16)
        attended = jnp.einsum('nhbk,nkhd->nbhd', weights.astype(jnp.float32), value_rows.astype(jnp.float32)).reshape(TOK_DEV, MEM_W)
        memory = (attended * jnp.tanh(memory_gate.astype(jnp.float32))).astype(jnp.bfloat16)
        running_sum = jnp.zeros((TOK_DEV, D), jnp.float32)
        for group_index in range(N_TP):
            conv_lo = group_index * conv_part
            head_lo = group_index * head_part
            partial_value = jnp.dot(conv_out[:, conv_lo:conv_lo + conv_part], conv_out_weight[conv_lo:conv_lo + conv_part], preferred_element_type=jnp.float32)
            partial_value = partial_value + jnp.dot(memory[:, head_lo:head_lo + head_part], memory_out_weight[head_lo:head_lo + head_part], preferred_element_type=jnp.float32)
            rounded = lax.optimization_barrier(partial_value.astype(jnp.bfloat16))
            running_sum = running_sum + rounded.astype(jnp.float32)
        return running_sum.astype(jnp.bfloat16)
    return lax.map(one_group, (token_groups, id_groups)).reshape(-1, D)
```

```python
import jax
import jax.numpy as jnp
from jax import lax
from jax.experimental import pallas as pl
from jax.experimental.pallas import tpu as pltpu
from jax.sharding import PartitionSpec as P

D = 2048
HALF_D = 1024
C_A = 1536
C_DEV = 768
MEM_HD = 64
MEM_DEV = 256
KW = 31
SEQ_LEN = 512
BLOCK = 64
PLEN = 64
PASS_DEV = 16
TOK_DEV = 1024
NORM_EPS = 1e-06
LAYER_EPS = 1e-05

KV_TILE = 256
TOK_TILE = 256
OUT_TILE = 256
ATT_TILE = 128
LANES = 128
CONV_ROWS = 128
HISTORY = 32

F32 = jnp.float32
BF16 = jnp.bfloat16


def matmul(a, b):
    return lax.dot_general(a, b, (((1,), (0,)), ((), ())), preferred_element_type=F32)


def matmul_t(a, b):
    return lax.dot_general(a, b, (((1,), (1,)), ((), ())), preferred_element_type=F32)


def head_norm(product, gain):
    width = product.shape[1]
    rows = lax.broadcasted_iota(jnp.int32, (width, width), 0) // MEM_HD
    cols = lax.broadcasted_iota(jnp.int32, (width, width), 1) // MEM_HD
    same_head = jnp.where(rows == cols, 1.0, 0.0).astype(BF16)
    squares = product * product
    coarse = squares.astype(BF16)
    fine = (squares - coarse.astype(F32)).astype(BF16)
    total = matmul(coarse, same_head) + matmul(fine, same_head)
    return product * lax.rsqrt(total * (1.0 / MEM_HD) + NORM_EPS) * gain


def kv_kernel(rows_ref, gain_ref, wk_ref, wv_ref, kg_ref, out_ref):
    widened = rows_ref[...].astype(F32)
    factor = lax.rsqrt(jnp.sum(widened * widened, axis=1, keepdims=True) * (1.0 / D) + NORM_EPS)
    normed = (widened * factor * gain_ref[...]).astype(BF16)
    keys = head_norm(matmul(normed, wk_ref[...]), kg_ref[...])
    out_ref[:, :MEM_DEV] = keys.astype(BF16)
    out_ref[:, MEM_DEV:] = matmul(normed, wv_ref[...]).astype(BF16)


def resident(shape):
    zeros = (0,) * len(shape)
    return pl.BlockSpec(shape, lambda *_: zeros, pipeline_mode=pl.Buffered(1))


def project_store(rows, passage_gain, key_weight, value_weight, key_gain):
    n = rows.shape[0]
    return pl.pallas_call(
        kv_kernel,
        out_shape=jax.ShapeDtypeStruct((n, 2 * MEM_DEV), BF16),
        grid=(n // KV_TILE,),
        in_specs=[
            pl.BlockSpec((KV_TILE, D), lambda i: (i, 0)),
            resident((1, D)),
            resident((D, MEM_DEV)),
            resident((D, MEM_DEV)),
            resident((1, MEM_DEV)),
        ],
        out_specs=pl.BlockSpec((KV_TILE, 2 * MEM_DEV), lambda i: (i, 0)),
        cost_estimate=pl.CostEstimate(flops=2 * n * D * 2 * MEM_DEV, transcendentals=0, bytes_accessed=8 << 20),
        name="project_store",
    )(rows, passage_gain, key_weight, value_weight, key_gain)


def slots_kernel(asked_ref, kv_ref, out_ref, sem):
    count = out_ref.shape[0]
    copies = [pltpu.make_async_copy(kv_ref.at[asked_ref[s]], out_ref.at[s], sem.at[s]) for s in range(count)]
    for c in copies:
        c.start()
    for c in copies:
        c.wait()


def fill_slots(asked, kv):
    count = asked.shape[0]
    return pl.pallas_call(
        slots_kernel,
        out_shape=jax.ShapeDtypeStruct((count, PLEN, 2 * MEM_DEV), BF16),
        grid_spec=pltpu.PrefetchScalarGridSpec(
            num_scalar_prefetch=1,
            grid=(1,),
            in_specs=[pl.BlockSpec((PASS_DEV, PLEN, 2 * MEM_DEV), lambda i, s: (0, 0, 0))],
            out_specs=pl.BlockSpec(memory_space=pl.ANY),
            scratch_shapes=[pltpu.SemaphoreType.DMA((count,))],
        ),
        name="fill_slots",
    )(asked, kv)


def token_kernel(
    tp_ref, own_ref, peer_ref, gain_ref, wv_ref, wg_ref, wq_ref, cw_ref, qg_ref, filt_ref, stat_ref, q_ref, xs_ref
):
    tile = pl.program_id(0)
    me = tp_ref[0]
    own_at = pl.multiple_of(me * HALF_D, HALF_D)
    peer_at = pl.multiple_of((1 - me) * HALF_D, HALF_D)
    own = own_ref[...].astype(F32)
    peer = peer_ref[...].astype(F32)
    total = jnp.sum(own * own, axis=1, keepdims=True) + jnp.sum(peer * peer, axis=1, keepdims=True)
    factor = lax.rsqrt(total * (1.0 / D) + NORM_EPS)
    own_n = (own * factor * gain_ref[me]).astype(BF16)
    peer_n = (peer * factor * gain_ref[1 - me]).astype(BF16)

    def product(w_ref):
        return matmul(own_n, w_ref[pl.ds(own_at, HALF_D), :]) + matmul(peer_n, w_ref[pl.ds(peer_at, HALF_D), :])

    q_ref[...] = head_norm(product(wq_ref), qg_ref[...]).astype(BF16)
    gated = (product(wv_ref) * jax.nn.sigmoid(product(wg_ref))).astype(BF16)

    @pl.when(tile % (SEQ_LEN // TOK_TILE) == 0)
    def _():
        xs_ref[:HISTORY, :] = jnp.zeros((HISTORY, C_DEV), F32)

    xs_ref[HISTORY:, :] = gated.astype(F32)
    first = HISTORY - (KW - 1)
    for base in range(0, TOK_TILE, CONV_ROWS):
        sums = jnp.zeros((CONV_ROWS, LANES), F32)
        squares = jnp.zeros((CONV_ROWS, LANES), F32)
        for lane in range(0, C_DEV, LANES):
            lanes = slice(lane, lane + LANES)
            acc = None
            for r in range(8):
                steps = [s for s in range(first, first + KW) if s % 8 == r]
                reach = max(steps) - r + CONV_ROWS
                shifted = xs_ref[base + r : base + r + reach, lanes]
                for s in steps:
                    term = shifted[s - r : s - r + CONV_ROWS] * cw_ref[s - first : s - first + 1, lanes]
                    acc = term if acc is None else acc + term
            filt_ref[base : base + CONV_ROWS, lanes] = acc
            sums = sums + acc
            squares = squares + acc * acc
        stat_ref[base : base + CONV_ROWS, 0:1] = jnp.sum(sums, axis=1, keepdims=True)
        stat_ref[base : base + CONV_ROWS, 1:2] = jnp.sum(squares, axis=1, keepdims=True)
    xs_ref[:HISTORY, :] = xs_ref[TOK_TILE:, :]


def token_branch(me, own, peer, gain, wv, wg, wq, cw, qg):
    n = own.shape[0]
    tile = lambda width: pl.BlockSpec((TOK_TILE, width), lambda i, s: (i, 0))
    return pl.pallas_call(
        token_kernel,
        out_shape=(
            jax.ShapeDtypeStruct((n, C_DEV), F32),
            jax.ShapeDtypeStruct((n, 2), F32),
            jax.ShapeDtypeStruct((n, MEM_DEV), BF16),
        ),
        grid_spec=pltpu.PrefetchScalarGridSpec(
            num_scalar_prefetch=1,
            grid=(n // TOK_TILE,),
            in_specs=[
                tile(HALF_D),
                tile(HALF_D),
                resident((2, 1, HALF_D)),
                resident((D, C_DEV)),
                resident((D, C_DEV)),
                resident((D, MEM_DEV)),
                resident((KW, C_DEV)),
                resident((1, MEM_DEV)),
            ],
            out_specs=(tile(C_DEV), tile(2), tile(MEM_DEV)),
            scratch_shapes=[pltpu.VMEM((HISTORY + TOK_TILE, C_DEV), F32)],
        ),
        cost_estimate=pl.CostEstimate(flops=20 * n * D * 768, transcendentals=0, bytes_accessed=16 << 20),
        name="token_branch",
    )(me, own, peer, gain, wv, wg, wq, cw, qg)


def conv_out_kernel(filt_ref, own_ref, peer_ref, gain_ref, w_ref, out_ref):
    stats = (own_ref[...] + peer_ref[...]) * (1.0 / C_A)
    mean = stats[:, 0:1]
    var = stats[:, 1:2] - mean * mean
    scaled = (filt_ref[...] - mean) * lax.rsqrt(var + LAYER_EPS) * gain_ref[...]
    out_ref[...] = matmul((scaled * jax.nn.sigmoid(scaled)).astype(BF16), w_ref[...])


def conv_product(filtered, own_stats, peer_stats, gain, weight):
    n = filtered.shape[0]
    tile = lambda width: pl.BlockSpec((OUT_TILE, width), lambda i: (i, 0))
    return pl.pallas_call(
        conv_out_kernel,
        out_shape=jax.ShapeDtypeStruct((n, D), F32),
        grid=(n // OUT_TILE,),
        in_specs=[tile(C_DEV), tile(2), tile(2), resident((1, C_DEV)), resident((C_DEV, D))],
        out_specs=tile(D),
        cost_estimate=pl.CostEstimate(flops=4 * n * D * 768, transcendentals=0, bytes_accessed=16 << 20),
        name="conv_product",
    )(filtered, own_stats, peer_stats, gain, weight)


def attend_kernel(half_ref, owner_ref, recv_ref, q_ref, conv_ref, gate_ref, w_ref, out_ref, kv_ref, sem):
    step = pl.program_id(0)
    steps = pl.num_programs(0)
    blocks = ATT_TILE // BLOCK
    count = kv_ref.shape[0]
    first = half_ref[0] * count

    def copy(i):
        return pltpu.make_async_copy(recv_ref.at[owner_ref[first + i]], kv_ref.at[i], sem.at[i])

    @pl.when(step == 0)
    def _():
        for i in range(count):
            copy(i).start()

    for j in range(2 * blocks):
        copy(step * 2 * blocks + j).wait()

    heads = MEM_DEV // MEM_HD
    lane_head = lax.broadcasted_iota(jnp.int32, (BLOCK, MEM_DEV), 1) // MEM_HD
    rows = []
    for b in range(blocks):
        at = step * 2 * blocks + 2 * b
        kv = kv_ref[pl.ds(at, 2)].reshape(2 * PLEN, 2 * MEM_DEV)
        q = q_ref[b * BLOCK : (b + 1) * BLOCK, :]
        spread = jnp.concatenate([jnp.where(lane_head == h, q, jnp.zeros_like(q)) for h in range(heads)], axis=0)
        scores = matmul_t(spread, kv[:, :MEM_DEV])
        expanded = jnp.exp(scores - jnp.max(scores, axis=1, keepdims=True))
        weights = (expanded / jnp.sum(expanded, axis=1, keepdims=True)).astype(BF16)
        mixed = matmul(weights, kv[:, MEM_DEV:])
        attended = mixed[:BLOCK]
        for h in range(1, heads):
            attended = jnp.where(lane_head == h, mixed[h * BLOCK : (h + 1) * BLOCK], attended)
        rows.append((attended * gate_ref[...]).astype(BF16))
    memory = jnp.concatenate(rows, axis=0)
    out_ref[...] = (conv_ref[...] + matmul(memory, w_ref[...])).astype(BF16)


def attend(half, owners, received, queries, conv_part, gate, weight):
    n = queries.shape[0] // 2
    steps = n // ATT_TILE
    count = owners.shape[0] // 2
    return pl.pallas_call(
        attend_kernel,
        out_shape=jax.ShapeDtypeStruct((n, D), BF16),
        grid_spec=pltpu.PrefetchScalarGridSpec(
            num_scalar_prefetch=2,
            grid=(steps,),
            in_specs=[
                pl.BlockSpec(memory_space=pl.ANY),
                pl.BlockSpec((ATT_TILE, MEM_DEV), lambda i, h, o: (h[0] * steps + i, 0)),
                pl.BlockSpec((ATT_TILE, D), lambda i, h, o: (h[0] * steps + i, 0)),
                resident((1, MEM_DEV)),
                resident((MEM_DEV, D)),
            ],
            out_specs=pl.BlockSpec((ATT_TILE, D), lambda i, h, o: (i, 0)),
            scratch_shapes=[
                pltpu.VMEM((count, PLEN, 2 * MEM_DEV), BF16),
                pltpu.SemaphoreType.DMA((count,)),
            ],
        ),
        cost_estimate=pl.CostEstimate(flops=4 * n * D * 256, transcendentals=0, bytes_accessed=8 << 20),
        name="attend",
    )(half, owners, received, queries, conv_part, gate, weight)


def body(
    tokens,
    passage_ids,
    passage_store,
    norm_gain,
    conv_value_weight,
    conv_gate_weight,
    conv_weight,
    ln_gain,
    query_weight,
    query_gain,
    passage_gain,
    key_weight,
    value_weight,
    key_gain,
    memory_gate,
    conv_out_weight,
    memory_out_weight,
):
    owner_count = lax.axis_size("st")
    swap = [(0, 1), (1, 0)]
    me = lax.axis_index("tp").astype(jnp.int32).reshape(1)
    row = lambda v: v.astype(F32).reshape(1, -1)

    owner_ids = passage_ids // PASS_DEV
    local_ids = passage_ids % PASS_DEV
    everyone = jnp.arange(owner_count, dtype=jnp.int32)[:, None, None]
    wanted = jnp.sum(jnp.where(owner_ids[None] == everyone, local_ids[None], 0), axis=(1, 2))
    asked = lax.all_to_all(wanted.reshape(owner_count, 1), "st", 0, 0, tiled=True).reshape(-1)
    peer_tokens = lax.ppermute(tokens, "tp", swap)

    kv = project_store(
        passage_store.reshape(-1, D), row(passage_gain), key_weight, value_weight, row(key_gain)
    ).reshape(PASS_DEV, PLEN, 2 * MEM_DEV)
    sent = fill_slots(asked, kv)
    received = lax.all_to_all(sent, "st", 0, 0, tiled=True)

    filtered, own_stats, queries = token_branch(
        me,
        tokens,
        peer_tokens,
        norm_gain.astype(F32).reshape(2, 1, HALF_D),
        conv_value_weight,
        conv_gate_weight,
        query_weight,
        conv_weight.astype(F32),
        row(query_gain) * MEM_HD ** (-0.5),
    )
    peer_stats = lax.ppermute(own_stats, "tp", swap)
    conv_part = conv_product(filtered, own_stats, peer_stats, row(ln_gain), conv_out_weight)

    owners = owner_ids.reshape(-1)
    gate = jnp.tanh(row(memory_gate))
    theirs = attend(1 - me, owners, received, queries, conv_part, gate, memory_out_weight)
    from_peer = lax.ppermute(theirs, "tp", swap)
    mine = attend(me, owners, received, queries, conv_part, gate, memory_out_weight)
    return (mine.astype(F32) + from_peer.astype(F32)).astype(BF16)


def solution(mesh):
    return jax.shard_map(
        body,
        mesh=mesh,
        in_specs=(
            P("st", "tp"),
            P("st", None),
            P("st", None, None),
            P(),
            P(None, "tp"),
            P(None, "tp"),
            P(None, "tp"),
            P("tp"),
            P(None, "tp"),
            P("tp"),
            P(),
            P(None, "tp"),
            P(None, "tp"),
            P("tp"),
            P("tp"),
            P("tp", None),
            P("tp", None),
        ),
        out_specs=P(("st", "tp"), None),
        check_vma=False,
    )
```

```python
import jax
import jax.numpy as jnp
from jax import lax
from jax.experimental import pallas as pl
from jax.experimental.pallas import tpu as pltpu
from jax.sharding import PartitionSpec as P

D = 2048
HALF_D = 1024
C_A = 1536
C_DEV = 768
MEM_HD = 64
MEM_DEV = 256
KW = 31
SEQ_LEN = 512
BLOCK = 64
PLEN = 64
PASS_DEV = 16
TOK_DEV = 1024
NORM_EPS = 1e-06
LAYER_EPS = 1e-05

KV_TILE = 256
TOK_TILE = 256
OUT_TILE = 256
ATT_TILE = 128
ATT_GROUP = 4
LANES = 128
CONV_ROWS = 128
HISTORY = 32

F32 = jnp.float32
BF16 = jnp.bfloat16


def matmul(a, b):
    return lax.dot_general(a, b, (((1,), (0,)), ((), ())), preferred_element_type=F32)


def matmul_t(a, b):
    return lax.dot_general(a, b, (((1,), (1,)), ((), ())), preferred_element_type=F32)


def row_norm(rows, gain):
    widened = rows.astype(F32)
    factor = lax.rsqrt(jnp.sum(widened * widened, axis=1, keepdims=True) * (1.0 / D) + NORM_EPS)
    return (widened * factor * gain).astype(BF16)


def head_norm(product, gain):
    width = product.shape[1]
    rows = lax.broadcasted_iota(jnp.int32, (width, width), 0) // MEM_HD
    cols = lax.broadcasted_iota(jnp.int32, (width, width), 1) // MEM_HD
    same_head = jnp.where(rows == cols, 1.0, 0.0).astype(BF16)
    squares = product * product
    coarse = squares.astype(BF16)
    fine = (squares - coarse.astype(F32)).astype(BF16)
    total = matmul(coarse, same_head) + matmul(fine, same_head)
    return product * lax.rsqrt(total * (1.0 / MEM_HD) + NORM_EPS) * gain


def wide_row(ref):
    values = ref[...].astype(F32)
    return jnp.concatenate([values[i : i + 1, :] for i in range(values.shape[0])], axis=1)


def kv_kernel(rows_hbm, gain_ref, wk_hbm, wv_hbm, kg_ref, out_hbm, rows_ref, wk_ref, wv_ref, out_ref, even, odd, r_sem, w_sem, o_sem):
    chunks = rows_hbm.shape[0] // KV_TILE
    span = lambda c: pl.ds(c * KV_TILE, KV_TILE)
    row_copies = [pltpu.make_async_copy(rows_hbm.at[span(c)], rows_ref.at[span(c)], r_sem.at[c]) for c in range(chunks)]
    out_copies = [pltpu.make_async_copy(out_ref.at[span(c)], out_hbm.at[span(c)], o_sem.at[c]) for c in range(chunks)]
    wk_copy = pltpu.make_async_copy(wk_hbm, wk_ref, w_sem.at[0])
    wv_copy = pltpu.make_async_copy(wv_hbm, wv_ref, w_sem.at[1])
    row_copies[0].start()
    wk_copy.start()
    wv_copy.start()
    for c in range(1, chunks):
        row_copies[c].start()
    gain = wide_row(gain_ref)
    key_gain = wide_row(kg_ref)
    held = (even, odd)

    def normalise(c):
        held[c % 2][...] = row_norm(rows_ref[span(c), :], gain)

    def project(c):
        normed = held[c % 2][...]
        keys = head_norm(matmul(normed, wk_ref[...]), key_gain)
        out_ref[span(c), :MEM_DEV] = keys.astype(BF16)
        out_ref[span(c), MEM_DEV:] = matmul(normed, wv_ref[...]).astype(BF16)

    row_copies[0].wait()
    normalise(0)
    wk_copy.wait()
    wv_copy.wait()
    for c in range(chunks):
        if c + 1 < chunks:
            row_copies[c + 1].wait()
            normalise(c + 1)
        project(c)
        out_copies[c].start()
    for c in range(chunks):
        out_copies[c].wait()


def resident(shape):
    zeros = (0,) * len(shape)
    return pl.BlockSpec(shape, lambda *_: zeros, pipeline_mode=pl.Buffered(1))


HBM = pl.BlockSpec(memory_space=pl.ANY)


def project_store(rows, passage_gain, key_weight, value_weight, key_gain):
    n = rows.shape[0]
    return pl.pallas_call(
        kv_kernel,
        out_shape=jax.ShapeDtypeStruct((n, 2 * MEM_DEV), BF16),
        grid=(1,),
        in_specs=[HBM, resident((D // LANES, LANES)), HBM, HBM, resident((MEM_DEV // LANES, LANES))],
        out_specs=HBM,
        scratch_shapes=[
            pltpu.VMEM((n, D), BF16),
            pltpu.VMEM((D, MEM_DEV), BF16),
            pltpu.VMEM((D, MEM_DEV), BF16),
            pltpu.VMEM((n, 2 * MEM_DEV), BF16),
            pltpu.VMEM((KV_TILE, D), BF16),
            pltpu.VMEM((KV_TILE, D), BF16),
            pltpu.SemaphoreType.DMA((n // KV_TILE,)),
            pltpu.SemaphoreType.DMA((2,)),
            pltpu.SemaphoreType.DMA((n // KV_TILE,)),
        ],
        cost_estimate=pl.CostEstimate(flops=2 * n * D * 2 * MEM_DEV, transcendentals=0, bytes_accessed=8 << 20),
        name="project_store",
    )(rows, passage_gain, key_weight, value_weight, key_gain)


def slots_kernel(asked_ref, kv_ref, out_ref, sem):
    count = out_ref.shape[0]
    copies = [pltpu.make_async_copy(kv_ref.at[asked_ref[s, 0]], out_ref.at[s], sem.at[s]) for s in range(count)]
    for c in copies:
        c.start()
    for c in copies:
        c.wait()


def fill_slots(asked, kv):
    count = asked.shape[0]
    return pl.pallas_call(
        slots_kernel,
        out_shape=jax.ShapeDtypeStruct((count, PLEN, 2 * MEM_DEV), BF16),
        grid_spec=pltpu.PrefetchScalarGridSpec(
            num_scalar_prefetch=1,
            grid=(1,),
            in_specs=[pl.BlockSpec((PASS_DEV, PLEN, 2 * MEM_DEV), lambda i, s: (0, 0, 0))],
            out_specs=pl.BlockSpec(memory_space=pl.ANY),
            scratch_shapes=[pltpu.SemaphoreType.DMA((count,))],
        ),
        name="fill_slots",
    )(asked, kv)


def token_kernel(
    tp_ref, own_ref, peer_ref, gain_ref, wv_ref, wg_ref, wq_ref, cw_ref, qg_ref, filt_ref, stat_ref, q_ref, xs_ref, taps_ref
):
    tile = pl.program_id(0)
    me = tp_ref[0]
    own_at = pl.multiple_of(me * HALF_D, HALF_D)
    peer_at = pl.multiple_of((1 - me) * HALF_D, HALF_D)
    own = own_ref[...].astype(F32)
    peer = peer_ref[...].astype(F32)
    total = jnp.sum(own * own, axis=1, keepdims=True) + jnp.sum(peer * peer, axis=1, keepdims=True)
    factor = lax.rsqrt(total * (1.0 / D) + NORM_EPS)
    own_n = (own * factor * wide_row(gain_ref.at[me])).astype(BF16)
    peer_n = (peer * factor * wide_row(gain_ref.at[1 - me])).astype(BF16)

    def product(w_ref):
        return matmul(own_n, w_ref[pl.ds(own_at, HALF_D), :]) + matmul(peer_n, w_ref[pl.ds(peer_at, HALF_D), :])

    q_ref[...] = head_norm(product(wq_ref), wide_row(qg_ref) * MEM_HD ** (-0.5)).astype(BF16)
    gated = (product(wv_ref) * jax.nn.sigmoid(product(wg_ref))).astype(BF16)

    @pl.when(tile % (SEQ_LEN // TOK_TILE) == 0)
    def _():
        xs_ref[:HISTORY, :] = jnp.zeros((HISTORY, C_DEV), F32)

    taps_ref[...] = cw_ref[...].astype(F32)
    xs_ref[HISTORY:, :] = gated.astype(F32)
    first = HISTORY - (KW - 1)
    for base in range(0, TOK_TILE, CONV_ROWS):
        sums = jnp.zeros((CONV_ROWS, LANES), F32)
        squares = jnp.zeros((CONV_ROWS, LANES), F32)
        for lane in range(0, C_DEV, LANES):
            lanes = slice(lane, lane + LANES)
            acc = None
            for r in range(8):
                steps = [s for s in range(first, first + KW) if s % 8 == r]
                reach = max(steps) - r + CONV_ROWS
                shifted = xs_ref[base + r : base + r + reach, lanes]
                part = None
                for s in steps:
                    term = shifted[s - r : s - r + CONV_ROWS] * taps_ref[s - first : s - first + 1, lanes]
                    part = term if part is None else part + term
                acc = part if acc is None else acc + part
            filt_ref[base : base + CONV_ROWS, lanes] = acc
            sums = sums + acc
            squares = squares + acc * acc
        stat_ref[base : base + CONV_ROWS, 0:1] = jnp.sum(sums, axis=1, keepdims=True)
        stat_ref[base : base + CONV_ROWS, 1:2] = jnp.sum(squares, axis=1, keepdims=True)
    xs_ref[:HISTORY, :] = xs_ref[TOK_TILE:, :]


def token_branch(me, own, peer, gain, wv, wg, wq, cw, qg):
    n = own.shape[0]
    tile = lambda width: pl.BlockSpec((TOK_TILE, width), lambda i, s: (i, 0))
    return pl.pallas_call(
        token_kernel,
        out_shape=(
            jax.ShapeDtypeStruct((n, C_DEV), F32),
            jax.ShapeDtypeStruct((n, 2), F32),
            jax.ShapeDtypeStruct((n, MEM_DEV), BF16),
        ),
        grid_spec=pltpu.PrefetchScalarGridSpec(
            num_scalar_prefetch=1,
            grid=(n // TOK_TILE,),
            in_specs=[
                tile(HALF_D),
                tile(HALF_D),
                resident((2, HALF_D // LANES, LANES)),
                resident((D, C_DEV)),
                resident((D, C_DEV)),
                resident((D, MEM_DEV)),
                resident((KW, C_DEV)),
                resident((MEM_DEV // LANES, LANES)),
            ],
            out_specs=(tile(C_DEV), tile(2), tile(MEM_DEV)),
            scratch_shapes=[pltpu.VMEM((HISTORY + TOK_TILE, C_DEV), F32), pltpu.VMEM((KW, C_DEV), F32)],
        ),
        cost_estimate=pl.CostEstimate(flops=20 * n * D * 768, transcendentals=0, bytes_accessed=16 << 20),
        name="token_branch",
    )(me, own, peer, gain, wv, wg, wq, cw, qg)


def swish_kernel(filt_ref, own_ref, peer_ref, gain_ref, out_ref):
    stats = (own_ref[...] + peer_ref[...]) * (1.0 / C_A)
    mean = stats[:, 0:1]
    var = stats[:, 1:2] - mean * mean
    scaled = (filt_ref[...] - mean) * lax.rsqrt(var + LAYER_EPS) * wide_row(gain_ref)
    out_ref[...] = (scaled * jax.nn.sigmoid(scaled)).astype(BF16)


def channel_swish(half, filtered, own_stats, peer_stats, gain):
    n = filtered.shape[0] // 2
    steps = n // OUT_TILE
    tile = lambda width: pl.BlockSpec((OUT_TILE, width), lambda i, h: (h[0] * steps + i, 0))
    return pl.pallas_call(
        lambda half_ref, *refs: swish_kernel(*refs),
        out_shape=jax.ShapeDtypeStruct((n, C_DEV), BF16),
        grid_spec=pltpu.PrefetchScalarGridSpec(
            num_scalar_prefetch=1,
            grid=(steps,),
            in_specs=[tile(C_DEV), tile(2), tile(2), resident((C_DEV // LANES, LANES))],
            out_specs=pl.BlockSpec((OUT_TILE, C_DEV), lambda i, h: (i, 0)),
        ),
        cost_estimate=pl.CostEstimate(flops=n * D * 768, transcendentals=0, bytes_accessed=4 << 20),
        name="channel_swish",
    )(half, filtered, own_stats, peer_stats, gain)


def pair_kernel(own_ref, peer_ref, w_own_ref, w_peer_ref, out_ref):
    out_ref[...] = matmul(own_ref[...], w_own_ref[...]) + matmul(peer_ref[...], w_peer_ref[...])


def conv_product(own, peer, w_own, w_peer):
    n = own.shape[0]
    tile = lambda width: pl.BlockSpec((OUT_TILE, width), lambda i: (i, 0))
    return pl.pallas_call(
        pair_kernel,
        out_shape=jax.ShapeDtypeStruct((n, D), F32),
        grid=(n // OUT_TILE,),
        in_specs=[tile(C_DEV), tile(C_DEV), resident((C_DEV, D)), resident((C_DEV, D))],
        out_specs=tile(D),
        cost_estimate=pl.CostEstimate(flops=4 * n * D * C_DEV, transcendentals=0, bytes_accessed=12 << 20),
        name="conv_product",
    )(own, peer, w_own, w_peer)


def attend_blocks(blocks, kv_ref, q_ref, gate):
    heads = MEM_DEV // MEM_HD
    lane_head = lax.broadcasted_iota(jnp.int32, (BLOCK, MEM_DEV), 1) // MEM_HD
    scores = []
    for b in blocks:
        q = q_ref[b * BLOCK : (b + 1) * BLOCK, :]
        spread = jnp.concatenate([jnp.where(lane_head == h, q, jnp.zeros_like(q)) for h in range(heads)], axis=0)
        scores.append(matmul_t(spread, kv_ref[2 * b : 2 * b + 2, :, :MEM_DEV].reshape(2 * PLEN, MEM_DEV)))
    expanded = [jnp.exp(s - jnp.max(s, axis=1, keepdims=True)) for s in scores]
    weights = [(e * (1.0 / jnp.sum(e, axis=1, keepdims=True))).astype(BF16) for e in expanded]
    rows = []
    for w, b in zip(weights, blocks):
        mixed = matmul(w, kv_ref[2 * b : 2 * b + 2, :, MEM_DEV:].reshape(2 * PLEN, MEM_DEV))
        attended = mixed[:BLOCK]
        for h in range(1, heads):
            attended = jnp.where(lane_head == h, mixed[h * BLOCK : (h + 1) * BLOCK], attended)
        rows.append((attended * gate).astype(BF16))
    return jnp.concatenate(rows, axis=0)


def read_copies(half_ref, owner_ref, recv_hbm, q_hbm, kv_ref, q_ref, sem, q_sem):
    count = kv_ref.shape[0]
    n = q_ref.shape[0]
    first = half_ref[0] * count
    q_copy = pltpu.make_async_copy(q_hbm.at[pl.ds(pl.multiple_of(half_ref[0] * n, n), n), :], q_ref, q_sem)
    return q_copy, [
        pltpu.make_async_copy(recv_hbm.at[owner_ref[first + i]], kv_ref.at[i], sem.at[i]) for i in range(count)
    ]


def attend_kernel(half_ref, owner_ref, recv_hbm, q_hbm, gate_hbm, out_ref, kv_ref, q_ref, gate_ref, sem, q_sem, gate_sem):
    q_copy, copies = read_copies(half_ref, owner_ref, recv_hbm, q_hbm, kv_ref, q_ref, sem, q_sem)
    gate_copy = pltpu.make_async_copy(gate_hbm, gate_ref, gate_sem)
    q_copy.start()
    for c in copies:
        c.start()
    gate_copy.start()
    q_copy.wait()
    gate_copy.wait()
    gate = jnp.tanh(wide_row(gate_ref))
    for group in range(0, q_ref.shape[0] // BLOCK, ATT_GROUP):
        for c in copies[2 * group : 2 * (group + ATT_GROUP)]:
            c.wait()
        blocks = range(group, group + ATT_GROUP)
        out_ref[group * BLOCK : (group + ATT_GROUP) * BLOCK, :] = attend_blocks(blocks, kv_ref, q_ref, gate)


def attend(half, owners, received, queries, gate):
    n = queries.shape[0] // 2
    count = owners.shape[0] // 2
    return pl.pallas_call(
        attend_kernel,
        out_shape=jax.ShapeDtypeStruct((n, MEM_DEV), BF16),
        grid_spec=pltpu.PrefetchScalarGridSpec(
            num_scalar_prefetch=2,
            grid=(1,),
            in_specs=[HBM, HBM, HBM],
            out_specs=pl.BlockSpec((n, MEM_DEV), lambda i, h, o: (0, 0)),
            scratch_shapes=[
                pltpu.VMEM((count, PLEN, 2 * MEM_DEV), BF16),
                pltpu.VMEM((n, MEM_DEV), BF16),
                pltpu.VMEM((MEM_DEV // LANES, LANES), BF16),
                pltpu.SemaphoreType.DMA((count,)),
                pltpu.SemaphoreType.DMA(()),
                pltpu.SemaphoreType.DMA(()),
            ],
        ),
        cost_estimate=pl.CostEstimate(flops=n * D * 256, transcendentals=0, bytes_accessed=2 << 20),
        name="attend",
    )(half, owners, received, queries, gate)


def finish_kernel(
    half_ref, owner_ref, recv_hbm, q_hbm, gate_hbm, peer_hbm, w_own_hbm, w_peer_hbm, conv_hbm, out_hbm,
    kv_ref, q_ref, gate_ref, peer_ref, w_own_ref, w_peer_ref, conv_ref, out_ref, sem, q_sem, gate_sem, w_sem, conv_sem, out_sem,
):
    q_copy, copies = read_copies(half_ref, owner_ref, recv_hbm, q_hbm, kv_ref, q_ref, sem, q_sem)
    size = ATT_GROUP * BLOCK
    groups = q_ref.shape[0] // size
    span = lambda g: pl.ds(g * size, size)
    gate_copy = pltpu.make_async_copy(gate_hbm, gate_ref, gate_sem)
    late = [
        pltpu.make_async_copy(w_own_hbm, w_own_ref, w_sem.at[0]),
        pltpu.make_async_copy(w_peer_hbm, w_peer_ref, w_sem.at[1]),
        pltpu.make_async_copy(peer_hbm, peer_ref, w_sem.at[2]),
    ]
    conv_copies = [pltpu.make_async_copy(conv_hbm.at[span(g)], conv_ref.at[span(g)], conv_sem.at[g]) for g in range(groups)]
    out_copies = [pltpu.make_async_copy(out_ref.at[span(g)], out_hbm.at[span(g)], out_sem.at[g]) for g in range(groups)]
    for c in [q_copy, *copies, gate_copy, *late, *conv_copies]:
        c.start()
    q_copy.wait()
    gate_copy.wait()
    gate = jnp.tanh(wide_row(gate_ref))
    for g in range(groups):
        for c in copies[2 * g * ATT_GROUP : 2 * (g + 1) * ATT_GROUP]:
            c.wait()
        own = attend_blocks(range(g * ATT_GROUP, (g + 1) * ATT_GROUP), kv_ref, q_ref, gate)
        if g == 0:
            for c in late:
                c.wait()
        conv_copies[g].wait()
        memory = matmul(own, w_own_ref[...]) + matmul(peer_ref[span(g), :], w_peer_ref[...])
        out_ref[span(g), :] = (conv_ref[span(g), :] + memory).astype(BF16)
        out_copies[g].start()
    for c in out_copies:
        c.wait()


def finish(half, owners, received, queries, gate, peer, w_own, w_peer, conv_sum):
    n = conv_sum.shape[0]
    count = owners.shape[0] // 2
    groups = n // (ATT_GROUP * BLOCK)
    return pl.pallas_call(
        finish_kernel,
        out_shape=jax.ShapeDtypeStruct((n, D), BF16),
        grid_spec=pltpu.PrefetchScalarGridSpec(
            num_scalar_prefetch=2,
            grid=(1,),
            in_specs=[HBM] * 7,
            out_specs=HBM,
            scratch_shapes=[
                pltpu.VMEM((count, PLEN, 2 * MEM_DEV), BF16),
                pltpu.VMEM((n, MEM_DEV), BF16),
                pltpu.VMEM((MEM_DEV // LANES, LANES), BF16),
                pltpu.VMEM((n, MEM_DEV), BF16),
                pltpu.VMEM((MEM_DEV, D), BF16),
                pltpu.VMEM((MEM_DEV, D), BF16),
                pltpu.VMEM((n, D), F32),
                pltpu.VMEM((n, D), BF16),
                pltpu.SemaphoreType.DMA((count,)),
                pltpu.SemaphoreType.DMA(()),
                pltpu.SemaphoreType.DMA(()),
                pltpu.SemaphoreType.DMA((3,)),
                pltpu.SemaphoreType.DMA((groups,)),
                pltpu.SemaphoreType.DMA((groups,)),
            ],
        ),
        cost_estimate=pl.CostEstimate(flops=5 * n * D * MEM_DEV, transcendentals=0, bytes_accessed=8 << 20),
        name="finish",
    )(half, owners, received, queries, gate, peer, w_own, w_peer, conv_sum)


def body(
    tokens,
    passage_ids,
    passage_store,
    norm_gain,
    conv_value_weight,
    conv_gate_weight,
    conv_weight,
    ln_gain,
    query_weight,
    query_gain,
    passage_gain,
    key_weight,
    value_weight,
    key_gain,
    memory_gate,
    conv_out_weight,
    memory_out_weight,
):
    owner_count = lax.axis_size("st")
    swap = [(0, 1), (1, 0)]
    me = lax.axis_index("tp").astype(jnp.int32).reshape(1)

    owner_ids = passage_ids // PASS_DEV
    local_ids = passage_ids % PASS_DEV
    everyone = jnp.arange(owner_count, dtype=jnp.int32)[:, None, None]
    wanted = jnp.sum(jnp.where(owner_ids[None] == everyone, local_ids[None], 0), axis=(1, 2))
    wanted = jnp.broadcast_to(wanted[:, None], (owner_count, LANES))
    asked = lax.all_to_all(wanted, "st", 0, 0, tiled=True)
    peer_tokens = lax.ppermute(tokens, "tp", swap)
    peer_conv_weight = lax.ppermute(conv_out_weight, "tp", swap)
    peer_memory_weight = lax.ppermute(memory_out_weight, "tp", swap)

    kv = project_store(
        passage_store.reshape(-1, D),
        passage_gain.reshape(-1, LANES),
        key_weight,
        value_weight,
        key_gain.reshape(-1, LANES),
    ).reshape(PASS_DEV, PLEN, 2 * MEM_DEV)
    sent = fill_slots(asked, kv)
    received = lax.all_to_all(sent, "st", 0, 0, tiled=True)

    filtered, own_stats, queries = token_branch(
        me,
        tokens,
        peer_tokens,
        norm_gain.reshape(2, -1, LANES),
        conv_value_weight,
        conv_gate_weight,
        query_weight,
        conv_weight,
        query_gain.reshape(-1, LANES),
    )
    peer_stats = lax.ppermute(own_stats, "tp", swap)
    conv_theirs = channel_swish(1 - me, filtered, own_stats, peer_stats, ln_gain.reshape(-1, LANES))
    conv_peer = lax.ppermute(conv_theirs, "tp", swap)
    conv_mine = channel_swish(me, filtered, own_stats, peer_stats, ln_gain.reshape(-1, LANES))
    conv_sum = conv_product(conv_mine, conv_peer, conv_out_weight, peer_conv_weight)

    received, conv_sum = lax.optimization_barrier((received, conv_sum))
    owners = owner_ids.reshape(-1)
    gate = memory_gate.reshape(-1, LANES)
    memory_theirs = attend(1 - me, owners, received, queries, gate)
    memory_peer = lax.ppermute(memory_theirs, "tp", swap)
    return finish(
        me, owners, received, queries, gate, memory_peer, memory_out_weight, peer_memory_weight, conv_sum
    )


def solution(mesh):
    return jax.shard_map(
        body,
        mesh=mesh,
        in_specs=(
            P("st", "tp"),
            P("st", None),
            P("st", None, None),
            P(),
            P(None, "tp"),
            P(None, "tp"),
            P(None, "tp"),
            P("tp"),
            P(None, "tp"),
            P("tp"),
            P(),
            P(None, "tp"),
            P(None, "tp"),
            P("tp"),
            P("tp"),
            P("tp", None),
            P("tp", None),
        ),
        out_specs=P(("st", "tp"), None),
        check_vma=False,
    )
```

```python
import jax
import jax.numpy as jnp
from jax import lax
from jax.experimental import pallas as pl
from jax.experimental.pallas import tpu as pltpu
from jax.sharding import PartitionSpec as P

D = 2048
HALF_D = 1024
C_A = 1536
C_DEV = 768
MEM_HD = 64
MEM_DEV = 256
KW = 31
SEQ_LEN = 512
BLOCK = 64
PLEN = 64
PASS_DEV = 16
TOK_DEV = 1024
NORM_EPS = 1e-06
LAYER_EPS = 1e-05

KV_TILE = 256
TOK_TILE = 256
OUT_TILE = 256
ATT_TILE = 128
ATT_GROUP = 4
LANES = 128
CONV_ROWS = 128
NORM_ROWS = 16
HISTORY = 32

F32 = jnp.float32
BF16 = jnp.bfloat16


def matmul(a, b):
    return lax.dot_general(a, b, (((1,), (0,)), ((), ())), preferred_element_type=F32)


def matmul_t(a, b):
    return lax.dot_general(a, b, (((1,), (1,)), ((), ())), preferred_element_type=F32)


def row_norm(rows, gain):
    widened = rows.astype(F32)
    factor = lax.rsqrt(jnp.sum(widened * widened, axis=1, keepdims=True) * (1.0 / D) + NORM_EPS)
    return (widened * factor * gain).astype(BF16)


def head_norm(product, gain):
    width = product.shape[1]
    rows = lax.broadcasted_iota(jnp.int32, (width, width), 0) // MEM_HD
    cols = lax.broadcasted_iota(jnp.int32, (width, width), 1) // MEM_HD
    same_head = jnp.where(rows == cols, 1.0, 0.0).astype(BF16)
    squares = product * product
    coarse = squares.astype(BF16)
    fine = (squares - coarse.astype(F32)).astype(BF16)
    total = matmul(coarse, same_head) + matmul(fine, same_head)
    return product * lax.rsqrt(total * (1.0 / MEM_HD) + NORM_EPS) * gain


def wide_row(ref):
    values = ref[...].astype(F32)
    return jnp.concatenate([values[i : i + 1, :] for i in range(values.shape[0])], axis=1)


def kv_kernel(
    rows_hbm, gain_hbm, wk_hbm, wv_hbm, kg_hbm, out_ref,
    rows_ref, gain_ref, wk_ref, wv_ref, kg_ref, even, odd, r_sem, w_sem
):
    chunks = rows_hbm.shape[0] // KV_TILE
    span = lambda c: pl.ds(c * KV_TILE, KV_TILE)
    row_copies = [pltpu.make_async_copy(rows_hbm.at[span(c)], rows_ref.at[span(c)], r_sem.at[c]) for c in range(chunks)]
    wk_copy = pltpu.make_async_copy(wk_hbm, wk_ref, w_sem.at[0])
    wv_copy = pltpu.make_async_copy(wv_hbm, wv_ref, w_sem.at[1])
    gain_copy = pltpu.make_async_copy(gain_hbm, gain_ref, w_sem.at[2])
    kg_copy = pltpu.make_async_copy(kg_hbm, kg_ref, w_sem.at[3])
    for c in [gain_copy, kg_copy, row_copies[0], wk_copy, wv_copy, *row_copies[1:]]:
        c.start()
    gain_copy.wait()
    kg_copy.wait()
    gain = wide_row(gain_ref)
    key_gain = wide_row(kg_ref)
    held = (even, odd)

    def normalise(c):
        for r in range(0, KV_TILE, NORM_ROWS):
            rows = rows_ref[c * KV_TILE + r : c * KV_TILE + r + NORM_ROWS, :]
            held[c % 2][r : r + NORM_ROWS, :] = row_norm(rows, gain)

    row_copies[0].wait()
    normalise(0)
    wk_copy.wait()
    wv_copy.wait()
    for c in range(chunks):
        if c + 1 < chunks:
            row_copies[c + 1].wait()
            normalise(c + 1)
        keys = head_norm(matmul(held[c % 2][...], wk_ref[...]), key_gain)
        out_ref[span(c), :MEM_DEV] = keys.astype(BF16)
        out_ref[span(c), MEM_DEV:] = matmul(held[c % 2][...], wv_ref[...]).astype(BF16)


def resident(shape):
    zeros = (0,) * len(shape)
    return pl.BlockSpec(shape, lambda *_: zeros, pipeline_mode=pl.Buffered(1))


HBM = pl.BlockSpec(memory_space=pl.ANY)
ONCHIP = pl.BlockSpec(memory_space=pltpu.VMEM)


def onchip(*arrays):
    return tuple(pltpu.with_memory_space_constraint(a, pltpu.VMEM) for a in arrays)


def offchip(*arrays):
    return tuple(pltpu.with_memory_space_constraint(a, pltpu.HBM) for a in arrays)


def grant(mib):
    return pltpu.CompilerParams(vmem_limit_bytes=mib << 20)


def project_store(rows, passage_gain, key_weight, value_weight, key_gain):
    n = rows.shape[0]
    return pl.pallas_call(
        kv_kernel,
        out_shape=pltpu.VMEM((n, 2 * MEM_DEV), BF16),
        in_specs=[HBM] * 5,
        out_specs=ONCHIP,
        scratch_shapes=[
            pltpu.VMEM((n, D), BF16),
            pltpu.VMEM((D // LANES, LANES), BF16),
            pltpu.VMEM((D, MEM_DEV), BF16),
            pltpu.VMEM((D, MEM_DEV), BF16),
            pltpu.VMEM((MEM_DEV // LANES, LANES), BF16),
            pltpu.VMEM((KV_TILE, D), BF16),
            pltpu.VMEM((KV_TILE, D), BF16),
            pltpu.SemaphoreType.DMA((n // KV_TILE,)),
            pltpu.SemaphoreType.DMA((4,)),
        ],
        compiler_params=grant(24),
        cost_estimate=pl.CostEstimate(flops=2 * n * D * 2 * MEM_DEV, transcendentals=0, bytes_accessed=8 << 20),
        name="project_store",
    )(*offchip(rows, passage_gain, key_weight, value_weight, key_gain))


def slots_kernel(asked_ref, kv_ref, out_ref, table, table_sem, sem):
    count = out_ref.shape[0]
    fetch = pltpu.make_async_copy(asked_ref, table, table_sem)
    fetch.start()
    fetch.wait()
    copies = [pltpu.make_async_copy(kv_ref.at[table[s, 0]], out_ref.at[s], sem.at[s]) for s in range(count)]
    for c in copies:
        c.start()
    for c in copies:
        c.wait()


def fill_slots(asked, kv):
    count = asked.shape[0]
    return pl.pallas_call(
        slots_kernel,
        out_shape=pltpu.HBM((count, PLEN, 2 * MEM_DEV), BF16),
        in_specs=[ONCHIP, ONCHIP],
        out_specs=HBM,
        scratch_shapes=[
            pltpu.SMEM(asked.shape, jnp.int32),
            pltpu.SemaphoreType.DMA(()),
            pltpu.SemaphoreType.DMA((count,)),
        ],
        compiler_params=grant(2),
        name="fill_slots",
    )(*onchip(asked, kv))


def token_kernel(
    tp_ref, own_ref, peer_ref, gain_ref, wv_ref, wg_ref, wq_ref, cw_ref, qg_ref, filt_ref, stat_ref, q_ref, xs_ref, taps_ref,
    own_n, peer_n
):
    tile = pl.program_id(0)
    me = tp_ref[0]
    own_at = pl.multiple_of(me * HALF_D, HALF_D)
    peer_at = pl.multiple_of((1 - me) * HALF_D, HALF_D)
    own_gain = wide_row(gain_ref.at[me])
    peer_gain = wide_row(gain_ref.at[1 - me])
    for r in range(0, TOK_TILE, NORM_ROWS):
        rows = slice(r, r + NORM_ROWS)
        own = own_ref[rows, :].astype(F32)
        peer = peer_ref[rows, :].astype(F32)
        total = jnp.sum(own * own + peer * peer, axis=1, keepdims=True)
        factor = lax.rsqrt(total * (1.0 / D) + NORM_EPS)
        own_n[rows, :] = (own * factor * own_gain).astype(BF16)
        peer_n[rows, :] = (peer * factor * peer_gain).astype(BF16)

    def product(w_ref):
        own_part = matmul(own_n[...], w_ref[pl.ds(own_at, HALF_D), :])
        return own_part + matmul(peer_n[...], w_ref[pl.ds(peer_at, HALF_D), :])

    q_ref[...] = head_norm(product(wq_ref), wide_row(qg_ref) * MEM_HD ** (-0.5)).astype(BF16)
    gated = (product(wv_ref) * jax.nn.sigmoid(product(wg_ref))).astype(BF16)

    @pl.when(tile % (SEQ_LEN // TOK_TILE) == 0)
    def _():
        xs_ref[:HISTORY, :] = jnp.zeros((HISTORY, C_DEV), F32)

    taps_ref[...] = cw_ref[...].astype(F32)
    xs_ref[HISTORY:, :] = gated.astype(F32)
    first = HISTORY - (KW - 1)
    for base in range(0, TOK_TILE, CONV_ROWS):
        sums = jnp.zeros((CONV_ROWS, LANES), F32)
        squares = jnp.zeros((CONV_ROWS, LANES), F32)
        for lane in range(0, C_DEV, LANES):
            lanes = slice(lane, lane + LANES)
            acc = None
            for r in range(8):
                steps = [s for s in range(first, first + KW) if s % 8 == r]
                reach = max(steps) - r + CONV_ROWS
                shifted = xs_ref[base + r : base + r + reach, lanes]
                part = None
                for s in steps:
                    term = shifted[s - r : s - r + CONV_ROWS] * taps_ref[s - first : s - first + 1, lanes]
                    part = term if part is None else part + term
                acc = part if acc is None else acc + part
            filt_ref[base : base + CONV_ROWS, lanes] = acc
            sums = sums + acc
            squares = squares + acc * acc
        stat_ref[base : base + CONV_ROWS, 0:1] = jnp.sum(sums, axis=1, keepdims=True)
        stat_ref[base : base + CONV_ROWS, 1:2] = jnp.sum(squares, axis=1, keepdims=True)
    xs_ref[:HISTORY, :] = xs_ref[TOK_TILE:, :]


def token_branch(me, own, peer, gain, wv, wg, wq, cw, qg):
    n = own.shape[0]
    tile = lambda width: pl.BlockSpec((TOK_TILE, width), lambda i, s: (i, 0))
    return pl.pallas_call(
        token_kernel,
        out_shape=(
            jax.ShapeDtypeStruct((n, C_DEV), F32),
            jax.ShapeDtypeStruct((n, 2), F32),
            jax.ShapeDtypeStruct((n, MEM_DEV), BF16),
        ),
        grid_spec=pltpu.PrefetchScalarGridSpec(
            num_scalar_prefetch=1,
            grid=(n // TOK_TILE,),
            in_specs=[
                tile(HALF_D),
                tile(HALF_D),
                resident((2, HALF_D // LANES, LANES)),
                resident((D, C_DEV)),
                resident((D, C_DEV)),
                resident((D, MEM_DEV)),
                resident((KW, C_DEV)),
                resident((MEM_DEV // LANES, LANES)),
            ],
            out_specs=(tile(C_DEV), tile(2), tile(MEM_DEV)),
            scratch_shapes=[
                pltpu.VMEM((HISTORY + TOK_TILE, C_DEV), F32),
                pltpu.VMEM((KW, C_DEV), F32),
                pltpu.VMEM((TOK_TILE, HALF_D), BF16),
                pltpu.VMEM((TOK_TILE, HALF_D), BF16),
            ],
        ),
        cost_estimate=pl.CostEstimate(flops=20 * n * D * 768, transcendentals=0, bytes_accessed=16 << 20),
        name="token_branch",
    )(me, own, peer, gain, wv, wg, wq, cw, qg)


def swish_kernel(filt_ref, own_ref, peer_ref, gain_ref, out_ref):
    stats = (own_ref[...] + peer_ref[...]) * (1.0 / C_A)
    mean = stats[:, 0:1]
    var = stats[:, 1:2] - mean * mean
    scaled = (filt_ref[...] - mean) * lax.rsqrt(var + LAYER_EPS) * wide_row(gain_ref)
    out_ref[...] = (scaled * jax.nn.sigmoid(scaled)).astype(BF16)


def channel_swish(half, filtered, own_stats, peer_stats, gain):
    n = filtered.shape[0] // 2
    steps = n // OUT_TILE
    tile = lambda width: pl.BlockSpec((OUT_TILE, width), lambda i, h: (h[0] * steps + i, 0))
    return pl.pallas_call(
        lambda half_ref, *refs: swish_kernel(*refs),
        out_shape=jax.ShapeDtypeStruct((n, C_DEV), BF16),
        grid_spec=pltpu.PrefetchScalarGridSpec(
            num_scalar_prefetch=1,
            grid=(steps,),
            in_specs=[tile(C_DEV), tile(2), tile(2), resident((C_DEV // LANES, LANES))],
            out_specs=pl.BlockSpec((OUT_TILE, C_DEV), lambda i, h: (i, 0)),
        ),
        cost_estimate=pl.CostEstimate(flops=n * D * 768, transcendentals=0, bytes_accessed=4 << 20),
        name="channel_swish",
    )(half, filtered, own_stats, peer_stats, gain)


def pair_kernel(own_ref, peer_ref, w_own_ref, w_peer_ref, out_ref):
    out_ref[...] = matmul(own_ref[...], w_own_ref[...]) + matmul(peer_ref[...], w_peer_ref[...])


def conv_product(own, peer, w_own, w_peer):
    n = own.shape[0]
    tile = lambda width: pl.BlockSpec((OUT_TILE, width), lambda i: (i, 0))
    return pl.pallas_call(
        pair_kernel,
        out_shape=jax.ShapeDtypeStruct((n, D), F32),
        grid=(n // OUT_TILE,),
        in_specs=[tile(C_DEV), tile(C_DEV), resident((C_DEV, D)), resident((C_DEV, D))],
        out_specs=tile(D),
        cost_estimate=pl.CostEstimate(flops=4 * n * D * C_DEV, transcendentals=0, bytes_accessed=12 << 20),
        name="conv_product",
    )(own, peer, w_own, w_peer)


def attend_blocks(blocks, kv_ref, q_ref, gate):
    heads = MEM_DEV // MEM_HD
    lane_head = lax.broadcasted_iota(jnp.int32, (BLOCK, MEM_DEV), 1) // MEM_HD
    scores = []
    for b in blocks:
        q = q_ref[b * BLOCK : (b + 1) * BLOCK, :]
        spread = jnp.concatenate([jnp.where(lane_head == h, q, jnp.zeros_like(q)) for h in range(heads)], axis=0)
        scores.append(matmul_t(spread, kv_ref[2 * b : 2 * b + 2, :, :MEM_DEV].reshape(2 * PLEN, MEM_DEV)))
    expanded = [jnp.exp(s - jnp.max(s, axis=1, keepdims=True)) for s in scores]
    weights = [(e * (1.0 / jnp.sum(e, axis=1, keepdims=True))).astype(BF16) for e in expanded]
    rows = []
    for w, b in zip(weights, blocks):
        mixed = matmul(w, kv_ref[2 * b : 2 * b + 2, :, MEM_DEV:].reshape(2 * PLEN, MEM_DEV))
        attended = mixed[:BLOCK]
        for h in range(1, heads):
            attended = jnp.where(lane_head == h, mixed[h * BLOCK : (h + 1) * BLOCK], attended)
        rows.append((attended * gate).astype(BF16))
    return jnp.concatenate(rows, axis=0)


def read_copies(half_ref, owner_ref, recv_hbm, q_hbm, kv_ref, q_ref, sem, q_sem):
    count = kv_ref.shape[0]
    n = q_ref.shape[0]
    first = half_ref[0] * count
    q_copy = pltpu.make_async_copy(q_hbm.at[pl.ds(pl.multiple_of(half_ref[0] * n, n), n), :], q_ref, q_sem)
    return q_copy, [
        pltpu.make_async_copy(recv_hbm.at[owner_ref[first + i]], kv_ref.at[i], sem.at[i]) for i in range(count)
    ]


SCALARS = pl.BlockSpec(memory_space=pltpu.SMEM)


def read_scratch(count, n):
    return [
        pltpu.VMEM((count, PLEN, 2 * MEM_DEV), BF16),
        pltpu.VMEM((n, MEM_DEV), BF16),
        pltpu.SemaphoreType.DMA((count,)),
        pltpu.SemaphoreType.DMA(()),
    ]


def attend_kernel(half_ref, owner_ref, recv_hbm, q_hbm, gate_ref, out_ref, kv_ref, q_ref, sem, q_sem):
    q_copy, copies = read_copies(half_ref, owner_ref, recv_hbm, q_hbm, kv_ref, q_ref, sem, q_sem)
    for c in [q_copy, *copies]:
        c.start()
    gate = jnp.tanh(wide_row(gate_ref))
    size = ATT_GROUP * BLOCK
    q_copy.wait()
    for g in range(out_ref.shape[0] // size):
        for c in copies[2 * g * ATT_GROUP : 2 * (g + 1) * ATT_GROUP]:
            c.wait()
        blocks = range(g * ATT_GROUP, (g + 1) * ATT_GROUP)
        out_ref[pl.ds(g * size, size), :] = attend_blocks(blocks, kv_ref, q_ref, gate)


def attend(half, owners, received, queries, gate):
    n = queries.shape[0] // 2
    return pl.pallas_call(
        attend_kernel,
        out_shape=pltpu.VMEM((n, MEM_DEV), BF16),
        in_specs=[SCALARS, SCALARS, HBM, HBM, ONCHIP],
        out_specs=ONCHIP,
        scratch_shapes=read_scratch(owners.shape[0] // 2, n),
        compiler_params=grant(8),
        cost_estimate=pl.CostEstimate(flops=n * D * 256, transcendentals=0, bytes_accessed=2 << 20),
        name="attend",
    )(half, owners, *offchip(received, queries), *onchip(gate))


def finish_kernel(
    half_ref, owner_ref, recv_hbm, q_hbm, gate_ref, peer_ref, w_own_ref, w_peer_ref, conv_ref, out_hbm,
    kv_ref, q_ref, sem, q_sem, out_ref, out_sem
):
    q_copy, copies = read_copies(half_ref, owner_ref, recv_hbm, q_hbm, kv_ref, q_ref, sem, q_sem)
    for c in [q_copy, *copies]:
        c.start()
    gate = jnp.tanh(wide_row(gate_ref))
    size = ATT_GROUP * BLOCK
    groups = out_ref.shape[0] // size
    span = lambda g: pl.ds(g * size, size)
    out_copies = [pltpu.make_async_copy(out_ref.at[span(g)], out_hbm.at[span(g)], out_sem.at[g]) for g in range(groups)]
    q_copy.wait()
    for g in range(groups):
        for c in copies[2 * g * ATT_GROUP : 2 * (g + 1) * ATT_GROUP]:
            c.wait()
        own = attend_blocks(range(g * ATT_GROUP, (g + 1) * ATT_GROUP), kv_ref, q_ref, gate)
        memory = matmul(own, w_own_ref[...]) + matmul(peer_ref[span(g), :], w_peer_ref[...])
        out_ref[span(g), :] = (conv_ref[span(g), :] + memory).astype(BF16)
        out_copies[g].start()
    for c in out_copies:
        c.wait()


def finish(half, owners, received, queries, gate, peer, w_own, w_peer, conv_sum):
    n = conv_sum.shape[0]
    return pl.pallas_call(
        finish_kernel,
        out_shape=pltpu.HBM((n, D), BF16),
        in_specs=[SCALARS, SCALARS, HBM, HBM] + [ONCHIP] * 5,
        out_specs=HBM,
        scratch_shapes=read_scratch(owners.shape[0] // 2, n)
        + [pltpu.VMEM((n, D), BF16), pltpu.SemaphoreType.DMA((n // (ATT_GROUP * BLOCK),))],
        compiler_params=grant(16),
        cost_estimate=pl.CostEstimate(flops=5 * n * D * MEM_DEV, transcendentals=0, bytes_accessed=8 << 20),
        name="finish",
    )(half, owners, *offchip(received, queries), *onchip(gate, peer, w_own, w_peer, conv_sum))


def body(
    tokens,
    passage_ids,
    passage_store,
    norm_gain,
    conv_value_weight,
    conv_gate_weight,
    conv_weight,
    ln_gain,
    query_weight,
    query_gain,
    passage_gain,
    key_weight,
    value_weight,
    key_gain,
    memory_gate,
    conv_out_weight,
    memory_out_weight,
):
    owner_count = lax.axis_size("st")
    swap = [(0, 1), (1, 0)]
    me = lax.axis_index("tp").astype(jnp.int32).reshape(1)

    owner_ids = passage_ids // PASS_DEV
    local_ids = passage_ids % PASS_DEV
    everyone = jnp.arange(owner_count, dtype=jnp.int32)[:, None, None]
    wanted = jnp.sum(jnp.where(owner_ids[None] == everyone, local_ids[None], 0), axis=(1, 2))
    wanted = jnp.broadcast_to(wanted[:, None], (owner_count, LANES))
    asked = lax.all_to_all(wanted, "st", 0, 0, tiled=True)
    peer_tokens = lax.ppermute(tokens, "tp", swap)
    peer_conv_weight = lax.ppermute(conv_out_weight, "tp", swap)
    peer_memory_weight = lax.ppermute(memory_out_weight, "tp", swap)

    kv = project_store(
        passage_store.reshape(-1, D),
        passage_gain.reshape(-1, LANES),
        key_weight,
        value_weight,
        key_gain.reshape(-1, LANES),
    ).reshape(PASS_DEV, PLEN, 2 * MEM_DEV)
    sent = fill_slots(asked, kv)
    received = lax.all_to_all(sent, "st", 0, 0, tiled=True)

    filtered, own_stats, queries = token_branch(
        me,
        tokens,
        peer_tokens,
        norm_gain.reshape(2, -1, LANES),
        conv_value_weight,
        conv_gate_weight,
        query_weight,
        conv_weight,
        query_gain.reshape(-1, LANES),
    )
    peer_stats = lax.ppermute(own_stats, "tp", swap)
    conv_theirs = channel_swish(1 - me, filtered, own_stats, peer_stats, ln_gain.reshape(-1, LANES))
    conv_peer = lax.ppermute(conv_theirs, "tp", swap)
    conv_mine = channel_swish(me, filtered, own_stats, peer_stats, ln_gain.reshape(-1, LANES))
    conv_sum = conv_product(conv_mine, conv_peer, conv_out_weight, peer_conv_weight)

    received, conv_sum = lax.optimization_barrier((received, conv_sum))
    owners = owner_ids.reshape(-1)
    gate = memory_gate.reshape(-1, LANES)
    memory_theirs = attend(1 - me, owners, received, queries, gate)
    memory_peer = lax.ppermute(memory_theirs, "tp", swap)
    return finish(
        me, owners, received, queries, gate, memory_peer, memory_out_weight, peer_memory_weight, conv_sum
    )


def solution(mesh):
    return jax.shard_map(
        body,
        mesh=mesh,
        in_specs=(
            P("st", "tp"),
            P("st", None),
            P("st", None, None),
            P(),
            P(None, "tp"),
            P(None, "tp"),
            P(None, "tp"),
            P("tp"),
            P(None, "tp"),
            P("tp"),
            P(),
            P(None, "tp"),
            P(None, "tp"),
            P("tp"),
            P("tp"),
            P("tp", None),
            P("tp", None),
        ),
        out_specs=P(("st", "tp"), None),
        check_vma=False,
    )
```

```python
import jax
import jax.numpy as jnp
from jax import lax
from jax.experimental import pallas as pl
from jax.experimental.pallas import tpu as pltpu
from jax.sharding import PartitionSpec as P

D = 2048
HALF_D = 1024
C_A = 1536
C_DEV = 768
MEM_HD = 64
MEM_DEV = 256
KW = 31
SEQ_LEN = 512
BLOCK = 64
PLEN = 64
PASS_DEV = 16
OWNER_SHIFT = 4
NORM_EPS = 1e-06
LAYER_EPS = 1e-05

KV_TILE = 256
TOK_TILE = 256
OUT_TILE = 256
ATT_TILE = 256
ATT_GROUP = 4
LANES = 128
CONV_ROWS = 128
NORM_ROWS = 16
HISTORY = 32

F32 = jnp.float32
BF16 = jnp.bfloat16


def matmul(a, b):
    return lax.dot_general(a, b, (((1,), (0,)), ((), ())), preferred_element_type=F32)


def matmul_t(a, b):
    return lax.dot_general(a, b, (((1,), (1,)), ((), ())), preferred_element_type=F32)


def row_norm(rows, gain):
    widened = rows.astype(F32)
    factor = lax.rsqrt(jnp.sum(widened * widened, axis=1, keepdims=True) * (1.0 / D) + NORM_EPS)
    return (widened * factor * gain).astype(BF16)


def head_norm(product, gain):
    width = product.shape[1]
    rows = lax.broadcasted_iota(jnp.int32, (width, width), 0) // MEM_HD
    cols = lax.broadcasted_iota(jnp.int32, (width, width), 1) // MEM_HD
    same_head = jnp.where(rows == cols, 1.0, 0.0).astype(BF16)
    squares = product * product
    coarse = squares.astype(BF16)
    fine = (squares - coarse.astype(F32)).astype(BF16)
    total = matmul(coarse, same_head) + matmul(fine, same_head)
    return product * lax.rsqrt(total * (1.0 / MEM_HD) + NORM_EPS) * gain


def wide_row(ref):
    values = ref[...].astype(F32)
    return jnp.concatenate([values[i : i + 1, :] for i in range(values.shape[0])], axis=1)


def kv_kernel(
    rows_hbm, gain_hbm, wk_hbm, wv_hbm, kg_hbm, out_ref,
    rows_ref, gain_ref, wk_ref, wv_ref, kg_ref, even, odd, r_sem, w_sem
):
    chunks = rows_hbm.shape[0] // KV_TILE
    span = lambda c: pl.ds(c * KV_TILE, KV_TILE)
    row_copies = [pltpu.make_async_copy(rows_hbm.at[span(c)], rows_ref.at[span(c)], r_sem.at[c]) for c in range(chunks)]
    wk_copy = pltpu.make_async_copy(wk_hbm, wk_ref, w_sem.at[0])
    wv_copy = pltpu.make_async_copy(wv_hbm, wv_ref, w_sem.at[1])
    gain_copy = pltpu.make_async_copy(gain_hbm, gain_ref, w_sem.at[2])
    kg_copy = pltpu.make_async_copy(kg_hbm, kg_ref, w_sem.at[3])
    for c in [gain_copy, kg_copy, row_copies[0], wk_copy, wv_copy, *row_copies[1:]]:
        c.start()
    gain_copy.wait()
    kg_copy.wait()
    gain = wide_row(gain_ref)
    key_gain = wide_row(kg_ref)
    held = (even, odd)

    def normalise(c):
        for r in range(0, KV_TILE, NORM_ROWS):
            rows = rows_ref[c * KV_TILE + r : c * KV_TILE + r + NORM_ROWS, :]
            held[c % 2][r : r + NORM_ROWS, :] = row_norm(rows, gain)

    row_copies[0].wait()
    normalise(0)
    wk_copy.wait()
    wv_copy.wait()
    for c in range(chunks):
        if c + 1 < chunks:
            row_copies[c + 1].wait()
            normalise(c + 1)
        keys = head_norm(matmul(held[c % 2][...], wk_ref[...]), key_gain)
        out_ref[span(c), :MEM_DEV] = keys.astype(BF16)
        out_ref[span(c), MEM_DEV:] = matmul(held[c % 2][...], wv_ref[...]).astype(BF16)


def resident(shape):
    zeros = (0,) * len(shape)
    return pl.BlockSpec(shape, lambda *_: zeros, pipeline_mode=pl.Buffered(1))


HBM = pl.BlockSpec(memory_space=pl.ANY)
ONCHIP = pl.BlockSpec(memory_space=pltpu.VMEM)


def onchip(*arrays):
    return tuple(pltpu.with_memory_space_constraint(a, pltpu.VMEM) for a in arrays)


def offchip(*arrays):
    return tuple(pltpu.with_memory_space_constraint(a, pltpu.HBM) for a in arrays)


def grant(mib):
    return pltpu.CompilerParams(vmem_limit_bytes=mib << 20)


def project_store(rows, passage_gain, key_weight, value_weight, key_gain):
    n = rows.shape[0]
    return pl.pallas_call(
        kv_kernel,
        out_shape=pltpu.VMEM((n, 2 * MEM_DEV), BF16),
        in_specs=[HBM] * 5,
        out_specs=ONCHIP,
        scratch_shapes=[
            pltpu.VMEM((n, D), BF16),
            pltpu.VMEM((D // LANES, LANES), BF16),
            pltpu.VMEM((D, MEM_DEV), BF16),
            pltpu.VMEM((D, MEM_DEV), BF16),
            pltpu.VMEM((MEM_DEV // LANES, LANES), BF16),
            pltpu.VMEM((KV_TILE, D), BF16),
            pltpu.VMEM((KV_TILE, D), BF16),
            pltpu.SemaphoreType.DMA((n // KV_TILE,)),
            pltpu.SemaphoreType.DMA((4,)),
        ],
        compiler_params=grant(24),
        cost_estimate=pl.CostEstimate(flops=2 * n * D * 2 * MEM_DEV, transcendentals=0, bytes_accessed=8 << 20),
        name="project_store",
    )(*offchip(rows, passage_gain, key_weight, value_weight, key_gain))


def slots_kernel(asked_ref, kv_ref, out_ref, table, table_sem, sem):
    count = out_ref.shape[0]
    fetch = pltpu.make_async_copy(asked_ref, table, table_sem)
    fetch.start()
    fetch.wait()
    copies = [pltpu.make_async_copy(kv_ref.at[table[s, 0]], out_ref.at[s], sem.at[s]) for s in range(count)]
    for c in copies:
        c.start()
    for c in copies:
        c.wait()


def fill_slots(asked, kv):
    count = asked.shape[0]
    return pl.pallas_call(
        slots_kernel,
        out_shape=pltpu.HBM((count, PLEN, 2 * MEM_DEV), BF16),
        in_specs=[ONCHIP, ONCHIP],
        out_specs=HBM,
        scratch_shapes=[
            pltpu.SMEM(asked.shape, jnp.int32),
            pltpu.SemaphoreType.DMA(()),
            pltpu.SemaphoreType.DMA((count,)),
        ],
        compiler_params=grant(2),
        name="fill_slots",
    )(*onchip(asked, kv))


def token_kernel(
    tp_ref, own_ref, peer_ref, gain_ref, wv_ref, wg_ref, wq_ref, cw_ref, qg_ref, filt_ref, stat_ref, q_ref, xs_ref, taps_ref,
    own_n, peer_n
):
    tile = pl.program_id(0)
    me = tp_ref[0]
    own_at = pl.multiple_of(me * HALF_D, HALF_D)
    peer_at = pl.multiple_of((1 - me) * HALF_D, HALF_D)
    own_gain = wide_row(gain_ref.at[me])
    peer_gain = wide_row(gain_ref.at[1 - me])
    for r in range(0, TOK_TILE, NORM_ROWS):
        rows = slice(r, r + NORM_ROWS)
        own = own_ref[rows, :].astype(F32)
        peer = peer_ref[rows, :].astype(F32)
        total = jnp.sum(own * own + peer * peer, axis=1, keepdims=True)
        factor = lax.rsqrt(total * (1.0 / D) + NORM_EPS)
        own_n[rows, :] = (own * factor * own_gain).astype(BF16)
        peer_n[rows, :] = (peer * factor * peer_gain).astype(BF16)

    def product(w_ref):
        own_part = matmul(own_n[...], w_ref[pl.ds(own_at, HALF_D), :])
        return own_part + matmul(peer_n[...], w_ref[pl.ds(peer_at, HALF_D), :])

    q_ref[...] = head_norm(product(wq_ref), wide_row(qg_ref) * MEM_HD ** (-0.5)).astype(BF16)
    gated = (product(wv_ref) * jax.nn.sigmoid(product(wg_ref))).astype(BF16)

    @pl.when(tile % (SEQ_LEN // TOK_TILE) == 0)
    def _():
        xs_ref[:HISTORY, :] = jnp.zeros((HISTORY, C_DEV), F32)

    taps_ref[...] = cw_ref[...].astype(F32)
    xs_ref[HISTORY:, :] = gated.astype(F32)
    first = HISTORY - (KW - 1)
    for base in range(0, TOK_TILE, CONV_ROWS):
        sums = jnp.zeros((CONV_ROWS, LANES), F32)
        squares = jnp.zeros((CONV_ROWS, LANES), F32)
        for lane in range(0, C_DEV, LANES):
            lanes = slice(lane, lane + LANES)
            acc = None
            for r in range(8):
                steps = [s for s in range(first, first + KW) if s % 8 == r]
                reach = max(steps) - r + CONV_ROWS
                shifted = xs_ref[base + r : base + r + reach, lanes]
                part = None
                for s in steps:
                    term = shifted[s - r : s - r + CONV_ROWS] * taps_ref[s - first : s - first + 1, lanes]
                    part = term if part is None else part + term
                acc = part if acc is None else acc + part
            filt_ref[base : base + CONV_ROWS, lanes] = acc
            sums = sums + acc
            squares = squares + acc * acc
        stat_ref[base : base + CONV_ROWS, 0:1] = jnp.sum(sums, axis=1, keepdims=True)
        stat_ref[base : base + CONV_ROWS, 1:2] = jnp.sum(squares, axis=1, keepdims=True)
    xs_ref[:HISTORY, :] = xs_ref[TOK_TILE:, :]


def token_branch(me, own, peer, gain, wv, wg, wq, cw, qg):
    n = own.shape[0]
    tile = lambda width: pl.BlockSpec((TOK_TILE, width), lambda i, s: (i, 0))
    return pl.pallas_call(
        token_kernel,
        out_shape=(
            jax.ShapeDtypeStruct((n, C_DEV), F32),
            jax.ShapeDtypeStruct((n, 2), F32),
            jax.ShapeDtypeStruct((n, MEM_DEV), BF16),
        ),
        grid_spec=pltpu.PrefetchScalarGridSpec(
            num_scalar_prefetch=1,
            grid=(n // TOK_TILE,),
            in_specs=[
                tile(HALF_D),
                tile(HALF_D),
                resident((2, HALF_D // LANES, LANES)),
                resident((D, C_DEV)),
                resident((D, C_DEV)),
                resident((D, MEM_DEV)),
                resident((KW, C_DEV)),
                resident((MEM_DEV // LANES, LANES)),
            ],
            out_specs=(tile(C_DEV), tile(2), tile(MEM_DEV)),
            scratch_shapes=[
                pltpu.VMEM((HISTORY + TOK_TILE, C_DEV), F32),
                pltpu.VMEM((KW, C_DEV), F32),
                pltpu.VMEM((TOK_TILE, HALF_D), BF16),
                pltpu.VMEM((TOK_TILE, HALF_D), BF16),
            ],
        ),
        cost_estimate=pl.CostEstimate(flops=20 * n * D * 768, transcendentals=0, bytes_accessed=16 << 20),
        name="token_branch",
    )(me, own, peer, gain, wv, wg, wq, cw, qg)


def swish_kernel(filt_ref, own_ref, peer_ref, gain_ref, out_ref):
    stats = (own_ref[...] + peer_ref[...]) * (1.0 / C_A)
    mean = stats[:, 0:1]
    var = stats[:, 1:2] - mean * mean
    scaled = (filt_ref[...] - mean) * lax.rsqrt(var + LAYER_EPS) * wide_row(gain_ref)
    out_ref[...] = (scaled * jax.nn.sigmoid(scaled)).astype(BF16)


def channel_swish(half, filtered, own_stats, peer_stats, gain):
    n = filtered.shape[0] // 2
    steps = n // OUT_TILE
    tile = lambda width: pl.BlockSpec((OUT_TILE, width), lambda i, h: (h[0] * steps + i, 0))
    return pl.pallas_call(
        lambda half_ref, *refs: swish_kernel(*refs),
        out_shape=jax.ShapeDtypeStruct((n, C_DEV), BF16),
        grid_spec=pltpu.PrefetchScalarGridSpec(
            num_scalar_prefetch=1,
            grid=(steps,),
            in_specs=[tile(C_DEV), tile(2), tile(2), resident((C_DEV // LANES, LANES))],
            out_specs=pl.BlockSpec((OUT_TILE, C_DEV), lambda i, h: (i, 0)),
        ),
        cost_estimate=pl.CostEstimate(flops=n * D * 768, transcendentals=0, bytes_accessed=4 << 20),
        name="channel_swish",
    )(half, filtered, own_stats, peer_stats, gain)


def pair_kernel(own_ref, peer_ref, w_own_ref, w_peer_ref, out_ref):
    out_ref[...] = matmul(own_ref[...], w_own_ref[...]) + matmul(peer_ref[...], w_peer_ref[...])


def conv_product(own, peer, w_own, w_peer):
    n = own.shape[0]
    tile = lambda width: pl.BlockSpec((OUT_TILE, width), lambda i: (i, 0))
    return pl.pallas_call(
        pair_kernel,
        out_shape=jax.ShapeDtypeStruct((n, D), F32),
        grid=(n // OUT_TILE,),
        in_specs=[tile(C_DEV), tile(C_DEV), resident((C_DEV, D)), resident((C_DEV, D))],
        out_specs=tile(D),
        cost_estimate=pl.CostEstimate(flops=4 * n * D * C_DEV, transcendentals=0, bytes_accessed=12 << 20),
        name="conv_product",
    )(own, peer, w_own, w_peer)


def attend_blocks(blocks, kv_ref, q_ref, gate):
    heads = MEM_DEV // MEM_HD
    lane_head = lax.broadcasted_iota(jnp.int32, (BLOCK, MEM_DEV), 1) // MEM_HD
    scores = []
    for b in blocks:
        q = q_ref[b * BLOCK : (b + 1) * BLOCK, :]
        spread = jnp.concatenate([jnp.where(lane_head == h, q, jnp.zeros_like(q)) for h in range(heads)], axis=0)
        scores.append(matmul_t(spread, kv_ref[2 * b : 2 * b + 2, :, :MEM_DEV].reshape(2 * PLEN, MEM_DEV)))
    expanded = [jnp.exp(s - jnp.max(s, axis=1, keepdims=True)) for s in scores]
    weights = [(e * (1.0 / jnp.sum(e, axis=1, keepdims=True))).astype(BF16) for e in expanded]
    rows = []
    for w, b in zip(weights, blocks):
        mixed = matmul(w, kv_ref[2 * b : 2 * b + 2, :, MEM_DEV:].reshape(2 * PLEN, MEM_DEV))
        attended = mixed[:BLOCK]
        for h in range(1, heads):
            attended = jnp.where(lane_head == h, mixed[h * BLOCK : (h + 1) * BLOCK], attended)
        rows.append((attended * gate).astype(BF16))
    return jnp.concatenate(rows, axis=0)


SCALARS = pl.BlockSpec(memory_space=pltpu.SMEM)


def read_scratch(count, n):
    return [
        pltpu.VMEM((count, PLEN, 2 * MEM_DEV), BF16),
        pltpu.VMEM((n, MEM_DEV), BF16),
        pltpu.SemaphoreType.DMA((count,)),
        pltpu.SemaphoreType.DMA(()),
    ]


def attend_all(out_ref, kv_ref, q_ref, gate, arrived):
    size = ATT_GROUP * BLOCK
    for g in range(out_ref.shape[0] // size):
        arrived(g)
        blocks = range(g * ATT_GROUP, (g + 1) * ATT_GROUP)
        out_ref[pl.ds(g * size, size), :] = attend_blocks(blocks, kv_ref, q_ref, gate)


def attend_kernel(
    half_ref, owner_ref, recv_hbm, q_hbm, gate_ref, out_ref, next_kv_ref, next_q_ref, kv_ref, q_ref, sem, q_sem, next_sem, next_q_sem
):
    count = kv_ref.shape[0]
    n = q_ref.shape[0]
    first, second = half_ref[0], 1 - half_ref[0]
    q_copy = pltpu.make_async_copy(q_hbm.at[pl.ds(pl.multiple_of(first * n, n), n), :], q_ref, q_sem)
    copies = [
        pltpu.make_async_copy(recv_hbm.at[owner_ref[first * count + i]], kv_ref.at[i], sem.at[i]) for i in range(count)
    ]
    later = [pltpu.make_async_copy(q_hbm.at[pl.ds(pl.multiple_of(second * n, n), n), :], next_q_ref, next_q_sem)] + [
        pltpu.make_async_copy(recv_hbm.at[owner_ref[second * count + i]], next_kv_ref.at[i], next_sem.at[i])
        for i in range(count)
    ]
    for c in [q_copy, *copies, *later]:
        c.start()
    gate = jnp.tanh(wide_row(gate_ref))
    q_copy.wait()

    def arrived(g):
        for c in copies[2 * g * ATT_GROUP : 2 * (g + 1) * ATT_GROUP]:
            c.wait()

    attend_all(out_ref, kv_ref, q_ref, gate, arrived)
    for c in later:
        c.wait()


def attend_first(half, owners, received, queries, gate):
    n = queries.shape[0] // 2
    count = owners.shape[0] // 2
    return pl.pallas_call(
        attend_kernel,
        out_shape=(
            pltpu.VMEM((n, MEM_DEV), BF16),
            pltpu.VMEM((count, PLEN, 2 * MEM_DEV), BF16),
            pltpu.VMEM((n, MEM_DEV), BF16),
        ),
        in_specs=[SCALARS, SCALARS, HBM, HBM, ONCHIP],
        out_specs=(ONCHIP, ONCHIP, ONCHIP),
        scratch_shapes=read_scratch(count, n) + [pltpu.SemaphoreType.DMA((count,)), pltpu.SemaphoreType.DMA(())],
        compiler_params=grant(8),
        cost_estimate=pl.CostEstimate(flops=n * D * 256, transcendentals=0, bytes_accessed=2 << 20),
        name="attend_first",
    )(half, owners, *offchip(received, queries), *onchip(gate))


def attend_rest_kernel(kv_ref, q_ref, gate_ref, out_ref):
    attend_all(out_ref, kv_ref, q_ref, jnp.tanh(wide_row(gate_ref)), lambda g: None)


def attend_rest(kv, queries, gate):
    n = queries.shape[0]
    return pl.pallas_call(
        attend_rest_kernel,
        out_shape=pltpu.VMEM((n, MEM_DEV), BF16),
        in_specs=[ONCHIP] * 3,
        out_specs=ONCHIP,
        compiler_params=grant(6),
        cost_estimate=pl.CostEstimate(flops=n * D * 256, transcendentals=0, bytes_accessed=2 << 20),
        name="attend_rest",
    )(*onchip(kv, queries, gate))


def finish_kernel(own_ref, peer_ref, w_own_ref, w_peer_ref, conv_ref, out_hbm, out_ref, out_sem):
    groups = out_ref.shape[0] // ATT_TILE
    span = lambda g: pl.ds(g * ATT_TILE, ATT_TILE)
    out_copies = [pltpu.make_async_copy(out_ref.at[span(g)], out_hbm.at[span(g)], out_sem.at[g]) for g in range(groups)]
    for g in range(groups):
        memory = matmul(own_ref[span(g), :], w_own_ref[...]) + matmul(peer_ref[span(g), :], w_peer_ref[...])
        out_ref[span(g), :] = (conv_ref[span(g), :] + memory).astype(BF16)
        out_copies[g].start()
    for c in out_copies:
        c.wait()


def finish(own, peer, w_own, w_peer, conv_sum):
    n = conv_sum.shape[0]
    return pl.pallas_call(
        finish_kernel,
        out_shape=pltpu.HBM((n, D), BF16),
        in_specs=[ONCHIP] * 5,
        out_specs=HBM,
        scratch_shapes=[pltpu.VMEM((n, D), BF16), pltpu.SemaphoreType.DMA((n // ATT_TILE,))],
        compiler_params=grant(12),
        cost_estimate=pl.CostEstimate(flops=4 * n * D * MEM_DEV, transcendentals=0, bytes_accessed=8 << 20),
        name="finish",
    )(*onchip(own, peer, w_own, w_peer, conv_sum))


def body(
    tokens,
    passage_ids,
    passage_store,
    norm_gain,
    conv_value_weight,
    conv_gate_weight,
    conv_weight,
    ln_gain,
    query_weight,
    query_gain,
    passage_gain,
    key_weight,
    value_weight,
    key_gain,
    memory_gate,
    conv_out_weight,
    memory_out_weight,
):
    owner_count = lax.axis_size("st")
    swap = [(0, 1), (1, 0)]
    me = lax.axis_index("tp").astype(jnp.int32).reshape(1)

    everyone = jnp.arange(owner_count, dtype=jnp.int32)[:, None, None, None]
    spread = jnp.broadcast_to(passage_ids, (owner_count, LANES, *passage_ids.shape))
    wanted = jnp.sum(jnp.where(spread >> OWNER_SHIFT == everyone, spread & (PASS_DEV - 1), 0), axis=(2, 3))
    asked = lax.all_to_all(wanted, "st", 0, 0, tiled=True)
    peer_tokens = lax.ppermute(tokens, "tp", swap)
    peer_conv_weight = lax.ppermute(conv_out_weight, "tp", swap)
    peer_memory_weight = lax.ppermute(memory_out_weight, "tp", swap)

    kv = project_store(
        passage_store.reshape(-1, D),
        passage_gain.reshape(-1, LANES),
        key_weight,
        value_weight,
        key_gain.reshape(-1, LANES),
    ).reshape(PASS_DEV, PLEN, 2 * MEM_DEV)
    sent = fill_slots(asked, kv)
    received = lax.all_to_all(sent, "st", 0, 0, tiled=True)

    filtered, own_stats, queries = token_branch(
        me,
        tokens,
        peer_tokens,
        norm_gain.reshape(2, -1, LANES),
        conv_value_weight,
        conv_gate_weight,
        query_weight,
        conv_weight,
        query_gain.reshape(-1, LANES),
    )
    peer_stats = lax.ppermute(own_stats, "tp", swap)
    conv_theirs = channel_swish(1 - me, filtered, own_stats, peer_stats, ln_gain.reshape(-1, LANES))
    conv_peer = lax.ppermute(conv_theirs, "tp", swap)
    conv_mine = channel_swish(me, filtered, own_stats, peer_stats, ln_gain.reshape(-1, LANES))
    conv_sum = conv_product(conv_mine, conv_peer, conv_out_weight, peer_conv_weight)

    received, conv_sum = lax.optimization_barrier((received, conv_sum))
    owners = lax.optimization_barrier((passage_ids, filtered))[0].reshape(-1) >> OWNER_SHIFT
    gate = memory_gate.reshape(-1, LANES)
    memory_theirs, next_kv, next_queries = attend_first(1 - me, owners, received, queries, gate)
    memory_peer = lax.ppermute(memory_theirs, "tp", swap)
    memory_mine = attend_rest(next_kv, next_queries, gate)
    return finish(memory_mine, memory_peer, memory_out_weight, peer_memory_weight, conv_sum)


def solution(mesh):
    return jax.shard_map(
        body,
        mesh=mesh,
        in_specs=(
            P("st", "tp"),
            P("st", None),
            P("st", None, None),
            P(),
            P(None, "tp"),
            P(None, "tp"),
            P(None, "tp"),
            P("tp"),
            P(None, "tp"),
            P("tp"),
            P(),
            P(None, "tp"),
            P(None, "tp"),
            P("tp"),
            P("tp"),
            P("tp", None),
            P("tp", None),
        ),
        out_specs=P(("st", "tp"), None),
        check_vma=False,
    )
```

```python
import jax
import jax.numpy as jnp
from jax import lax
from jax.experimental import pallas as pl
from jax.experimental.pallas import tpu as pltpu
from jax.sharding import PartitionSpec as P

D = 2048
HALF_D = 1024
C_A = 1536
C_DEV = 768
MEM_HD = 64
MEM_DEV = 256
KW = 31
SEQ_LEN = 512
BLOCK = 64
PLEN = 64
PASS_DEV = 16
OWNER_SHIFT = 4
NORM_EPS = 1e-06
LAYER_EPS = 1e-05

KV_TILE = 512
TOK_TILE = 256
OUT_TILE = 256
OUT_COLS = 512
ATT_TILE = 256
ATT_GROUP = 4
LANES = 128
CONV_ROWS = 128
NORM_ROWS = 16
HISTORY = 32

F32 = jnp.float32
BF16 = jnp.bfloat16


def matmul(a, b):
    return lax.dot_general(a, b, (((1,), (0,)), ((), ())), preferred_element_type=F32)


def matmul_t(a, b):
    return lax.dot_general(a, b, (((1,), (1,)), ((), ())), preferred_element_type=F32)


def row_norm(rows, gain):
    widened = rows.astype(F32)
    factor = lax.rsqrt(jnp.sum(widened * widened, axis=1, keepdims=True) * (1.0 / D) + NORM_EPS)
    return (widened * factor * gain).astype(BF16)


def head_norm(product, gain):
    width = product.shape[1]
    rows = lax.broadcasted_iota(jnp.int32, (width, width), 0) // MEM_HD
    cols = lax.broadcasted_iota(jnp.int32, (width, width), 1) // MEM_HD
    same_head = jnp.where(rows == cols, 1.0, 0.0).astype(BF16)
    squares = product * product
    coarse = squares.astype(BF16)
    fine = (squares - coarse.astype(F32)).astype(BF16)
    total = matmul(coarse, same_head) + matmul(fine, same_head)
    return product * lax.rsqrt(total * (1.0 / MEM_HD) + NORM_EPS) * gain


def wide_row(ref):
    values = ref[...].astype(F32)
    return jnp.concatenate([values[i : i + 1, :] for i in range(values.shape[0])], axis=1)


def kv_kernel(
    rows_hbm, gain_hbm, wk_hbm, wv_hbm, kg_hbm, out_ref,
    rows_ref, gain_ref, w_ref, kg_ref, even, odd, r_sem, w_sem
):
    chunks = rows_hbm.shape[0] // KV_TILE
    span = lambda c: pl.ds(c * KV_TILE, KV_TILE)
    row_copies = [pltpu.make_async_copy(rows_hbm.at[span(c)], rows_ref.at[span(c)], r_sem.at[c]) for c in range(chunks)]
    wk_copy = pltpu.make_async_copy(wk_hbm, w_ref.at[:, :MEM_DEV], w_sem.at[0])
    wv_copy = pltpu.make_async_copy(wv_hbm, w_ref.at[:, MEM_DEV:], w_sem.at[1])
    gain_copy = pltpu.make_async_copy(gain_hbm, gain_ref, w_sem.at[2])
    kg_copy = pltpu.make_async_copy(kg_hbm, kg_ref, w_sem.at[3])
    for c in [gain_copy, kg_copy, row_copies[0], wk_copy, wv_copy, *row_copies[1:]]:
        c.start()
    gain_copy.wait()
    kg_copy.wait()
    gain = wide_row(gain_ref)
    key_gain = wide_row(kg_ref)
    held = (even, odd)

    def normalise(c):
        for r in range(0, KV_TILE, NORM_ROWS):
            rows = rows_ref[c * KV_TILE + r : c * KV_TILE + r + NORM_ROWS, :]
            held[c % 2][r : r + NORM_ROWS, :] = row_norm(rows, gain)

    row_copies[0].wait()
    normalise(0)
    wk_copy.wait()
    wv_copy.wait()
    for c in range(chunks):
        if c + 1 < chunks:
            row_copies[c + 1].wait()
            normalise(c + 1)
        both = matmul(held[c % 2][...], w_ref[...])
        out_ref[span(c), :MEM_DEV] = head_norm(both[:, :MEM_DEV], key_gain).astype(BF16)
        out_ref[span(c), MEM_DEV:] = both[:, MEM_DEV:].astype(BF16)


def resident(shape):
    zeros = (0,) * len(shape)
    return pl.BlockSpec(shape, lambda *_: zeros, pipeline_mode=pl.Buffered(1))


HBM = pl.BlockSpec(memory_space=pl.ANY)
ONCHIP = pl.BlockSpec(memory_space=pltpu.VMEM)


def onchip(*arrays):
    return tuple(pltpu.with_memory_space_constraint(a, pltpu.VMEM) for a in arrays)


def offchip(*arrays):
    return tuple(pltpu.with_memory_space_constraint(a, pltpu.HBM) for a in arrays)


def grant(mib):
    return pltpu.CompilerParams(vmem_limit_bytes=mib << 20)


def project_store(rows, passage_gain, key_weight, value_weight, key_gain):
    n = rows.shape[0]
    return pl.pallas_call(
        kv_kernel,
        out_shape=pltpu.VMEM((n, 2 * MEM_DEV), BF16),
        in_specs=[HBM] * 5,
        out_specs=ONCHIP,
        scratch_shapes=[
            pltpu.VMEM((n, D), BF16),
            pltpu.VMEM((D // LANES, LANES), BF16),
            pltpu.VMEM((D, 2 * MEM_DEV), BF16),
            pltpu.VMEM((MEM_DEV // LANES, LANES), BF16),
            pltpu.VMEM((KV_TILE, D), BF16),
            pltpu.VMEM((KV_TILE, D), BF16),
            pltpu.SemaphoreType.DMA((n // KV_TILE,)),
            pltpu.SemaphoreType.DMA((4,)),
        ],
        compiler_params=grant(24),
        cost_estimate=pl.CostEstimate(flops=2 * n * D * 2 * MEM_DEV, transcendentals=0, bytes_accessed=8 << 20),
        name="project_store",
    )(*offchip(rows, passage_gain, key_weight, value_weight, key_gain))


def slots_kernel(asked_ref, kv_ref, out_ref, table, table_sem, sem):
    count = out_ref.shape[0]
    fetch = pltpu.make_async_copy(asked_ref, table, table_sem)
    fetch.start()
    fetch.wait()
    copies = [pltpu.make_async_copy(kv_ref.at[table[s, 0]], out_ref.at[s], sem.at[s]) for s in range(count)]
    for c in copies:
        c.start()
    for c in copies:
        c.wait()


def fill_slots(asked, kv):
    count = asked.shape[0]
    return pl.pallas_call(
        slots_kernel,
        out_shape=pltpu.HBM((count, PLEN, 2 * MEM_DEV), BF16),
        in_specs=[ONCHIP, ONCHIP],
        out_specs=HBM,
        scratch_shapes=[
            pltpu.SMEM(asked.shape, jnp.int32),
            pltpu.SemaphoreType.DMA(()),
            pltpu.SemaphoreType.DMA((count,)),
        ],
        compiler_params=grant(2),
        name="fill_slots",
    )(*onchip(asked, kv))


def token_kernel(
    tp_ref, own_ref, peer_ref, gain_ref, wv_ref, wg_ref, wq_ref, cw_ref, qg_ref, filt_ref, stat_ref, q_ref, xs_ref, taps_ref,
    own_n, peer_n
):
    tile = pl.program_id(0)
    me = tp_ref[0]
    own_at = pl.multiple_of(me * HALF_D, HALF_D)
    peer_at = pl.multiple_of((1 - me) * HALF_D, HALF_D)
    own_gain = wide_row(gain_ref.at[me])
    peer_gain = wide_row(gain_ref.at[1 - me])
    for r in range(0, TOK_TILE, NORM_ROWS):
        rows = slice(r, r + NORM_ROWS)
        own = own_ref[rows, :].astype(F32)
        peer = peer_ref[rows, :].astype(F32)
        total = jnp.sum(own * own + peer * peer, axis=1, keepdims=True)
        factor = lax.rsqrt(total * (1.0 / D) + NORM_EPS)
        own_n[rows, :] = (own * factor * own_gain).astype(BF16)
        peer_n[rows, :] = (peer * factor * peer_gain).astype(BF16)

    def product(w_ref):
        own_part = matmul(own_n[...], w_ref[pl.ds(own_at, HALF_D), :])
        return own_part + matmul(peer_n[...], w_ref[pl.ds(peer_at, HALF_D), :])

    q_ref[...] = head_norm(product(wq_ref), wide_row(qg_ref) * MEM_HD ** (-0.5)).astype(BF16)
    gated = (product(wv_ref) * jax.nn.sigmoid(product(wg_ref))).astype(BF16)

    @pl.when(tile % (SEQ_LEN // TOK_TILE) == 0)
    def _():
        xs_ref[:HISTORY, :] = jnp.zeros((HISTORY, C_DEV), F32)

    taps_ref[...] = cw_ref[...].astype(F32)
    xs_ref[HISTORY:, :] = gated.astype(F32)
    first = HISTORY - (KW - 1)
    for base in range(0, TOK_TILE, CONV_ROWS):
        sums = jnp.zeros((CONV_ROWS, LANES), F32)
        squares = jnp.zeros((CONV_ROWS, LANES), F32)
        for lane in range(0, C_DEV, LANES):
            lanes = slice(lane, lane + LANES)
            acc = None
            for r in range(8):
                steps = [s for s in range(first, first + KW) if s % 8 == r]
                reach = max(steps) - r + CONV_ROWS
                shifted = xs_ref[base + r : base + r + reach, lanes]
                part = None
                for s in steps:
                    term = shifted[s - r : s - r + CONV_ROWS] * taps_ref[s - first : s - first + 1, lanes]
                    part = term if part is None else part + term
                acc = part if acc is None else acc + part
            filt_ref[base : base + CONV_ROWS, lanes] = acc
            sums = sums + acc
            squares = squares + acc * acc
        stat_ref[base : base + CONV_ROWS, 0:1] = jnp.sum(sums, axis=1, keepdims=True)
        stat_ref[base : base + CONV_ROWS, 1:2] = jnp.sum(squares, axis=1, keepdims=True)
    xs_ref[:HISTORY, :] = xs_ref[TOK_TILE:, :]


def token_branch(me, own, peer, gain, wv, wg, wq, cw, qg):
    n = own.shape[0]
    tile = lambda width: pl.BlockSpec((TOK_TILE, width), lambda i, s: (i, 0))
    return pl.pallas_call(
        token_kernel,
        out_shape=(
            jax.ShapeDtypeStruct((n, C_DEV), F32),
            jax.ShapeDtypeStruct((n, 2), F32),
            jax.ShapeDtypeStruct((n, MEM_DEV), BF16),
        ),
        grid_spec=pltpu.PrefetchScalarGridSpec(
            num_scalar_prefetch=1,
            grid=(n // TOK_TILE,),
            in_specs=[
                tile(HALF_D),
                tile(HALF_D),
                resident((2, HALF_D // LANES, LANES)),
                resident((D, C_DEV)),
                resident((D, C_DEV)),
                resident((D, MEM_DEV)),
                resident((KW, C_DEV)),
                resident((MEM_DEV // LANES, LANES)),
            ],
            out_specs=(tile(C_DEV), tile(2), tile(MEM_DEV)),
            scratch_shapes=[
                pltpu.VMEM((HISTORY + TOK_TILE, C_DEV), F32),
                pltpu.VMEM((KW, C_DEV), F32),
                pltpu.VMEM((TOK_TILE, HALF_D), BF16),
                pltpu.VMEM((TOK_TILE, HALF_D), BF16),
            ],
        ),
        cost_estimate=pl.CostEstimate(flops=20 * n * D * 768, transcendentals=0, bytes_accessed=16 << 20),
        name="token_branch",
    )(me, own, peer, gain, wv, wg, wq, cw, qg)


def swish_kernel(filt_ref, own_ref, peer_ref, gain_ref, out_ref):
    stats = (own_ref[...] + peer_ref[...]) * (1.0 / C_A)
    mean = stats[:, 0:1]
    var = stats[:, 1:2] - mean * mean
    scaled = (filt_ref[...] - mean) * lax.rsqrt(var + LAYER_EPS) * wide_row(gain_ref)
    out_ref[...] = (scaled * jax.nn.sigmoid(scaled)).astype(BF16)


def channel_swish(half, filtered, own_stats, peer_stats, gain):
    n = filtered.shape[0] // 2
    steps = n // OUT_TILE
    tile = lambda width: pl.BlockSpec((OUT_TILE, width), lambda i, h: (h[0] * steps + i, 0))
    return pl.pallas_call(
        lambda half_ref, *refs: swish_kernel(*refs),
        out_shape=jax.ShapeDtypeStruct((n, C_DEV), BF16),
        grid_spec=pltpu.PrefetchScalarGridSpec(
            num_scalar_prefetch=1,
            grid=(steps,),
            in_specs=[tile(C_DEV), tile(2), tile(2), resident((C_DEV // LANES, LANES))],
            out_specs=pl.BlockSpec((OUT_TILE, C_DEV), lambda i, h: (i, 0)),
        ),
        cost_estimate=pl.CostEstimate(flops=n * D * 768, transcendentals=0, bytes_accessed=4 << 20),
        name="channel_swish",
    )(half, filtered, own_stats, peer_stats, gain)


def pair_kernel(own_ref, peer_ref, w_own_hbm, w_peer_hbm, out_ref, w_own_ref, w_peer_ref, sem):
    parts = D // OUT_COLS
    cols = lambda c: pl.ds(c * OUT_COLS, OUT_COLS)
    copies = [
        pltpu.make_async_copy(hbm.at[:, cols(c)], ref.at[:, cols(c)], sem.at[i, c])
        for c in range(parts)
        for i, (hbm, ref) in enumerate(((w_own_hbm, w_own_ref), (w_peer_hbm, w_peer_ref)))
    ]
    for c in copies:
        c.start()
    for c in range(parts):
        copies[2 * c].wait()
        copies[2 * c + 1].wait()
        own_part = matmul(own_ref[...], w_own_ref[:, cols(c)])
        out_ref[:, cols(c)] = (own_part + matmul(peer_ref[...], w_peer_ref[:, cols(c)])).astype(BF16)


def conv_product(own, peer, w_own, w_peer):
    n = own.shape[0]
    return pl.pallas_call(
        pair_kernel,
        out_shape=pltpu.HBM((n, D), BF16),
        in_specs=[ONCHIP, ONCHIP, HBM, HBM],
        out_specs=pl.BlockSpec((n, D), lambda: (0, 0)),
        scratch_shapes=[
            pltpu.VMEM((C_DEV, D), BF16),
            pltpu.VMEM((C_DEV, D), BF16),
            pltpu.SemaphoreType.DMA((2, D // OUT_COLS)),
        ],
        compiler_params=grant(16),
        cost_estimate=pl.CostEstimate(flops=4 * n * D * C_DEV, transcendentals=0, bytes_accessed=12 << 20),
        name="conv_product",
    )(*onchip(own, peer), *offchip(w_own, w_peer))


def attend_blocks(blocks, kv_ref, q_ref, base, gate):
    heads = MEM_DEV // MEM_HD
    lane_head = lax.broadcasted_iota(jnp.int32, (BLOCK, MEM_DEV), 1) // MEM_HD
    scores = []
    for b in blocks:
        q = q_ref[pl.ds(base + b * BLOCK, BLOCK), :]
        spread = jnp.concatenate([jnp.where(lane_head == h, q, jnp.zeros_like(q)) for h in range(heads)], axis=0)
        scores.append(matmul_t(spread, kv_ref[2 * b : 2 * b + 2, :, :MEM_DEV].reshape(2 * PLEN, MEM_DEV)))
    expanded = [jnp.exp(s - jnp.max(s, axis=1, keepdims=True)) for s in scores]
    weights = [(e * (1.0 / jnp.sum(e, axis=1, keepdims=True))).astype(BF16) for e in expanded]
    rows = []
    for w, b in zip(weights, blocks):
        mixed = matmul(w, kv_ref[2 * b : 2 * b + 2, :, MEM_DEV:].reshape(2 * PLEN, MEM_DEV))
        attended = mixed[:BLOCK]
        for h in range(1, heads):
            attended = jnp.where(lane_head == h, mixed[h * BLOCK : (h + 1) * BLOCK], attended)
        rows.append((attended * gate).astype(BF16))
    return jnp.concatenate(rows, axis=0)


SCALARS = pl.BlockSpec(memory_space=pltpu.SMEM)


def attend_all(out_ref, kv_ref, q_ref, base, gate, arrived):
    size = ATT_GROUP * BLOCK
    for g in range(out_ref.shape[0] // size):
        arrived(g)
        blocks = range(g * ATT_GROUP, (g + 1) * ATT_GROUP)
        out_ref[pl.ds(g * size, size), :] = attend_blocks(blocks, kv_ref, q_ref, base, gate)


def attend_kernel(
    half_ref, owner_ref, recv_hbm, q_ref, gate_ref, out_ref, next_kv_ref, next_q_ref, kv_ref, sem, next_sem, q_sem
):
    count = kv_ref.shape[0]
    n = next_q_ref.shape[0]
    first, second = half_ref[0], 1 - half_ref[0]
    copies = [
        pltpu.make_async_copy(recv_hbm.at[owner_ref[first * count + i]], kv_ref.at[i], sem.at[i]) for i in range(count)
    ]
    later = [
        pltpu.make_async_copy(recv_hbm.at[owner_ref[second * count + i]], next_kv_ref.at[i], next_sem.at[i])
        for i in range(count)
    ] + [pltpu.make_async_copy(q_ref.at[pl.ds(pl.multiple_of(second * n, n), n), :], next_q_ref, q_sem)]
    for c in copies:
        c.start()
    gate = jnp.tanh(wide_row(gate_ref))

    def arrived(g):
        for c in copies[2 * g * ATT_GROUP : 2 * (g + 1) * ATT_GROUP]:
            c.wait()
        if g == 0:
            for c in later:
                c.start()

    attend_all(out_ref, kv_ref, q_ref, pl.multiple_of(first * n, n), gate, arrived)
    for c in later:
        c.wait()


def attend_first(half, owners, received, queries, gate):
    n = queries.shape[0] // 2
    count = owners.shape[0] // 2
    return pl.pallas_call(
        attend_kernel,
        out_shape=(
            pltpu.VMEM((n, MEM_DEV), BF16),
            pltpu.VMEM((count, PLEN, 2 * MEM_DEV), BF16),
            pltpu.VMEM((n, MEM_DEV), BF16),
        ),
        in_specs=[SCALARS, SCALARS, HBM, ONCHIP, ONCHIP],
        out_specs=(ONCHIP, ONCHIP, ONCHIP),
        scratch_shapes=[
            pltpu.VMEM((count, PLEN, 2 * MEM_DEV), BF16),
            pltpu.SemaphoreType.DMA((count,)),
            pltpu.SemaphoreType.DMA((count,)),
            pltpu.SemaphoreType.DMA(()),
        ],
        compiler_params=grant(8),
        cost_estimate=pl.CostEstimate(flops=n * D * 256, transcendentals=0, bytes_accessed=2 << 20),
        name="attend_first",
    )(half, owners, *offchip(received), *onchip(queries, gate))


def attend_rest_kernel(kv_ref, q_ref, gate_ref, out_ref):
    attend_all(out_ref, kv_ref, q_ref, 0, jnp.tanh(wide_row(gate_ref)), lambda g: None)


def attend_rest(kv, queries, gate):
    n = queries.shape[0]
    return pl.pallas_call(
        attend_rest_kernel,
        out_shape=pltpu.VMEM((n, MEM_DEV), BF16),
        in_specs=[ONCHIP] * 3,
        out_specs=ONCHIP,
        compiler_params=grant(6),
        cost_estimate=pl.CostEstimate(flops=n * D * 256, transcendentals=0, bytes_accessed=2 << 20),
        name="attend_rest",
    )(*onchip(kv, queries, gate))


def finish_kernel(own_ref, peer_ref, w_own_ref, w_peer_ref, conv_ref, out_hbm, out_ref, out_sem):
    groups = out_ref.shape[0] // ATT_TILE
    span = lambda g: pl.ds(g * ATT_TILE, ATT_TILE)
    out_copies = [pltpu.make_async_copy(out_ref.at[span(g)], out_hbm.at[span(g)], out_sem.at[g]) for g in range(groups)]
    for g in range(groups):
        memory = matmul(own_ref[span(g), :], w_own_ref[...]) + matmul(peer_ref[span(g), :], w_peer_ref[...])
        out_ref[span(g), :] = (conv_ref[span(g), :].astype(F32) + memory).astype(BF16)
        out_copies[g].start()
    for c in out_copies:
        c.wait()


def finish(own, peer, w_own, w_peer, conv_sum):
    n = conv_sum.shape[0]
    return pl.pallas_call(
        finish_kernel,
        out_shape=pltpu.HBM((n, D), BF16),
        in_specs=[ONCHIP] * 5,
        out_specs=HBM,
        scratch_shapes=[pltpu.VMEM((n, D), BF16), pltpu.SemaphoreType.DMA((n // ATT_TILE,))],
        compiler_params=grant(12),
        cost_estimate=pl.CostEstimate(flops=4 * n * D * MEM_DEV, transcendentals=0, bytes_accessed=8 << 20),
        name="finish",
    )(*onchip(own, peer, w_own, w_peer, conv_sum))


def body(
    tokens,
    passage_ids,
    passage_store,
    norm_gain,
    conv_value_weight,
    conv_gate_weight,
    conv_weight,
    ln_gain,
    query_weight,
    query_gain,
    passage_gain,
    key_weight,
    value_weight,
    key_gain,
    memory_gate,
    conv_out_weight,
    memory_out_weight,
):
    owner_count = lax.axis_size("st")
    swap = [(0, 1), (1, 0)]
    me = lax.axis_index("tp").astype(jnp.int32).reshape(1)

    everyone = lax.broadcasted_iota(jnp.int32, (owner_count, LANES, *passage_ids.shape), 0)
    local = passage_ids ^ (everyone << OWNER_SHIFT)
    wanted = jnp.sum(jnp.where(local < PASS_DEV, local, 0), axis=(2, 3))
    asked = lax.all_to_all(wanted, "st", 0, 0, tiled=True)
    peer_tokens = lax.ppermute(tokens, "tp", swap)
    peer_conv_weight = lax.ppermute(conv_out_weight, "tp", swap)
    peer_memory_weight = lax.ppermute(memory_out_weight, "tp", swap)

    kv = project_store(
        passage_store.reshape(-1, D),
        passage_gain.reshape(-1, LANES),
        key_weight,
        value_weight,
        key_gain.reshape(-1, LANES),
    ).reshape(PASS_DEV, PLEN, 2 * MEM_DEV)
    sent = fill_slots(asked, kv)
    received = lax.all_to_all(sent, "st", 0, 0, tiled=True)

    filtered, own_stats, queries = token_branch(
        me,
        tokens,
        peer_tokens,
        norm_gain.reshape(2, -1, LANES),
        conv_value_weight,
        conv_gate_weight,
        query_weight,
        conv_weight,
        query_gain.reshape(-1, LANES),
    )
    peer_stats = lax.ppermute(own_stats, "tp", swap)
    conv_theirs = channel_swish(1 - me, filtered, own_stats, peer_stats, ln_gain.reshape(-1, LANES))
    conv_peer = lax.ppermute(conv_theirs, "tp", swap)
    conv_mine = channel_swish(me, filtered, own_stats, peer_stats, ln_gain.reshape(-1, LANES))
    conv_sum = conv_product(conv_mine, conv_peer, conv_out_weight, peer_conv_weight)

    owners = lax.optimization_barrier((passage_ids, filtered))[0].reshape(-1) >> OWNER_SHIFT
    gate = memory_gate.reshape(-1, LANES)
    memory_theirs, next_kv, next_queries = attend_first(1 - me, owners, received, queries, gate)
    memory_peer = lax.ppermute(memory_theirs, "tp", swap)
    memory_mine = attend_rest(next_kv, next_queries, gate)
    return finish(memory_mine, memory_peer, memory_out_weight, peer_memory_weight, conv_sum)


def solution(mesh):
    return jax.shard_map(
        body,
        mesh=mesh,
        in_specs=(
            P("st", "tp"),
            P("st", None),
            P("st", None, None),
            P(),
            P(None, "tp"),
            P(None, "tp"),
            P(None, "tp"),
            P("tp"),
            P(None, "tp"),
            P("tp"),
            P(),
            P(None, "tp"),
            P(None, "tp"),
            P("tp"),
            P("tp"),
            P("tp", None),
            P("tp", None),
        ),
        out_specs=P(("st", "tp"), None),
        check_vma=False,
    )
```

```python
import jax
import jax.numpy as jnp
from jax import lax
from jax.experimental import pallas as pl
from jax.experimental.pallas import tpu as pltpu
from jax.sharding import PartitionSpec as P

D = 2048
HALF_D = 1024
C_A = 1536
C_DEV = 768
MEM_HD = 64
MEM_DEV = 256
KW = 31
SEQ_LEN = 512
BLOCK = 64
PLEN = 64
PASS_DEV = 16
OWNER_SHIFT = 4
NORM_EPS = 1e-06
LAYER_EPS = 1e-05

KV_TILE = 512
TOK_TILE = 256
OUT_TILE = 256
OUT_COLS = 512
ATT_TILE = 256
ATT_GROUP = 4
LANES = 128
CONV_ROWS = 128
NORM_ROWS = 16
HISTORY = 32

F32 = jnp.float32
BF16 = jnp.bfloat16


def matmul(a, b):
    return lax.dot_general(a, b, (((1,), (0,)), ((), ())), preferred_element_type=F32)


def matmul_t(a, b):
    return lax.dot_general(a, b, (((1,), (1,)), ((), ())), preferred_element_type=F32)


def row_norm(rows, gain):
    widened = rows.astype(F32)
    factor = lax.rsqrt(jnp.sum(widened * widened, axis=1, keepdims=True) * (1.0 / D) + NORM_EPS)
    return (widened * factor * gain).astype(BF16)


def head_norm(product, gain):
    width = product.shape[1]
    rows = lax.broadcasted_iota(jnp.int32, (width, width), 0) // MEM_HD
    cols = lax.broadcasted_iota(jnp.int32, (width, width), 1) // MEM_HD
    same_head = jnp.where(rows == cols, 1.0, 0.0).astype(BF16)
    squares = product * product
    coarse = squares.astype(BF16)
    fine = (squares - coarse.astype(F32)).astype(BF16)
    total = matmul(coarse, same_head) + matmul(fine, same_head)
    return product * lax.rsqrt(total * (1.0 / MEM_HD) + NORM_EPS) * gain


def wide_row(ref):
    values = ref[...].astype(F32)
    return jnp.concatenate([values[i : i + 1, :] for i in range(values.shape[0])], axis=1)


def kv_kernel(
    rows_hbm, gain_hbm, wk_hbm, wv_hbm, kg_hbm, out_ref,
    rows_ref, gain_ref, w_ref, kg_ref, even, odd, r_sem, w_sem
):
    chunks = rows_hbm.shape[0] // KV_TILE
    span = lambda c: pl.ds(c * KV_TILE, KV_TILE)
    row_copies = [pltpu.make_async_copy(rows_hbm.at[span(c)], rows_ref.at[span(c)], r_sem.at[c]) for c in range(chunks)]
    wk_copy = pltpu.make_async_copy(wk_hbm, w_ref.at[:, :MEM_DEV], w_sem.at[0])
    wv_copy = pltpu.make_async_copy(wv_hbm, w_ref.at[:, MEM_DEV:], w_sem.at[1])
    gain_copy = pltpu.make_async_copy(gain_hbm, gain_ref, w_sem.at[2])
    kg_copy = pltpu.make_async_copy(kg_hbm, kg_ref, w_sem.at[3])
    for c in [gain_copy, kg_copy, row_copies[0], wk_copy, wv_copy, *row_copies[1:]]:
        c.start()
    gain_copy.wait()
    kg_copy.wait()
    gain = wide_row(gain_ref)
    key_gain = wide_row(kg_ref)
    held = (even, odd)

    def normalise(c):
        for r in range(0, KV_TILE, NORM_ROWS):
            rows = rows_ref[c * KV_TILE + r : c * KV_TILE + r + NORM_ROWS, :]
            held[c % 2][r : r + NORM_ROWS, :] = row_norm(rows, gain)

    row_copies[0].wait()
    normalise(0)
    wk_copy.wait()
    wv_copy.wait()
    for c in range(chunks):
        if c + 1 < chunks:
            row_copies[c + 1].wait()
            normalise(c + 1)
        both = matmul(held[c % 2][...], w_ref[...])
        out_ref[span(c), :MEM_DEV] = head_norm(both[:, :MEM_DEV], key_gain).astype(BF16)
        out_ref[span(c), MEM_DEV:] = both[:, MEM_DEV:].astype(BF16)


def resident(shape):
    zeros = (0,) * len(shape)
    return pl.BlockSpec(shape, lambda *_: zeros, pipeline_mode=pl.Buffered(1))


HBM = pl.BlockSpec(memory_space=pl.ANY)
ONCHIP = pl.BlockSpec(memory_space=pltpu.VMEM)


def onchip(*arrays):
    return tuple(pltpu.with_memory_space_constraint(a, pltpu.VMEM) for a in arrays)


def offchip(*arrays):
    return tuple(pltpu.with_memory_space_constraint(a, pltpu.HBM) for a in arrays)


def grant(mib):
    return pltpu.CompilerParams(vmem_limit_bytes=mib << 20)


def project_store(rows, passage_gain, key_weight, value_weight, key_gain):
    n = rows.shape[0]
    return pl.pallas_call(
        kv_kernel,
        out_shape=pltpu.VMEM((n, 2 * MEM_DEV), BF16),
        in_specs=[HBM] * 5,
        out_specs=ONCHIP,
        scratch_shapes=[
            pltpu.VMEM((n, D), BF16),
            pltpu.VMEM((D // LANES, LANES), BF16),
            pltpu.VMEM((D, 2 * MEM_DEV), BF16),
            pltpu.VMEM((MEM_DEV // LANES, LANES), BF16),
            pltpu.VMEM((KV_TILE, D), BF16),
            pltpu.VMEM((KV_TILE, D), BF16),
            pltpu.SemaphoreType.DMA((n // KV_TILE,)),
            pltpu.SemaphoreType.DMA((4,)),
        ],
        compiler_params=grant(24),
        cost_estimate=pl.CostEstimate(flops=2 * n * D * 2 * MEM_DEV, transcendentals=0, bytes_accessed=8 << 20),
        name="project_store",
    )(*offchip(rows, passage_gain, key_weight, value_weight, key_gain))


def slots_kernel(st_ref, ids_ref, kv_ref, out_hbm, row_ref, table, table_sem, sem):
    count = out_hbm.shape[0]
    local = ids_ref[...] ^ (st_ref[0] * PASS_DEV)
    asked = jnp.where(local < PASS_DEV, local, 0)
    asked = jnp.sum(asked[:, 0, :] + asked[:, 1, :], axis=1, keepdims=True).astype(F32)
    square = jnp.concatenate([jnp.broadcast_to(asked, (count, LANES)), jnp.zeros((LANES - count, LANES), F32)], axis=0)
    row_ref[...] = square.T[:8, :].astype(jnp.int32)
    fetch = pltpu.make_async_copy(row_ref, table, table_sem)
    fetch.start()
    fetch.wait()
    copies = [pltpu.make_async_copy(kv_ref.at[table[0, s]], out_hbm.at[s], sem.at[s]) for s in range(count)]
    for c in copies:
        c.start()
    for c in copies:
        c.wait()


def fill_slots(st, ids, kv):
    count = ids.shape[0]
    return pl.pallas_call(
        slots_kernel,
        out_shape=pltpu.HBM((count, PLEN, 2 * MEM_DEV), BF16),
        in_specs=[pl.BlockSpec(memory_space=pltpu.SMEM), ONCHIP, ONCHIP],
        out_specs=HBM,
        scratch_shapes=[
            pltpu.VMEM((8, LANES), jnp.int32),
            pltpu.SMEM((8, LANES), jnp.int32),
            pltpu.SemaphoreType.DMA(()),
            pltpu.SemaphoreType.DMA((count,)),
        ],
        compiler_params=grant(2),
        name="fill_slots",
    )(st, *onchip(ids, kv))


def token_kernel(
    tp_ref, own_ref, peer_ref, gain_ref, wv_ref, wg_ref, wq_ref, cw_ref, qg_ref, filt_ref, stat_ref, q_ref, xs_ref, taps_ref,
    own_n, peer_n
):
    tile = pl.program_id(0)
    me = tp_ref[0]
    own_at = pl.multiple_of(me * HALF_D, HALF_D)
    peer_at = pl.multiple_of((1 - me) * HALF_D, HALF_D)
    own_gain = wide_row(gain_ref.at[me])
    peer_gain = wide_row(gain_ref.at[1 - me])
    for r in range(0, TOK_TILE, NORM_ROWS):
        rows = slice(r, r + NORM_ROWS)
        own = own_ref[rows, :].astype(F32)
        peer = peer_ref[rows, :].astype(F32)
        total = jnp.sum(own * own + peer * peer, axis=1, keepdims=True)
        factor = lax.rsqrt(total * (1.0 / D) + NORM_EPS)
        own_n[rows, :] = (own * factor * own_gain).astype(BF16)
        peer_n[rows, :] = (peer * factor * peer_gain).astype(BF16)

    def product(w_ref):
        own_part = matmul(own_n[...], w_ref[pl.ds(own_at, HALF_D), :])
        return own_part + matmul(peer_n[...], w_ref[pl.ds(peer_at, HALF_D), :])

    q_ref[...] = head_norm(product(wq_ref), wide_row(qg_ref) * MEM_HD ** (-0.5)).astype(BF16)
    gated = (product(wv_ref) * jax.nn.sigmoid(product(wg_ref))).astype(BF16)

    @pl.when(tile % (SEQ_LEN // TOK_TILE) == 0)
    def _():
        xs_ref[:HISTORY, :] = jnp.zeros((HISTORY, C_DEV), F32)

    taps_ref[...] = cw_ref[...].astype(F32)
    xs_ref[HISTORY:, :] = gated.astype(F32)
    first = HISTORY - (KW - 1)
    for base in range(0, TOK_TILE, CONV_ROWS):
        sums = jnp.zeros((CONV_ROWS, LANES), F32)
        squares = jnp.zeros((CONV_ROWS, LANES), F32)
        for lane in range(0, C_DEV, LANES):
            lanes = slice(lane, lane + LANES)
            acc = None
            for r in range(8):
                steps = [s for s in range(first, first + KW) if s % 8 == r]
                reach = max(steps) - r + CONV_ROWS
                shifted = xs_ref[base + r : base + r + reach, lanes]
                part = None
                for s in steps:
                    term = shifted[s - r : s - r + CONV_ROWS] * taps_ref[s - first : s - first + 1, lanes]
                    part = term if part is None else part + term
                acc = part if acc is None else acc + part
            filt_ref[base : base + CONV_ROWS, lanes] = acc
            sums = sums + acc
            squares = squares + acc * acc
        stat_ref[base : base + CONV_ROWS, 0:1] = jnp.sum(sums, axis=1, keepdims=True)
        stat_ref[base : base + CONV_ROWS, 1:2] = jnp.sum(squares, axis=1, keepdims=True)
    xs_ref[:HISTORY, :] = xs_ref[TOK_TILE:, :]


def token_branch(me, own, peer, gain, wv, wg, wq, cw, qg):
    n = own.shape[0]
    tile = lambda width: pl.BlockSpec((TOK_TILE, width), lambda i, s: (i, 0))
    return pl.pallas_call(
        token_kernel,
        out_shape=(
            jax.ShapeDtypeStruct((n, C_DEV), F32),
            jax.ShapeDtypeStruct((n, 2), F32),
            jax.ShapeDtypeStruct((n, MEM_DEV), BF16),
        ),
        grid_spec=pltpu.PrefetchScalarGridSpec(
            num_scalar_prefetch=1,
            grid=(n // TOK_TILE,),
            in_specs=[
                tile(HALF_D),
                tile(HALF_D),
                resident((2, HALF_D // LANES, LANES)),
                resident((D, C_DEV)),
                resident((D, C_DEV)),
                resident((D, MEM_DEV)),
                resident((KW, C_DEV)),
                resident((MEM_DEV // LANES, LANES)),
            ],
            out_specs=(tile(C_DEV), tile(2), tile(MEM_DEV)),
            scratch_shapes=[
                pltpu.VMEM((HISTORY + TOK_TILE, C_DEV), F32),
                pltpu.VMEM((KW, C_DEV), F32),
                pltpu.VMEM((TOK_TILE, HALF_D), BF16),
                pltpu.VMEM((TOK_TILE, HALF_D), BF16),
            ],
        ),
        cost_estimate=pl.CostEstimate(flops=20 * n * D * 768, transcendentals=0, bytes_accessed=16 << 20),
        name="token_branch",
    )(me, own, peer, gain, wv, wg, wq, cw, qg)


def swish_kernel(filt_ref, own_ref, peer_ref, gain_ref, out_ref):
    stats = (own_ref[...] + peer_ref[...]) * (1.0 / C_A)
    mean = stats[:, 0:1]
    var = stats[:, 1:2] - mean * mean
    scaled = (filt_ref[...] - mean) * lax.rsqrt(var + LAYER_EPS) * wide_row(gain_ref)
    out_ref[...] = (scaled * jax.nn.sigmoid(scaled)).astype(BF16)


def channel_swish(half, filtered, own_stats, peer_stats, gain):
    n = filtered.shape[0] // 2
    steps = n // OUT_TILE
    tile = lambda width: pl.BlockSpec((OUT_TILE, width), lambda i, h: (h[0] * steps + i, 0))
    return pl.pallas_call(
        lambda half_ref, *refs: swish_kernel(*refs),
        out_shape=jax.ShapeDtypeStruct((n, C_DEV), BF16),
        grid_spec=pltpu.PrefetchScalarGridSpec(
            num_scalar_prefetch=1,
            grid=(steps,),
            in_specs=[tile(C_DEV), tile(2), tile(2), resident((C_DEV // LANES, LANES))],
            out_specs=pl.BlockSpec((OUT_TILE, C_DEV), lambda i, h: (i, 0)),
        ),
        cost_estimate=pl.CostEstimate(flops=n * D * 768, transcendentals=0, bytes_accessed=4 << 20),
        name="channel_swish",
    )(half, filtered, own_stats, peer_stats, gain)


def pair_kernel(own_ref, peer_ref, w_own_hbm, w_peer_hbm, out_ref, w_own_ref, w_peer_ref, sem):
    parts = D // OUT_COLS
    cols = lambda c: pl.ds(c * OUT_COLS, OUT_COLS)
    copies = [
        pltpu.make_async_copy(hbm.at[:, cols(c)], ref.at[:, cols(c)], sem.at[i, c])
        for c in range(parts)
        for i, (hbm, ref) in enumerate(((w_own_hbm, w_own_ref), (w_peer_hbm, w_peer_ref)))
    ]
    for c in copies:
        c.start()
    for c in range(parts):
        copies[2 * c].wait()
        copies[2 * c + 1].wait()
        own_part = matmul(own_ref[...], w_own_ref[:, cols(c)])
        out_ref[:, cols(c)] = (own_part + matmul(peer_ref[...], w_peer_ref[:, cols(c)])).astype(BF16)


def conv_product(own, peer, w_own, w_peer):
    n = own.shape[0]
    return pl.pallas_call(
        pair_kernel,
        out_shape=pltpu.HBM((n, D), BF16),
        in_specs=[ONCHIP, ONCHIP, HBM, HBM],
        out_specs=pl.BlockSpec((n, D), lambda: (0, 0)),
        scratch_shapes=[
            pltpu.VMEM((C_DEV, D), BF16),
            pltpu.VMEM((C_DEV, D), BF16),
            pltpu.SemaphoreType.DMA((2, D // OUT_COLS)),
        ],
        compiler_params=grant(16),
        cost_estimate=pl.CostEstimate(flops=4 * n * D * C_DEV, transcendentals=0, bytes_accessed=12 << 20),
        name="conv_product",
    )(*onchip(own, peer), *offchip(w_own, w_peer))


def attend_blocks(blocks, kv_ref, q_ref, base, gate):
    heads = MEM_DEV // MEM_HD
    lane_head = lax.broadcasted_iota(jnp.int32, (BLOCK, MEM_DEV), 1) // MEM_HD
    scores = []
    for b in blocks:
        q = q_ref[pl.ds(base + b * BLOCK, BLOCK), :]
        spread = jnp.concatenate([jnp.where(lane_head == h, q, jnp.zeros_like(q)) for h in range(heads)], axis=0)
        scores.append(matmul_t(spread, kv_ref[2 * b : 2 * b + 2, :, :MEM_DEV].reshape(2 * PLEN, MEM_DEV)))
    expanded = [jnp.exp(s - jnp.max(s, axis=1, keepdims=True)) for s in scores]
    weights = [(e * (1.0 / jnp.sum(e, axis=1, keepdims=True))).astype(BF16) for e in expanded]
    rows = []
    for w, b in zip(weights, blocks):
        mixed = matmul(w, kv_ref[2 * b : 2 * b + 2, :, MEM_DEV:].reshape(2 * PLEN, MEM_DEV))
        attended = mixed[:BLOCK]
        for h in range(1, heads):
            attended = jnp.where(lane_head == h, mixed[h * BLOCK : (h + 1) * BLOCK], attended)
        rows.append((attended * gate).astype(BF16))
    return jnp.concatenate(rows, axis=0)


SCALARS = pl.BlockSpec(memory_space=pltpu.SMEM)


def attend_all(out_ref, kv_ref, q_ref, base, gate, arrived):
    size = ATT_GROUP * BLOCK
    for g in range(out_ref.shape[0] // size):
        arrived(g)
        blocks = range(g * ATT_GROUP, (g + 1) * ATT_GROUP)
        out_ref[pl.ds(g * size, size), :] = attend_blocks(blocks, kv_ref, q_ref, base, gate)


def attend_kernel(
    half_ref, owner_ref, recv_hbm, q_ref, gate_ref, out_ref, next_kv_ref, next_q_ref, kv_ref, sem, next_sem, q_sem
):
    count = kv_ref.shape[0]
    n = next_q_ref.shape[0]
    first, second = half_ref[0], 1 - half_ref[0]
    copies = [
        pltpu.make_async_copy(recv_hbm.at[owner_ref[first * count + i]], kv_ref.at[i], sem.at[i]) for i in range(count)
    ]
    later = [
        pltpu.make_async_copy(recv_hbm.at[owner_ref[second * count + i]], next_kv_ref.at[i], next_sem.at[i])
        for i in range(count)
    ] + [pltpu.make_async_copy(q_ref.at[pl.ds(pl.multiple_of(second * n, n), n), :], next_q_ref, q_sem)]
    for c in copies:
        c.start()
    gate = jnp.tanh(wide_row(gate_ref))

    def arrived(g):
        for c in copies[2 * g * ATT_GROUP : 2 * (g + 1) * ATT_GROUP]:
            c.wait()
        if g == 0:
            for c in later:
                c.start()

    attend_all(out_ref, kv_ref, q_ref, pl.multiple_of(first * n, n), gate, arrived)
    for c in later:
        c.wait()


def attend_first(half, owners, received, queries, gate):
    n = queries.shape[0] // 2
    count = owners.shape[0] // 2
    return pl.pallas_call(
        attend_kernel,
        out_shape=(
            pltpu.VMEM((n, MEM_DEV), BF16),
            pltpu.VMEM((count, PLEN, 2 * MEM_DEV), BF16),
            pltpu.VMEM((n, MEM_DEV), BF16),
        ),
        in_specs=[SCALARS, SCALARS, HBM, ONCHIP, ONCHIP],
        out_specs=(ONCHIP, ONCHIP, ONCHIP),
        scratch_shapes=[
            pltpu.VMEM((count, PLEN, 2 * MEM_DEV), BF16),
            pltpu.SemaphoreType.DMA((count,)),
            pltpu.SemaphoreType.DMA((count,)),
            pltpu.SemaphoreType.DMA(()),
        ],
        compiler_params=grant(8),
        cost_estimate=pl.CostEstimate(flops=n * D * 256, transcendentals=0, bytes_accessed=2 << 20),
        name="attend_first",
    )(half, owners, *offchip(received), *onchip(queries, gate))


def attend_rest_kernel(kv_ref, q_ref, gate_ref, out_ref):
    attend_all(out_ref, kv_ref, q_ref, 0, jnp.tanh(wide_row(gate_ref)), lambda g: None)


def attend_rest(kv, queries, gate):
    n = queries.shape[0]
    return pl.pallas_call(
        attend_rest_kernel,
        out_shape=pltpu.VMEM((n, MEM_DEV), BF16),
        in_specs=[ONCHIP] * 3,
        out_specs=ONCHIP,
        compiler_params=grant(6),
        cost_estimate=pl.CostEstimate(flops=n * D * 256, transcendentals=0, bytes_accessed=2 << 20),
        name="attend_rest",
    )(*onchip(kv, queries, gate))


def finish_kernel(own_ref, peer_ref, w_own_ref, w_peer_ref, conv_ref, out_hbm, out_ref, out_sem):
    groups = out_ref.shape[0] // ATT_TILE
    span = lambda g: pl.ds(g * ATT_TILE, ATT_TILE)
    out_copies = [pltpu.make_async_copy(out_ref.at[span(g)], out_hbm.at[span(g)], out_sem.at[g]) for g in range(groups)]
    for g in range(groups):
        memory = matmul(own_ref[span(g), :], w_own_ref[...]) + matmul(peer_ref[span(g), :], w_peer_ref[...])
        out_ref[span(g), :] = (conv_ref[span(g), :].astype(F32) + memory).astype(BF16)
        out_copies[g].start()
    for c in out_copies:
        c.wait()


def finish(own, peer, w_own, w_peer, conv_sum):
    n = conv_sum.shape[0]
    return pl.pallas_call(
        finish_kernel,
        out_shape=pltpu.HBM((n, D), BF16),
        in_specs=[ONCHIP] * 5,
        out_specs=HBM,
        scratch_shapes=[pltpu.VMEM((n, D), BF16), pltpu.SemaphoreType.DMA((n // ATT_TILE,))],
        compiler_params=grant(12),
        cost_estimate=pl.CostEstimate(flops=4 * n * D * MEM_DEV, transcendentals=0, bytes_accessed=8 << 20),
        name="finish",
    )(*onchip(own, peer, w_own, w_peer, conv_sum))


def body(
    tokens,
    passage_ids,
    passage_store,
    norm_gain,
    conv_value_weight,
    conv_gate_weight,
    conv_weight,
    ln_gain,
    query_weight,
    query_gain,
    passage_gain,
    key_weight,
    value_weight,
    key_gain,
    memory_gate,
    conv_out_weight,
    memory_out_weight,
):
    owner_count = lax.axis_size("st")
    swap = [(0, 1), (1, 0)]
    me = lax.axis_index("tp").astype(jnp.int32).reshape(1)

    ids = lax.all_to_all(jnp.broadcast_to(passage_ids.T, (owner_count, *passage_ids.shape[::-1])), "st", 0, 0, tiled=True)
    peer_tokens = lax.ppermute(tokens, "tp", swap)
    peer_conv_weight = lax.ppermute(conv_out_weight, "tp", swap)
    peer_memory_weight = lax.ppermute(memory_out_weight, "tp", swap)

    kv = project_store(
        passage_store.reshape(-1, D),
        passage_gain.reshape(-1, LANES),
        key_weight,
        value_weight,
        key_gain.reshape(-1, LANES),
    ).reshape(PASS_DEV, PLEN, 2 * MEM_DEV)
    sent = fill_slots(lax.axis_index("st").astype(jnp.int32).reshape(1), ids, kv)
    received = lax.all_to_all(sent, "st", 0, 0, tiled=True)

    filtered, own_stats, queries = token_branch(
        me,
        tokens,
        peer_tokens,
        norm_gain.reshape(2, -1, LANES),
        conv_value_weight,
        conv_gate_weight,
        query_weight,
        conv_weight,
        query_gain.reshape(-1, LANES),
    )
    peer_stats = lax.ppermute(own_stats, "tp", swap)
    conv_theirs = channel_swish(1 - me, filtered, own_stats, peer_stats, ln_gain.reshape(-1, LANES))
    conv_peer = lax.ppermute(conv_theirs, "tp", swap)
    conv_mine = channel_swish(me, filtered, own_stats, peer_stats, ln_gain.reshape(-1, LANES))
    conv_sum = conv_product(conv_mine, conv_peer, conv_out_weight, peer_conv_weight)

    owners = lax.optimization_barrier((passage_ids, filtered))[0].reshape(-1) >> OWNER_SHIFT
    gate = memory_gate.reshape(-1, LANES)
    memory_theirs, next_kv, next_queries = attend_first(1 - me, owners, received, queries, gate)
    memory_peer = lax.ppermute(memory_theirs, "tp", swap)
    memory_mine = attend_rest(next_kv, next_queries, gate)
    return finish(memory_mine, memory_peer, memory_out_weight, peer_memory_weight, conv_sum)


def solution(mesh):
    return jax.shard_map(
        body,
        mesh=mesh,
        in_specs=(
            P("st", "tp"),
            P("st", None),
            P("st", None, None),
            P(),
            P(None, "tp"),
            P(None, "tp"),
            P(None, "tp"),
            P("tp"),
            P(None, "tp"),
            P("tp"),
            P(),
            P(None, "tp"),
            P(None, "tp"),
            P("tp"),
            P("tp"),
            P("tp", None),
            P("tp", None),
        ),
        out_specs=P(("st", "tp"), None),
        check_vma=False,
    )
```

```python
import jax
import jax.numpy as jnp
from jax import lax
from jax.experimental import pallas as pl
from jax.experimental.pallas import tpu as pltpu
from jax.sharding import PartitionSpec as P

D = 2048
HALF_D = 1024
C_A = 1536
C_DEV = 768
MEM_HD = 64
MEM_DEV = 256
KW = 31
SEQ_LEN = 512
BLOCK = 64
PLEN = 64
PASS_DEV = 16
OWNER_SHIFT = 4
NORM_EPS = 1e-06
LAYER_EPS = 1e-05

KV_TILE = 512
TOK_TILE = 256
OUT_TILE = 256
OUT_COLS = 512
ATT_TILE = 256
ATT_GROUP = 4
LANES = 128
CONV_ROWS = 128
NORM_ROWS = 16
HISTORY = 32

F32 = jnp.float32
BF16 = jnp.bfloat16


def matmul(a, b):
    return lax.dot_general(a, b, (((1,), (0,)), ((), ())), preferred_element_type=F32)


def matmul_t(a, b):
    return lax.dot_general(a, b, (((1,), (1,)), ((), ())), preferred_element_type=F32)


def row_norm(rows, gain):
    widened = rows.astype(F32)
    factor = lax.rsqrt(jnp.sum(widened * widened, axis=1, keepdims=True) * (1.0 / D) + NORM_EPS)
    return (widened * factor * gain).astype(BF16)


def head_norm(product, gain):
    width = product.shape[1]
    rows = lax.broadcasted_iota(jnp.int32, (width, width), 0) // MEM_HD
    cols = lax.broadcasted_iota(jnp.int32, (width, width), 1) // MEM_HD
    same_head = jnp.where(rows == cols, 1.0, 0.0).astype(BF16)
    squares = product * product
    coarse = squares.astype(BF16)
    fine = (squares - coarse.astype(F32)).astype(BF16)
    total = matmul(coarse, same_head) + matmul(fine, same_head)
    return product * lax.rsqrt(total * (1.0 / MEM_HD) + NORM_EPS) * gain


def wide_row(ref):
    values = ref[...].astype(F32)
    return jnp.concatenate([values[i : i + 1, :] for i in range(values.shape[0])], axis=1)


def kv_kernel(
    rows_hbm, gain_hbm, wk_hbm, wv_hbm, kg_hbm, out_ref,
    rows_ref, gain_ref, w_ref, kg_ref, even, odd, r_sem, w_sem
):
    chunks = rows_hbm.shape[0] // KV_TILE
    span = lambda c: pl.ds(c * KV_TILE, KV_TILE)
    row_copies = [pltpu.make_async_copy(rows_hbm.at[span(c)], rows_ref.at[span(c)], r_sem.at[c]) for c in range(chunks)]
    wk_copy = pltpu.make_async_copy(wk_hbm, w_ref.at[:, :MEM_DEV], w_sem.at[0])
    wv_copy = pltpu.make_async_copy(wv_hbm, w_ref.at[:, MEM_DEV:], w_sem.at[1])
    gain_copy = pltpu.make_async_copy(gain_hbm, gain_ref, w_sem.at[2])
    kg_copy = pltpu.make_async_copy(kg_hbm, kg_ref, w_sem.at[3])
    for c in [gain_copy, kg_copy, row_copies[0], wk_copy, wv_copy, *row_copies[1:]]:
        c.start()
    gain_copy.wait()
    kg_copy.wait()
    gain = wide_row(gain_ref)
    key_gain = wide_row(kg_ref)
    held = (even, odd)

    def normalise(c):
        for r in range(0, KV_TILE, NORM_ROWS):
            rows = rows_ref[c * KV_TILE + r : c * KV_TILE + r + NORM_ROWS, :]
            held[c % 2][r : r + NORM_ROWS, :] = row_norm(rows, gain)

    row_copies[0].wait()
    normalise(0)
    wk_copy.wait()
    wv_copy.wait()
    for c in range(chunks):
        if c + 1 < chunks:
            row_copies[c + 1].wait()
            normalise(c + 1)
        both = matmul(held[c % 2][...], w_ref[...])
        out_ref[span(c), :MEM_DEV] = head_norm(both[:, :MEM_DEV], key_gain).astype(BF16)
        out_ref[span(c), MEM_DEV:] = both[:, MEM_DEV:].astype(BF16)


def resident(shape):
    zeros = (0,) * len(shape)
    return pl.BlockSpec(shape, lambda *_: zeros, pipeline_mode=pl.Buffered(1))


HBM = pl.BlockSpec(memory_space=pl.ANY)
ONCHIP = pl.BlockSpec(memory_space=pltpu.VMEM)


def onchip(*arrays):
    return tuple(pltpu.with_memory_space_constraint(a, pltpu.VMEM) for a in arrays)


def offchip(*arrays):
    return tuple(pltpu.with_memory_space_constraint(a, pltpu.HBM) for a in arrays)


def grant(mib):
    return pltpu.CompilerParams(vmem_limit_bytes=mib << 20)


def project_store(rows, passage_gain, key_weight, value_weight, key_gain):
    n = rows.shape[0]
    return pl.pallas_call(
        kv_kernel,
        out_shape=pltpu.VMEM((n, 2 * MEM_DEV), BF16),
        in_specs=[HBM] * 5,
        out_specs=ONCHIP,
        scratch_shapes=[
            pltpu.VMEM((n, D), BF16),
            pltpu.VMEM((D // LANES, LANES), BF16),
            pltpu.VMEM((D, 2 * MEM_DEV), BF16),
            pltpu.VMEM((MEM_DEV // LANES, LANES), BF16),
            pltpu.VMEM((KV_TILE, D), BF16),
            pltpu.VMEM((KV_TILE, D), BF16),
            pltpu.SemaphoreType.DMA((n // KV_TILE,)),
            pltpu.SemaphoreType.DMA((4,)),
        ],
        compiler_params=grant(24),
        cost_estimate=pl.CostEstimate(flops=2 * n * D * 2 * MEM_DEV, transcendentals=0, bytes_accessed=8 << 20),
        name="project_store",
    )(*offchip(rows, passage_gain, key_weight, value_weight, key_gain))


def slots_kernel(ids_ref, kv_ref, out_hbm, row_ref, table, table_sem, sem):
    count = out_hbm.shape[0]
    local = ids_ref[...] ^ (lax.axis_index("st") * PASS_DEV)
    asked = jnp.where(local < PASS_DEV, local, 0)
    asked = jnp.sum(asked[:, 0, :] + asked[:, 1, :], axis=1, keepdims=True).astype(F32)
    square = jnp.concatenate([jnp.broadcast_to(asked, (count, LANES)), jnp.zeros((LANES - count, LANES), F32)], axis=0)
    row_ref[...] = square.T[:8, :].astype(jnp.int32)
    fetch = pltpu.make_async_copy(row_ref, table, table_sem)
    fetch.start()
    fetch.wait()
    copies = [pltpu.make_async_copy(kv_ref.at[table[0, s]], out_hbm.at[s], sem.at[s]) for s in range(count)]
    for c in copies:
        c.start()
    for c in copies:
        c.wait()


def fill_slots(ids, kv):
    count = ids.shape[0]
    return pl.pallas_call(
        slots_kernel,
        out_shape=pltpu.HBM((count, PLEN, 2 * MEM_DEV), BF16),
        in_specs=[ONCHIP, ONCHIP],
        out_specs=HBM,
        scratch_shapes=[
            pltpu.VMEM((8, LANES), jnp.int32),
            pltpu.SMEM((8, LANES), jnp.int32),
            pltpu.SemaphoreType.DMA(()),
            pltpu.SemaphoreType.DMA((count,)),
        ],
        compiler_params=grant(2),
        name="fill_slots",
    )(*onchip(ids, kv))


def token_kernel(
    tp_ref, own_ref, peer_ref, gain_ref, wv_ref, wg_ref, wq_ref, cw_ref, qg_ref, filt_ref, stat_ref, q_ref, xs_ref, taps_ref,
    own_n, peer_n
):
    tile = pl.program_id(0)
    me = tp_ref[0]
    own_at = pl.multiple_of(me * HALF_D, HALF_D)
    peer_at = pl.multiple_of((1 - me) * HALF_D, HALF_D)
    own_gain = wide_row(gain_ref.at[me])
    peer_gain = wide_row(gain_ref.at[1 - me])
    for r in range(0, TOK_TILE, NORM_ROWS):
        rows = slice(r, r + NORM_ROWS)
        own = own_ref[rows, :].astype(F32)
        peer = peer_ref[rows, :].astype(F32)
        total = jnp.sum(own * own + peer * peer, axis=1, keepdims=True)
        factor = lax.rsqrt(total * (1.0 / D) + NORM_EPS)
        own_n[rows, :] = (own * factor * own_gain).astype(BF16)
        peer_n[rows, :] = (peer * factor * peer_gain).astype(BF16)

    def product(w_ref):
        own_part = matmul(own_n[...], w_ref[pl.ds(own_at, HALF_D), :])
        return own_part + matmul(peer_n[...], w_ref[pl.ds(peer_at, HALF_D), :])

    q_ref[...] = head_norm(product(wq_ref), wide_row(qg_ref) * MEM_HD ** (-0.5)).astype(BF16)
    gated = (product(wv_ref) * jax.nn.sigmoid(product(wg_ref))).astype(BF16)

    @pl.when(tile % (SEQ_LEN // TOK_TILE) == 0)
    def _():
        xs_ref[:HISTORY, :] = jnp.zeros((HISTORY, C_DEV), F32)

    taps_ref[...] = cw_ref[...].astype(F32)
    xs_ref[HISTORY:, :] = gated.astype(F32)
    first = HISTORY - (KW - 1)
    for base in range(0, TOK_TILE, CONV_ROWS):
        sums = jnp.zeros((CONV_ROWS, LANES), F32)
        squares = jnp.zeros((CONV_ROWS, LANES), F32)
        for lane in range(0, C_DEV, LANES):
            lanes = slice(lane, lane + LANES)
            acc = None
            for r in range(8):
                steps = [s for s in range(first, first + KW) if s % 8 == r]
                reach = max(steps) - r + CONV_ROWS
                shifted = xs_ref[base + r : base + r + reach, lanes]
                part = None
                for s in steps:
                    term = shifted[s - r : s - r + CONV_ROWS] * taps_ref[s - first : s - first + 1, lanes]
                    part = term if part is None else part + term
                acc = part if acc is None else acc + part
            filt_ref[base : base + CONV_ROWS, lanes] = acc
            sums = sums + acc
            squares = squares + acc * acc
        stat_ref[base : base + CONV_ROWS, 0:1] = jnp.sum(sums, axis=1, keepdims=True)
        stat_ref[base : base + CONV_ROWS, 1:2] = jnp.sum(squares, axis=1, keepdims=True)
    xs_ref[:HISTORY, :] = xs_ref[TOK_TILE:, :]


def token_branch(me, own, peer, gain, wv, wg, wq, cw, qg):
    n = own.shape[0]
    tile = lambda width: pl.BlockSpec((TOK_TILE, width), lambda i, s: (i, 0))
    return pl.pallas_call(
        token_kernel,
        out_shape=(
            jax.ShapeDtypeStruct((n, C_DEV), F32),
            jax.ShapeDtypeStruct((n, 2), F32),
            jax.ShapeDtypeStruct((n, MEM_DEV), BF16),
        ),
        grid_spec=pltpu.PrefetchScalarGridSpec(
            num_scalar_prefetch=1,
            grid=(n // TOK_TILE,),
            in_specs=[
                tile(HALF_D),
                tile(HALF_D),
                resident((2, HALF_D // LANES, LANES)),
                resident((D, C_DEV)),
                resident((D, C_DEV)),
                resident((D, MEM_DEV)),
                resident((KW, C_DEV)),
                resident((MEM_DEV // LANES, LANES)),
            ],
            out_specs=(tile(C_DEV), tile(2), tile(MEM_DEV)),
            scratch_shapes=[
                pltpu.VMEM((HISTORY + TOK_TILE, C_DEV), F32),
                pltpu.VMEM((KW, C_DEV), F32),
                pltpu.VMEM((TOK_TILE, HALF_D), BF16),
                pltpu.VMEM((TOK_TILE, HALF_D), BF16),
            ],
        ),
        cost_estimate=pl.CostEstimate(flops=20 * n * D * 768, transcendentals=0, bytes_accessed=16 << 20),
        name="token_branch",
    )(me, own, peer, gain, wv, wg, wq, cw, qg)


def swish_kernel(filt_ref, own_ref, peer_ref, gain_ref, out_ref):
    stats = (own_ref[...] + peer_ref[...]) * (1.0 / C_A)
    mean = stats[:, 0:1]
    var = stats[:, 1:2] - mean * mean
    scaled = (filt_ref[...] - mean) * lax.rsqrt(var + LAYER_EPS) * wide_row(gain_ref)
    out_ref[...] = (scaled * jax.nn.sigmoid(scaled)).astype(BF16)


def channel_swish(half, filtered, own_stats, peer_stats, gain):
    n = filtered.shape[0] // 2
    steps = n // OUT_TILE
    tile = lambda width: pl.BlockSpec((OUT_TILE, width), lambda i, h: (h[0] * steps + i, 0))
    return pl.pallas_call(
        lambda half_ref, *refs: swish_kernel(*refs),
        out_shape=jax.ShapeDtypeStruct((n, C_DEV), BF16),
        grid_spec=pltpu.PrefetchScalarGridSpec(
            num_scalar_prefetch=1,
            grid=(steps,),
            in_specs=[tile(C_DEV), tile(2), tile(2), resident((C_DEV // LANES, LANES))],
            out_specs=pl.BlockSpec((OUT_TILE, C_DEV), lambda i, h: (i, 0)),
        ),
        cost_estimate=pl.CostEstimate(flops=n * D * 768, transcendentals=0, bytes_accessed=4 << 20),
        name="channel_swish",
    )(half, filtered, own_stats, peer_stats, gain)


def pair_kernel(own_ref, peer_ref, w_own_hbm, w_peer_hbm, out_ref, w_own_ref, w_peer_ref, sem):
    parts = D // OUT_COLS
    cols = lambda c: pl.ds(c * OUT_COLS, OUT_COLS)
    copies = [
        pltpu.make_async_copy(hbm.at[:, cols(c)], ref.at[:, cols(c)], sem.at[i, c])
        for c in range(parts)
        for i, (hbm, ref) in enumerate(((w_own_hbm, w_own_ref), (w_peer_hbm, w_peer_ref)))
    ]
    for c in copies:
        c.start()
    for c in range(parts):
        copies[2 * c].wait()
        copies[2 * c + 1].wait()
        own_part = matmul(own_ref[...], w_own_ref[:, cols(c)])
        out_ref[:, cols(c)] = (own_part + matmul(peer_ref[...], w_peer_ref[:, cols(c)])).astype(BF16)


def conv_product(own, peer, w_own, w_peer):
    n = own.shape[0]
    return pl.pallas_call(
        pair_kernel,
        out_shape=pltpu.HBM((n, D), BF16),
        in_specs=[ONCHIP, ONCHIP, HBM, HBM],
        out_specs=pl.BlockSpec((n, D), lambda: (0, 0)),
        scratch_shapes=[
            pltpu.VMEM((C_DEV, D), BF16),
            pltpu.VMEM((C_DEV, D), BF16),
            pltpu.SemaphoreType.DMA((2, D // OUT_COLS)),
        ],
        compiler_params=grant(16),
        cost_estimate=pl.CostEstimate(flops=4 * n * D * C_DEV, transcendentals=0, bytes_accessed=12 << 20),
        name="conv_product",
    )(*onchip(own, peer), *offchip(w_own, w_peer))


def attend_blocks(blocks, kv_ref, q_ref, base, gate):
    heads = MEM_DEV // MEM_HD
    lane_head = lax.broadcasted_iota(jnp.int32, (BLOCK, MEM_DEV), 1) // MEM_HD
    scores = []
    for b in blocks:
        q = q_ref[pl.ds(base + b * BLOCK, BLOCK), :]
        spread = jnp.concatenate([jnp.where(lane_head == h, q, jnp.zeros_like(q)) for h in range(heads)], axis=0)
        scores.append(matmul_t(spread, kv_ref[2 * b : 2 * b + 2, :, :MEM_DEV].reshape(2 * PLEN, MEM_DEV)))
    expanded = [jnp.exp(s - jnp.max(s, axis=1, keepdims=True)) for s in scores]
    weights = [(e * (1.0 / jnp.sum(e, axis=1, keepdims=True))).astype(BF16) for e in expanded]
    rows = []
    for w, b in zip(weights, blocks):
        mixed = matmul(w, kv_ref[2 * b : 2 * b + 2, :, MEM_DEV:].reshape(2 * PLEN, MEM_DEV))
        attended = mixed[:BLOCK]
        for h in range(1, heads):
            attended = jnp.where(lane_head == h, mixed[h * BLOCK : (h + 1) * BLOCK], attended)
        rows.append((attended * gate).astype(BF16))
    return jnp.concatenate(rows, axis=0)


SCALARS = pl.BlockSpec(memory_space=pltpu.SMEM)


def attend_all(out_ref, kv_ref, q_ref, base, gate, arrived):
    size = ATT_GROUP * BLOCK
    for g in range(out_ref.shape[0] // size):
        arrived(g)
        blocks = range(g * ATT_GROUP, (g + 1) * ATT_GROUP)
        out_ref[pl.ds(g * size, size), :] = attend_blocks(blocks, kv_ref, q_ref, base, gate)


def attend_kernel(
    half_ref, owner_ref, recv_hbm, q_ref, gate_ref, out_ref, next_kv_ref, next_q_ref, kv_ref, sem, next_sem, q_sem
):
    count = kv_ref.shape[0]
    n = next_q_ref.shape[0]
    first, second = half_ref[0], 1 - half_ref[0]
    copies = [
        pltpu.make_async_copy(recv_hbm.at[owner_ref[first * count + i]], kv_ref.at[i], sem.at[i]) for i in range(count)
    ]
    later = [
        pltpu.make_async_copy(recv_hbm.at[owner_ref[second * count + i]], next_kv_ref.at[i], next_sem.at[i])
        for i in range(count)
    ] + [pltpu.make_async_copy(q_ref.at[pl.ds(pl.multiple_of(second * n, n), n), :], next_q_ref, q_sem)]
    for c in copies:
        c.start()
    gate = jnp.tanh(wide_row(gate_ref))

    def arrived(g):
        for c in copies[2 * g * ATT_GROUP : 2 * (g + 1) * ATT_GROUP]:
            c.wait()
        if g == 0:
            for c in later:
                c.start()

    attend_all(out_ref, kv_ref, q_ref, pl.multiple_of(first * n, n), gate, arrived)
    for c in later:
        c.wait()


def attend_first(half, owners, received, queries, gate):
    n = queries.shape[0] // 2
    count = owners.shape[0] // 2
    return pl.pallas_call(
        attend_kernel,
        out_shape=(
            pltpu.VMEM((n, MEM_DEV), BF16),
            pltpu.VMEM((count, PLEN, 2 * MEM_DEV), BF16),
            pltpu.VMEM((n, MEM_DEV), BF16),
        ),
        in_specs=[SCALARS, SCALARS, HBM, ONCHIP, ONCHIP],
        out_specs=(ONCHIP, ONCHIP, ONCHIP),
        scratch_shapes=[
            pltpu.VMEM((count, PLEN, 2 * MEM_DEV), BF16),
            pltpu.SemaphoreType.DMA((count,)),
            pltpu.SemaphoreType.DMA((count,)),
            pltpu.SemaphoreType.DMA(()),
        ],
        compiler_params=grant(8),
        cost_estimate=pl.CostEstimate(flops=n * D * 256, transcendentals=0, bytes_accessed=2 << 20),
        name="attend_first",
    )(half, owners, *offchip(received), *onchip(queries, gate))


def attend_rest_kernel(kv_ref, q_ref, gate_ref, out_ref):
    attend_all(out_ref, kv_ref, q_ref, 0, jnp.tanh(wide_row(gate_ref)), lambda g: None)


def attend_rest(kv, queries, gate):
    n = queries.shape[0]
    return pl.pallas_call(
        attend_rest_kernel,
        out_shape=pltpu.VMEM((n, MEM_DEV), BF16),
        in_specs=[ONCHIP] * 3,
        out_specs=ONCHIP,
        compiler_params=grant(6),
        cost_estimate=pl.CostEstimate(flops=n * D * 256, transcendentals=0, bytes_accessed=2 << 20),
        name="attend_rest",
    )(*onchip(kv, queries, gate))


def finish_kernel(own_ref, peer_ref, w_own_ref, w_peer_ref, conv_ref, out_hbm, out_ref, out_sem):
    groups = out_ref.shape[0] // ATT_TILE
    span = lambda g: pl.ds(g * ATT_TILE, ATT_TILE)
    out_copies = [pltpu.make_async_copy(out_ref.at[span(g)], out_hbm.at[span(g)], out_sem.at[g]) for g in range(groups)]
    for g in range(groups):
        memory = matmul(own_ref[span(g), :], w_own_ref[...]) + matmul(peer_ref[span(g), :], w_peer_ref[...])
        out_ref[span(g), :] = (conv_ref[span(g), :].astype(F32) + memory).astype(BF16)
        out_copies[g].start()
    for c in out_copies:
        c.wait()


def finish(own, peer, w_own, w_peer, conv_sum):
    n = conv_sum.shape[0]
    return pl.pallas_call(
        finish_kernel,
        out_shape=pltpu.HBM((n, D), BF16),
        in_specs=[ONCHIP] * 5,
        out_specs=HBM,
        scratch_shapes=[pltpu.VMEM((n, D), BF16), pltpu.SemaphoreType.DMA((n // ATT_TILE,))],
        compiler_params=grant(12),
        cost_estimate=pl.CostEstimate(flops=4 * n * D * MEM_DEV, transcendentals=0, bytes_accessed=8 << 20),
        name="finish",
    )(*onchip(own, peer, w_own, w_peer, conv_sum))


def body(
    tokens,
    passage_ids,
    passage_store,
    norm_gain,
    conv_value_weight,
    conv_gate_weight,
    conv_weight,
    ln_gain,
    query_weight,
    query_gain,
    passage_gain,
    key_weight,
    value_weight,
    key_gain,
    memory_gate,
    conv_out_weight,
    memory_out_weight,
):
    owner_count = lax.axis_size("st")
    swap = [(0, 1), (1, 0)]
    me = lax.axis_index("tp").astype(jnp.int32).reshape(1)

    ids = lax.all_to_all(jnp.broadcast_to(passage_ids.T, (owner_count, *passage_ids.shape[::-1])), "st", 0, 0, tiled=True)
    peer_tokens = lax.ppermute(tokens, "tp", swap)
    peer_conv_weight = lax.ppermute(conv_out_weight, "tp", swap)
    peer_memory_weight = lax.ppermute(memory_out_weight, "tp", swap)

    kv = project_store(
        passage_store.reshape(-1, D),
        passage_gain.reshape(-1, LANES),
        key_weight,
        value_weight,
        key_gain.reshape(-1, LANES),
    ).reshape(PASS_DEV, PLEN, 2 * MEM_DEV)
    sent = fill_slots(ids, kv)
    received = lax.all_to_all(sent, "st", 0, 0, tiled=True)

    filtered, own_stats, queries = token_branch(
        me,
        tokens,
        peer_tokens,
        norm_gain.reshape(2, -1, LANES),
        conv_value_weight,
        conv_gate_weight,
        query_weight,
        conv_weight,
        query_gain.reshape(-1, LANES),
    )
    peer_stats = lax.ppermute(own_stats, "tp", swap)
    conv_theirs = channel_swish(1 - me, filtered, own_stats, peer_stats, ln_gain.reshape(-1, LANES))
    conv_peer = lax.ppermute(conv_theirs, "tp", swap)
    conv_mine = channel_swish(me, filtered, own_stats, peer_stats, ln_gain.reshape(-1, LANES))
    conv_sum = conv_product(conv_mine, conv_peer, conv_out_weight, peer_conv_weight)

    owners = lax.optimization_barrier((passage_ids, filtered))[0].reshape(-1) >> OWNER_SHIFT
    gate = memory_gate.reshape(-1, LANES)
    memory_theirs, next_kv, next_queries = attend_first(1 - me, owners, received, queries, gate)
    memory_peer = lax.ppermute(memory_theirs, "tp", swap)
    memory_mine = attend_rest(next_kv, next_queries, gate)
    return finish(memory_mine, memory_peer, memory_out_weight, peer_memory_weight, conv_sum)


def solution(mesh):
    return jax.shard_map(
        body,
        mesh=mesh,
        in_specs=(
            P("st", "tp"),
            P("st", None),
            P("st", None, None),
            P(),
            P(None, "tp"),
            P(None, "tp"),
            P(None, "tp"),
            P("tp"),
            P(None, "tp"),
            P("tp"),
            P(),
            P(None, "tp"),
            P(None, "tp"),
            P("tp"),
            P("tp"),
            P("tp", None),
            P("tp", None),
        ),
        out_specs=P(("st", "tp"), None),
        check_vma=False,
    )
```

```python
import jax
import jax.numpy as jnp
from jax import lax
from jax.experimental import pallas as pl
from jax.experimental.pallas import tpu as pltpu
from jax.sharding import PartitionSpec as P

D = 2048
HALF_D = 1024
C_A = 1536
C_DEV = 768
MEM_HD = 64
MEM_DEV = 256
KW = 31
SEQ_LEN = 512
BLOCK = 64
PLEN = 64
PASS_DEV = 16
OWNER_SHIFT = 4
NORM_EPS = 1e-06
LAYER_EPS = 1e-05

KV_TILE = 512
TOK_TILE = 256
OUT_TILE = 256
OUT_COLS = 512
ATT_TILE = 256
ATT_GROUP = 8
LANES = 128
CONV_ROWS = 128
NORM_ROWS = 16
HISTORY = 32

F32 = jnp.float32
BF16 = jnp.bfloat16


def matmul(a, b):
    return lax.dot_general(a, b, (((1,), (0,)), ((), ())), preferred_element_type=F32)


def matmul_t(a, b):
    return lax.dot_general(a, b, (((1,), (1,)), ((), ())), preferred_element_type=F32)


def row_norm(rows, gain):
    widened = rows.astype(F32)
    factor = lax.rsqrt(jnp.sum(widened * widened, axis=1, keepdims=True) * (1.0 / D) + NORM_EPS)
    return (widened * factor * gain).astype(BF16)


def head_norm(product, gain):
    width = product.shape[1]
    rows = lax.broadcasted_iota(jnp.int32, (width, width), 0) // MEM_HD
    cols = lax.broadcasted_iota(jnp.int32, (width, width), 1) // MEM_HD
    same_head = jnp.where(rows == cols, 1.0, 0.0).astype(BF16)
    squares = product * product
    coarse = squares.astype(BF16)
    fine = (squares - coarse.astype(F32)).astype(BF16)
    total = matmul(coarse, same_head) + matmul(fine, same_head)
    return product * lax.rsqrt(total * (1.0 / MEM_HD) + NORM_EPS) * gain


def wide_row(ref):
    values = ref[...].astype(F32)
    return jnp.concatenate([values[i : i + 1, :] for i in range(values.shape[0])], axis=1)


def kv_kernel(
    rows_hbm, gain_hbm, wk_hbm, wv_hbm, kg_hbm, out_ref,
    rows_ref, gain_ref, w_ref, kg_ref, even, odd, r_sem, w_sem
):
    chunks = rows_hbm.shape[0] // KV_TILE
    span = lambda c: pl.ds(c * KV_TILE, KV_TILE)
    row_copies = [pltpu.make_async_copy(rows_hbm.at[span(c)], rows_ref.at[span(c)], r_sem.at[c]) for c in range(chunks)]
    wk_copy = pltpu.make_async_copy(wk_hbm, w_ref.at[:, :MEM_DEV], w_sem.at[0])
    wv_copy = pltpu.make_async_copy(wv_hbm, w_ref.at[:, MEM_DEV:], w_sem.at[1])
    gain_copy = pltpu.make_async_copy(gain_hbm, gain_ref, w_sem.at[2])
    kg_copy = pltpu.make_async_copy(kg_hbm, kg_ref, w_sem.at[3])
    for c in [gain_copy, kg_copy, row_copies[0], wk_copy, wv_copy, *row_copies[1:]]:
        c.start()
    gain_copy.wait()
    kg_copy.wait()
    gain = wide_row(gain_ref)
    key_gain = wide_row(kg_ref)
    held = (even, odd)

    def normalise(c):
        for r in range(0, KV_TILE, NORM_ROWS):
            rows = rows_ref[c * KV_TILE + r : c * KV_TILE + r + NORM_ROWS, :]
            held[c % 2][r : r + NORM_ROWS, :] = row_norm(rows, gain)

    row_copies[0].wait()
    normalise(0)
    wk_copy.wait()
    wv_copy.wait()
    for c in range(chunks):
        if c + 1 < chunks:
            row_copies[c + 1].wait()
            normalise(c + 1)
        both = matmul(held[c % 2][...], w_ref[...])
        out_ref[span(c), :MEM_DEV] = head_norm(both[:, :MEM_DEV], key_gain).astype(BF16)
        out_ref[span(c), MEM_DEV:] = both[:, MEM_DEV:].astype(BF16)


def resident(shape):
    zeros = (0,) * len(shape)
    return pl.BlockSpec(shape, lambda *_: zeros, pipeline_mode=pl.Buffered(1))


HBM = pl.BlockSpec(memory_space=pl.ANY)
ONCHIP = pl.BlockSpec(memory_space=pltpu.VMEM)


def onchip(*arrays):
    return tuple(pltpu.with_memory_space_constraint(a, pltpu.VMEM) for a in arrays)


def offchip(*arrays):
    return tuple(pltpu.with_memory_space_constraint(a, pltpu.HBM) for a in arrays)


def grant(mib):
    return pltpu.CompilerParams(vmem_limit_bytes=mib << 20)


def project_store(rows, passage_gain, key_weight, value_weight, key_gain):
    n = rows.shape[0]
    return pl.pallas_call(
        kv_kernel,
        out_shape=pltpu.VMEM((n, 2 * MEM_DEV), BF16),
        in_specs=[HBM] * 5,
        out_specs=ONCHIP,
        scratch_shapes=[
            pltpu.VMEM((n, D), BF16),
            pltpu.VMEM((D // LANES, LANES), BF16),
            pltpu.VMEM((D, 2 * MEM_DEV), BF16),
            pltpu.VMEM((MEM_DEV // LANES, LANES), BF16),
            pltpu.VMEM((KV_TILE, D), BF16),
            pltpu.VMEM((KV_TILE, D), BF16),
            pltpu.SemaphoreType.DMA((n // KV_TILE,)),
            pltpu.SemaphoreType.DMA((4,)),
        ],
        compiler_params=grant(24),
        cost_estimate=pl.CostEstimate(flops=2 * n * D * 2 * MEM_DEV, transcendentals=0, bytes_accessed=8 << 20),
        name="project_store",
    )(*offchip(rows, passage_gain, key_weight, value_weight, key_gain))


def slots_kernel(ids_ref, kv_ref, out_hbm, row_ref, sem):
    count = out_hbm.shape[0]
    local = ids_ref[...] ^ (lax.axis_index("st") * PASS_DEV)
    asked = jnp.where(local < PASS_DEV, local, 0)
    asked = jnp.sum(asked[:, 0, :] + asked[:, 1, :], axis=1, keepdims=True).astype(F32)
    square = jnp.concatenate([jnp.broadcast_to(asked, (count, LANES)), jnp.zeros((LANES - count, LANES), F32)], axis=0)
    row_ref[...] = square.T[:8, :].astype(jnp.int32)
    copies = [pltpu.make_async_copy(kv_ref.at[row_ref[0, s]], out_hbm.at[s], sem.at[s]) for s in range(count)]
    for c in copies:
        c.start()
    for c in copies:
        c.wait()


def fill_slots(ids, kv):
    count = ids.shape[0]
    return pl.pallas_call(
        slots_kernel,
        out_shape=pltpu.HBM((count, PLEN, 2 * MEM_DEV), BF16),
        in_specs=[ONCHIP, ONCHIP],
        out_specs=HBM,
        scratch_shapes=[
            pltpu.VMEM((8, LANES), jnp.int32),
            pltpu.SemaphoreType.DMA((count,)),
        ],
        compiler_params=grant(2),
        name="fill_slots",
    )(*onchip(ids, kv))


def token_kernel(
    tp_ref, own_ref, peer_ref, gain_ref, wv_ref, wg_ref, wq_ref, cw_ref, qg_ref, filt_ref, stat_ref, q_ref, xs_ref, taps_ref,
    own_n, peer_n
):
    tile = pl.program_id(0)
    me = tp_ref[0]
    own_at = pl.multiple_of(me * HALF_D, HALF_D)
    peer_at = pl.multiple_of((1 - me) * HALF_D, HALF_D)
    own_gain = wide_row(gain_ref.at[me])
    peer_gain = wide_row(gain_ref.at[1 - me])
    for r in range(0, TOK_TILE, NORM_ROWS):
        rows = slice(r, r + NORM_ROWS)
        own = own_ref[rows, :].astype(F32)
        peer = peer_ref[rows, :].astype(F32)
        total = jnp.sum(own * own + peer * peer, axis=1, keepdims=True)
        factor = lax.rsqrt(total * (1.0 / D) + NORM_EPS)
        own_n[rows, :] = (own * factor * own_gain).astype(BF16)
        peer_n[rows, :] = (peer * factor * peer_gain).astype(BF16)

    def product(w_ref):
        own_part = matmul(own_n[...], w_ref[pl.ds(own_at, HALF_D), :])
        return own_part + matmul(peer_n[...], w_ref[pl.ds(peer_at, HALF_D), :])

    q_ref[...] = head_norm(product(wq_ref), wide_row(qg_ref) * MEM_HD ** (-0.5)).astype(BF16)
    gated = (product(wv_ref) * jax.nn.sigmoid(product(wg_ref))).astype(BF16)

    @pl.when(tile % (SEQ_LEN // TOK_TILE) == 0)
    def _():
        xs_ref[:HISTORY, :] = jnp.zeros((HISTORY, C_DEV), F32)

    taps_ref[...] = cw_ref[...].astype(F32)
    xs_ref[HISTORY:, :] = gated.astype(F32)
    first = HISTORY - (KW - 1)
    for base in range(0, TOK_TILE, CONV_ROWS):
        sums = jnp.zeros((CONV_ROWS, LANES), F32)
        squares = jnp.zeros((CONV_ROWS, LANES), F32)
        for lane in range(0, C_DEV, LANES):
            lanes = slice(lane, lane + LANES)
            acc = None
            for r in range(8):
                steps = [s for s in range(first, first + KW) if s % 8 == r]
                reach = max(steps) - r + CONV_ROWS
                shifted = xs_ref[base + r : base + r + reach, lanes]
                part = None
                for s in steps:
                    term = shifted[s - r : s - r + CONV_ROWS] * taps_ref[s - first : s - first + 1, lanes]
                    part = term if part is None else part + term
                acc = part if acc is None else acc + part
            filt_ref[base : base + CONV_ROWS, lanes] = acc
            sums = sums + acc
            squares = squares + acc * acc
        stat_ref[base : base + CONV_ROWS, 0:1] = jnp.sum(sums, axis=1, keepdims=True)
        stat_ref[base : base + CONV_ROWS, 1:2] = jnp.sum(squares, axis=1, keepdims=True)
    xs_ref[:HISTORY, :] = xs_ref[TOK_TILE:, :]


def token_branch(me, own, peer, gain, wv, wg, wq, cw, qg):
    n = own.shape[0]
    tile = lambda width: pl.BlockSpec((TOK_TILE, width), lambda i, s: (i, 0))
    return pl.pallas_call(
        token_kernel,
        out_shape=(
            jax.ShapeDtypeStruct((n, C_DEV), F32),
            jax.ShapeDtypeStruct((n, 2), F32),
            jax.ShapeDtypeStruct((n, MEM_DEV), BF16),
        ),
        grid_spec=pltpu.PrefetchScalarGridSpec(
            num_scalar_prefetch=1,
            grid=(n // TOK_TILE,),
            in_specs=[
                tile(HALF_D),
                tile(HALF_D),
                resident((2, HALF_D // LANES, LANES)),
                resident((D, C_DEV)),
                resident((D, C_DEV)),
                resident((D, MEM_DEV)),
                resident((KW, C_DEV)),
                resident((MEM_DEV // LANES, LANES)),
            ],
            out_specs=(tile(C_DEV), tile(2), tile(MEM_DEV)),
            scratch_shapes=[
                pltpu.VMEM((HISTORY + TOK_TILE, C_DEV), F32),
                pltpu.VMEM((KW, C_DEV), F32),
                pltpu.VMEM((TOK_TILE, HALF_D), BF16),
                pltpu.VMEM((TOK_TILE, HALF_D), BF16),
            ],
        ),
        cost_estimate=pl.CostEstimate(flops=20 * n * D * 768, transcendentals=0, bytes_accessed=16 << 20),
        name="token_branch",
    )(me, own, peer, gain, wv, wg, wq, cw, qg)


def swish_kernel(filt_ref, own_ref, peer_ref, gain_ref, out_ref):
    stats = (own_ref[...] + peer_ref[...]) * (1.0 / C_A)
    mean = stats[:, 0:1]
    var = stats[:, 1:2] - mean * mean
    scaled = (filt_ref[...] - mean) * lax.rsqrt(var + LAYER_EPS) * wide_row(gain_ref)
    out_ref[...] = (scaled * jax.nn.sigmoid(scaled)).astype(BF16)


def channel_swish(half, filtered, own_stats, peer_stats, gain):
    n = filtered.shape[0] // 2
    steps = n // OUT_TILE
    tile = lambda width: pl.BlockSpec((OUT_TILE, width), lambda i, h: (h[0] * steps + i, 0))
    return pl.pallas_call(
        lambda half_ref, *refs: swish_kernel(*refs),
        out_shape=jax.ShapeDtypeStruct((n, C_DEV), BF16),
        grid_spec=pltpu.PrefetchScalarGridSpec(
            num_scalar_prefetch=1,
            grid=(steps,),
            in_specs=[tile(C_DEV), tile(2), tile(2), resident((C_DEV // LANES, LANES))],
            out_specs=pl.BlockSpec((OUT_TILE, C_DEV), lambda i, h: (i, 0)),
        ),
        cost_estimate=pl.CostEstimate(flops=n * D * 768, transcendentals=0, bytes_accessed=4 << 20),
        name="channel_swish",
    )(half, filtered, own_stats, peer_stats, gain)


def pair_kernel(own_ref, peer_ref, w_own_hbm, w_peer_hbm, out_ref, w_own_ref, w_peer_ref, sem):
    parts = D // OUT_COLS
    cols = lambda c: pl.ds(c * OUT_COLS, OUT_COLS)
    copies = [
        pltpu.make_async_copy(hbm.at[:, cols(c)], ref.at[:, cols(c)], sem.at[i, c])
        for c in range(parts)
        for i, (hbm, ref) in enumerate(((w_own_hbm, w_own_ref), (w_peer_hbm, w_peer_ref)))
    ]
    for c in copies:
        c.start()
    for c in range(parts):
        copies[2 * c].wait()
        copies[2 * c + 1].wait()
        own_part = matmul(own_ref[...], w_own_ref[:, cols(c)])
        out_ref[:, cols(c)] = (own_part + matmul(peer_ref[...], w_peer_ref[:, cols(c)])).astype(BF16)


def conv_product(own, peer, w_own, w_peer):
    n = own.shape[0]
    return pl.pallas_call(
        pair_kernel,
        out_shape=pltpu.HBM((n, D), BF16),
        in_specs=[ONCHIP, ONCHIP, HBM, HBM],
        out_specs=pl.BlockSpec((n, D), lambda: (0, 0)),
        scratch_shapes=[
            pltpu.VMEM((C_DEV, D), BF16),
            pltpu.VMEM((C_DEV, D), BF16),
            pltpu.SemaphoreType.DMA((2, D // OUT_COLS)),
        ],
        compiler_params=grant(16),
        cost_estimate=pl.CostEstimate(flops=4 * n * D * C_DEV, transcendentals=0, bytes_accessed=12 << 20),
        name="conv_product",
    )(*onchip(own, peer), *offchip(w_own, w_peer))


def attend_blocks(blocks, kv_ref, q_ref, base, gate):
    heads = MEM_DEV // MEM_HD
    lane_head = lax.broadcasted_iota(jnp.int32, (BLOCK, MEM_DEV), 1) // MEM_HD
    scores = []
    for b in blocks:
        q = q_ref[pl.ds(base + b * BLOCK, BLOCK), :]
        spread = jnp.concatenate([jnp.where(lane_head == h, q, jnp.zeros_like(q)) for h in range(heads)], axis=0)
        scores.append(matmul_t(spread, kv_ref[2 * b : 2 * b + 2, :, :MEM_DEV].reshape(2 * PLEN, MEM_DEV)))
    expanded = [jnp.exp(s - jnp.max(s, axis=1, keepdims=True)) for s in scores]
    weights = [(e * (1.0 / jnp.sum(e, axis=1, keepdims=True))).astype(BF16) for e in expanded]
    rows = []
    for w, b in zip(weights, blocks):
        mixed = matmul(w, kv_ref[2 * b : 2 * b + 2, :, MEM_DEV:].reshape(2 * PLEN, MEM_DEV))
        attended = mixed[:BLOCK]
        for h in range(1, heads):
            attended = jnp.where(lane_head == h, mixed[h * BLOCK : (h + 1) * BLOCK], attended)
        rows.append((attended * gate).astype(BF16))
    return jnp.concatenate(rows, axis=0)


def attend_all(out_ref, kv_ref, q_ref, base, gate, arrived):
    size = ATT_GROUP * BLOCK
    for g in range(out_ref.shape[0] // size):
        arrived(g)
        blocks = range(g * ATT_GROUP, (g + 1) * ATT_GROUP)
        out_ref[pl.ds(g * size, size), :] = attend_blocks(blocks, kv_ref, q_ref, base, gate)


def attend_kernel(
    owner_ref, recv_hbm, q_ref, gate_ref, out_ref, next_kv_ref, next_q_ref, kv_ref, sem, next_sem, q_sem
):
    count = kv_ref.shape[0]
    n = next_q_ref.shape[0]
    second = lax.axis_index("tp")
    first = 1 - second
    low, high = ([owner_ref[0, h * count + i] for i in range(count)] for h in range(2))
    owners = [jnp.where(first == 0, a, b) for a, b in zip(low, high)]
    others = [jnp.where(first == 0, b, a) for a, b in zip(low, high)]
    copies = [pltpu.make_async_copy(recv_hbm.at[owners[i]], kv_ref.at[i], sem.at[i]) for i in range(count)]
    later = [
        pltpu.make_async_copy(recv_hbm.at[others[i]], next_kv_ref.at[i], next_sem.at[i])
        for i in range(count)
    ] + [pltpu.make_async_copy(q_ref.at[pl.ds(pl.multiple_of(second * n, n), n), :], next_q_ref, q_sem)]
    for c in copies:
        c.start()
    gate = jnp.tanh(wide_row(gate_ref))

    def arrived(g):
        for c in copies[2 * g * ATT_GROUP : 2 * (g + 1) * ATT_GROUP]:
            c.wait()
        if g == 0:
            for c in later:
                c.start()

    attend_all(out_ref, kv_ref, q_ref, pl.multiple_of(first * n, n), gate, arrived)
    for c in later:
        c.wait()


def attend_first(owners, received, queries, gate):
    n = queries.shape[0] // 2
    count = owners.shape[1] // 2
    return pl.pallas_call(
        attend_kernel,
        out_shape=(
            pltpu.VMEM((n, MEM_DEV), BF16),
            pltpu.VMEM((count, PLEN, 2 * MEM_DEV), BF16),
            pltpu.VMEM((n, MEM_DEV), BF16),
        ),
        in_specs=[ONCHIP, HBM, ONCHIP, ONCHIP],
        out_specs=(ONCHIP, ONCHIP, ONCHIP),
        scratch_shapes=[
            pltpu.VMEM((count, PLEN, 2 * MEM_DEV), BF16),
            pltpu.SemaphoreType.DMA((count,)),
            pltpu.SemaphoreType.DMA((count,)),
            pltpu.SemaphoreType.DMA(()),
        ],
        compiler_params=grant(8),
        cost_estimate=pl.CostEstimate(flops=n * D * 256, transcendentals=0, bytes_accessed=2 << 20),
        name="attend_first",
    )(*onchip(owners), *offchip(received), *onchip(queries, gate))


def attend_rest_kernel(kv_ref, q_ref, gate_ref, out_ref):
    attend_all(out_ref, kv_ref, q_ref, 0, jnp.tanh(wide_row(gate_ref)), lambda g: None)


def attend_rest(kv, queries, gate):
    n = queries.shape[0]
    return pl.pallas_call(
        attend_rest_kernel,
        out_shape=pltpu.VMEM((n, MEM_DEV), BF16),
        in_specs=[ONCHIP] * 3,
        out_specs=ONCHIP,
        compiler_params=grant(6),
        cost_estimate=pl.CostEstimate(flops=n * D * 256, transcendentals=0, bytes_accessed=2 << 20),
        name="attend_rest",
    )(*onchip(kv, queries, gate))


def finish_kernel(own_ref, peer_ref, w_own_ref, w_peer_ref, conv_ref, out_hbm, out_ref, out_sem):
    groups = out_ref.shape[0] // ATT_TILE
    span = lambda g: pl.ds(g * ATT_TILE, ATT_TILE)
    out_copies = [pltpu.make_async_copy(out_ref.at[span(g)], out_hbm.at[span(g)], out_sem.at[g]) for g in range(groups)]
    for g in range(groups):
        memory = matmul(own_ref[span(g), :], w_own_ref[...]) + matmul(peer_ref[span(g), :], w_peer_ref[...])
        out_ref[span(g), :] = (conv_ref[span(g), :].astype(F32) + memory).astype(BF16)
        out_copies[g].start()
    for c in out_copies:
        c.wait()


def finish(own, peer, w_own, w_peer, conv_sum):
    n = conv_sum.shape[0]
    return pl.pallas_call(
        finish_kernel,
        out_shape=pltpu.HBM((n, D), BF16),
        in_specs=[ONCHIP] * 5,
        out_specs=HBM,
        scratch_shapes=[pltpu.VMEM((n, D), BF16), pltpu.SemaphoreType.DMA((n // ATT_TILE,))],
        compiler_params=grant(12),
        cost_estimate=pl.CostEstimate(flops=4 * n * D * MEM_DEV, transcendentals=0, bytes_accessed=8 << 20),
        name="finish",
    )(*onchip(own, peer, w_own, w_peer, conv_sum))


def body(
    tokens,
    passage_ids,
    passage_store,
    norm_gain,
    conv_value_weight,
    conv_gate_weight,
    conv_weight,
    ln_gain,
    query_weight,
    query_gain,
    passage_gain,
    key_weight,
    value_weight,
    key_gain,
    memory_gate,
    conv_out_weight,
    memory_out_weight,
):
    owner_count = lax.axis_size("st")
    swap = [(0, 1), (1, 0)]
    me = lax.axis_index("tp").astype(jnp.int32).reshape(1)

    ids = lax.all_to_all(jnp.broadcast_to(passage_ids.T, (owner_count, *passage_ids.shape[::-1])), "st", 0, 0, tiled=True)
    peer_tokens = lax.ppermute(tokens, "tp", swap)
    peer_conv_weight = lax.ppermute(conv_out_weight, "tp", swap)
    peer_memory_weight = lax.ppermute(memory_out_weight, "tp", swap)

    kv = project_store(
        passage_store.reshape(-1, D),
        passage_gain.reshape(-1, LANES),
        key_weight,
        value_weight,
        key_gain.reshape(-1, LANES),
    ).reshape(PASS_DEV, PLEN, 2 * MEM_DEV)
    sent = fill_slots(ids, kv)
    received = lax.all_to_all(sent, "st", 0, 0, tiled=True)

    filtered, own_stats, queries = token_branch(
        me,
        tokens,
        peer_tokens,
        norm_gain.reshape(2, -1, LANES),
        conv_value_weight,
        conv_gate_weight,
        query_weight,
        conv_weight,
        query_gain.reshape(-1, LANES),
    )
    peer_stats = lax.ppermute(own_stats, "tp", swap)
    conv_theirs = channel_swish(1 - me, filtered, own_stats, peer_stats, ln_gain.reshape(-1, LANES))
    conv_peer = lax.ppermute(conv_theirs, "tp", swap)
    conv_mine = channel_swish(me, filtered, own_stats, peer_stats, ln_gain.reshape(-1, LANES))
    conv_sum = conv_product(conv_mine, conv_peer, conv_out_weight, peer_conv_weight)

    owners = lax.optimization_barrier((passage_ids, filtered))[0].reshape(1, -1) >> OWNER_SHIFT
    gate = memory_gate.reshape(-1, LANES)
    memory_theirs, next_kv, next_queries = attend_first(owners, received, queries, gate)
    memory_peer = lax.ppermute(memory_theirs, "tp", swap)
    memory_mine = attend_rest(next_kv, next_queries, gate)
    return finish(memory_mine, memory_peer, memory_out_weight, peer_memory_weight, conv_sum)


def solution(mesh):
    return jax.shard_map(
        body,
        mesh=mesh,
        in_specs=(
            P("st", "tp"),
            P("st", None),
            P("st", None, None),
            P(),
            P(None, "tp"),
            P(None, "tp"),
            P(None, "tp"),
            P("tp"),
            P(None, "tp"),
            P("tp"),
            P(),
            P(None, "tp"),
            P(None, "tp"),
            P("tp"),
            P("tp"),
            P("tp", None),
            P("tp", None),
        ),
        out_specs=P(("st", "tp"), None),
        check_vma=False,
    )
```

```python
import jax
import jax.numpy as jnp
from jax import lax
from jax.experimental import pallas as pl
from jax.experimental.pallas import tpu as pltpu
from jax.sharding import PartitionSpec as P

D = 2048
HALF_D = 1024
C_A = 1536
C_DEV = 768
MEM_HD = 64
MEM_DEV = 256
KW = 31
SEQ_LEN = 512
BLOCK = 64
PLEN = 64
PASS_DEV = 16
OWNER_SHIFT = 4
NORM_EPS = 1e-06
LAYER_EPS = 1e-05

KV_TILE = 512
COPY_ROWS = 256
TOK_TILE = 256
OUT_TILE = 256
OUT_COLS = 512
ATT_TILE = 256
ATT_GROUP = 8
LANES = 128
CONV_ROWS = 128
NORM_ROWS = 16
HISTORY = 32

F32 = jnp.float32
BF16 = jnp.bfloat16


def matmul(a, b):
    return lax.dot_general(a, b, (((1,), (0,)), ((), ())), preferred_element_type=F32)


def matmul_t(a, b):
    return lax.dot_general(a, b, (((1,), (1,)), ((), ())), preferred_element_type=F32)


def row_norm(rows, gain):
    widened = rows.astype(F32)
    factor = lax.rsqrt(jnp.sum(widened * widened, axis=1, keepdims=True) * (1.0 / D) + NORM_EPS)
    return (widened * factor * gain).astype(BF16)


def head_norm(product, gain):
    width = product.shape[1]
    rows = lax.broadcasted_iota(jnp.int32, (width, width), 0) // MEM_HD
    cols = lax.broadcasted_iota(jnp.int32, (width, width), 1) // MEM_HD
    same_head = jnp.where(rows == cols, 1.0, 0.0).astype(BF16)
    squares = product * product
    coarse = squares.astype(BF16)
    fine = (squares - coarse.astype(F32)).astype(BF16)
    total = matmul(coarse, same_head) + matmul(fine, same_head)
    return product * lax.rsqrt(total * (1.0 / MEM_HD) + NORM_EPS) * gain


def wide_row(ref):
    values = ref[...].astype(F32)
    return jnp.concatenate([values[i : i + 1, :] for i in range(values.shape[0])], axis=1)


def kv_kernel(
    rows_hbm, gain_hbm, wk_hbm, wv_hbm, kg_hbm, out_ref,
    rows_ref, gain_ref, w_ref, kg_ref, even, odd, r_sem, w_sem
):
    chunks = rows_hbm.shape[0] // KV_TILE
    span = lambda c: pl.ds(c * KV_TILE, KV_TILE)
    pieces = KV_TILE // COPY_ROWS
    part = lambda p: pl.ds(p * COPY_ROWS, COPY_ROWS)
    row_copies = [
        pltpu.make_async_copy(rows_hbm.at[part(p)], rows_ref.at[part(p)], r_sem.at[p]) for p in range(chunks * pieces)
    ]
    wk_copy = pltpu.make_async_copy(wk_hbm, w_ref.at[:, :MEM_DEV], w_sem.at[0])
    wv_copy = pltpu.make_async_copy(wv_hbm, w_ref.at[:, MEM_DEV:], w_sem.at[1])
    gain_copy = pltpu.make_async_copy(gain_hbm, gain_ref, w_sem.at[2])
    kg_copy = pltpu.make_async_copy(kg_hbm, kg_ref, w_sem.at[3])
    for c in [gain_copy, kg_copy, *row_copies[:pieces], wk_copy, wv_copy, *row_copies[pieces:]]:
        c.start()
    gain_copy.wait()
    kg_copy.wait()
    gain = wide_row(gain_ref)
    key_gain = wide_row(kg_ref)
    held = (even, odd)

    def normalise(c):
        for p in range(pieces):
            row_copies[c * pieces + p].wait()
            for r in range(p * COPY_ROWS, (p + 1) * COPY_ROWS, NORM_ROWS):
                rows = rows_ref[c * KV_TILE + r : c * KV_TILE + r + NORM_ROWS, :]
                held[c % 2][r : r + NORM_ROWS, :] = row_norm(rows, gain)

    normalise(0)
    wk_copy.wait()
    wv_copy.wait()
    for c in range(chunks):
        if c + 1 < chunks:
            normalise(c + 1)
        both = matmul(held[c % 2][...], w_ref[...])
        out_ref[span(c), :MEM_DEV] = head_norm(both[:, :MEM_DEV], key_gain).astype(BF16)
        out_ref[span(c), MEM_DEV:] = both[:, MEM_DEV:].astype(BF16)


def resident(shape):
    zeros = (0,) * len(shape)
    return pl.BlockSpec(shape, lambda *_: zeros, pipeline_mode=pl.Buffered(1))


HBM = pl.BlockSpec(memory_space=pl.ANY)
ONCHIP = pl.BlockSpec(memory_space=pltpu.VMEM)


def onchip(*arrays):
    return tuple(pltpu.with_memory_space_constraint(a, pltpu.VMEM) for a in arrays)


def offchip(*arrays):
    return tuple(pltpu.with_memory_space_constraint(a, pltpu.HBM) for a in arrays)


def grant(mib):
    return pltpu.CompilerParams(vmem_limit_bytes=mib << 20)


def project_store(rows, passage_gain, key_weight, value_weight, key_gain):
    n = rows.shape[0]
    return pl.pallas_call(
        kv_kernel,
        out_shape=pltpu.VMEM((n, 2 * MEM_DEV), BF16),
        in_specs=[HBM] * 5,
        out_specs=ONCHIP,
        scratch_shapes=[
            pltpu.VMEM((n, D), BF16),
            pltpu.VMEM((D // LANES, LANES), BF16),
            pltpu.VMEM((D, 2 * MEM_DEV), BF16),
            pltpu.VMEM((MEM_DEV // LANES, LANES), BF16),
            pltpu.VMEM((KV_TILE, D), BF16),
            pltpu.VMEM((KV_TILE, D), BF16),
            pltpu.SemaphoreType.DMA((n // COPY_ROWS,)),
            pltpu.SemaphoreType.DMA((4,)),
        ],
        compiler_params=grant(24),
        cost_estimate=pl.CostEstimate(flops=2 * n * D * 2 * MEM_DEV, transcendentals=0, bytes_accessed=8 << 20),
        name="project_store",
    )(*offchip(rows, passage_gain, key_weight, value_weight, key_gain))


def slots_kernel(ids_ref, kv_ref, out_hbm, row_ref, sem):
    count = out_hbm.shape[0]
    local = ids_ref[...] ^ (lax.axis_index("st") * PASS_DEV)
    asked = jnp.where(local < PASS_DEV, local, 0)
    asked = jnp.sum(asked[:, 0, :] + asked[:, 1, :], axis=1, keepdims=True).astype(F32)
    square = jnp.concatenate([jnp.broadcast_to(asked, (count, LANES)), jnp.zeros((LANES - count, LANES), F32)], axis=0)
    row_ref[...] = square.T[:8, :].astype(jnp.int32)
    copies = [pltpu.make_async_copy(kv_ref.at[row_ref[0, s]], out_hbm.at[s], sem.at[s]) for s in range(count)]
    for c in copies:
        c.start()
    for c in copies:
        c.wait()


def fill_slots(ids, kv):
    count = ids.shape[0]
    return pl.pallas_call(
        slots_kernel,
        out_shape=pltpu.HBM((count, PLEN, 2 * MEM_DEV), BF16),
        in_specs=[ONCHIP, ONCHIP],
        out_specs=HBM,
        scratch_shapes=[
            pltpu.VMEM((8, LANES), jnp.int32),
            pltpu.SemaphoreType.DMA((count,)),
        ],
        compiler_params=grant(2),
        name="fill_slots",
    )(*onchip(ids, kv))


def token_kernel(
    tp_ref, own_ref, peer_ref, gain_ref, wv_ref, wg_ref, wq_ref, cw_ref, qg_ref, filt_ref, stat_ref, q_ref, xs_ref, taps_ref,
    own_n, peer_n
):
    tile = pl.program_id(0)
    me = tp_ref[0]
    own_at = pl.multiple_of(me * HALF_D, HALF_D)
    peer_at = pl.multiple_of((1 - me) * HALF_D, HALF_D)
    own_gain = wide_row(gain_ref.at[me])
    peer_gain = wide_row(gain_ref.at[1 - me])
    for r in range(0, TOK_TILE, NORM_ROWS):
        rows = slice(r, r + NORM_ROWS)
        own = own_ref[rows, :].astype(F32)
        peer = peer_ref[rows, :].astype(F32)
        total = jnp.sum(own * own + peer * peer, axis=1, keepdims=True)
        factor = lax.rsqrt(total * (1.0 / D) + NORM_EPS)
        own_n[rows, :] = (own * factor * own_gain).astype(BF16)
        peer_n[rows, :] = (peer * factor * peer_gain).astype(BF16)

    def product(w_ref):
        own_part = matmul(own_n[...], w_ref[pl.ds(own_at, HALF_D), :])
        return own_part + matmul(peer_n[...], w_ref[pl.ds(peer_at, HALF_D), :])

    q_ref[...] = head_norm(product(wq_ref), wide_row(qg_ref) * MEM_HD ** (-0.5)).astype(BF16)
    gated = (product(wv_ref) * jax.nn.sigmoid(product(wg_ref))).astype(BF16)

    @pl.when(tile % (SEQ_LEN // TOK_TILE) == 0)
    def _():
        xs_ref[:HISTORY, :] = jnp.zeros((HISTORY, C_DEV), F32)

    taps_ref[...] = cw_ref[...].astype(F32)
    xs_ref[HISTORY:, :] = gated.astype(F32)
    first = HISTORY - (KW - 1)
    for base in range(0, TOK_TILE, CONV_ROWS):
        sums = jnp.zeros((CONV_ROWS, LANES), F32)
        squares = jnp.zeros((CONV_ROWS, LANES), F32)
        for lane in range(0, C_DEV, LANES):
            lanes = slice(lane, lane + LANES)
            acc = None
            for r in range(8):
                steps = [s for s in range(first, first + KW) if s % 8 == r]
                reach = max(steps) - r + CONV_ROWS
                shifted = xs_ref[base + r : base + r + reach, lanes]
                part = None
                for s in steps:
                    term = shifted[s - r : s - r + CONV_ROWS] * taps_ref[s - first : s - first + 1, lanes]
                    part = term if part is None else part + term
                acc = part if acc is None else acc + part
            filt_ref[base : base + CONV_ROWS, lanes] = acc
            sums = sums + acc
            squares = squares + acc * acc
        stat_ref[base : base + CONV_ROWS, 0:1] = jnp.sum(sums, axis=1, keepdims=True)
        stat_ref[base : base + CONV_ROWS, 1:2] = jnp.sum(squares, axis=1, keepdims=True)
    xs_ref[:HISTORY, :] = xs_ref[TOK_TILE:, :]


def token_branch(me, own, peer, gain, wv, wg, wq, cw, qg):
    n = own.shape[0]
    tile = lambda width: pl.BlockSpec((TOK_TILE, width), lambda i, s: (i, 0))
    return pl.pallas_call(
        token_kernel,
        out_shape=(
            jax.ShapeDtypeStruct((n, C_DEV), F32),
            jax.ShapeDtypeStruct((n, 2), F32),
            jax.ShapeDtypeStruct((n, MEM_DEV), BF16),
        ),
        grid_spec=pltpu.PrefetchScalarGridSpec(
            num_scalar_prefetch=1,
            grid=(n // TOK_TILE,),
            in_specs=[
                tile(HALF_D),
                tile(HALF_D),
                resident((2, HALF_D // LANES, LANES)),
                resident((D, C_DEV)),
                resident((D, C_DEV)),
                resident((D, MEM_DEV)),
                resident((KW, C_DEV)),
                resident((MEM_DEV // LANES, LANES)),
            ],
            out_specs=(tile(C_DEV), tile(2), tile(MEM_DEV)),
            scratch_shapes=[
                pltpu.VMEM((HISTORY + TOK_TILE, C_DEV), F32),
                pltpu.VMEM((KW, C_DEV), F32),
                pltpu.VMEM((TOK_TILE, HALF_D), BF16),
                pltpu.VMEM((TOK_TILE, HALF_D), BF16),
            ],
        ),
        cost_estimate=pl.CostEstimate(flops=20 * n * D * 768, transcendentals=0, bytes_accessed=16 << 20),
        name="token_branch",
    )(me, own, peer, gain, wv, wg, wq, cw, qg)


def swish_kernel(filt_ref, own_ref, peer_ref, gain_ref, out_ref):
    stats = (own_ref[...] + peer_ref[...]) * (1.0 / C_A)
    mean = stats[:, 0:1]
    var = stats[:, 1:2] - mean * mean
    scaled = (filt_ref[...] - mean) * lax.rsqrt(var + LAYER_EPS) * wide_row(gain_ref)
    out_ref[...] = (scaled * jax.nn.sigmoid(scaled)).astype(BF16)


def channel_swish(half, filtered, own_stats, peer_stats, gain):
    n = filtered.shape[0] // 2
    steps = n // OUT_TILE
    tile = lambda width: pl.BlockSpec((OUT_TILE, width), lambda i, h: (h[0] * steps + i, 0))
    return pl.pallas_call(
        lambda half_ref, *refs: swish_kernel(*refs),
        out_shape=jax.ShapeDtypeStruct((n, C_DEV), BF16),
        grid_spec=pltpu.PrefetchScalarGridSpec(
            num_scalar_prefetch=1,
            grid=(steps,),
            in_specs=[tile(C_DEV), tile(2), tile(2), resident((C_DEV // LANES, LANES))],
            out_specs=pl.BlockSpec((OUT_TILE, C_DEV), lambda i, h: (i, 0)),
        ),
        cost_estimate=pl.CostEstimate(flops=n * D * 768, transcendentals=0, bytes_accessed=4 << 20),
        name="channel_swish",
    )(half, filtered, own_stats, peer_stats, gain)


def pair_kernel(own_ref, peer_ref, w_own_hbm, w_peer_hbm, out_ref, w_own_ref, w_peer_ref, sem):
    parts = D // OUT_COLS
    cols = lambda c: pl.ds(c * OUT_COLS, OUT_COLS)
    copies = [
        pltpu.make_async_copy(hbm.at[:, cols(c)], ref.at[:, cols(c)], sem.at[i, c])
        for c in range(parts)
        for i, (hbm, ref) in enumerate(((w_own_hbm, w_own_ref), (w_peer_hbm, w_peer_ref)))
    ]
    for c in copies:
        c.start()
    for c in range(parts):
        copies[2 * c].wait()
        copies[2 * c + 1].wait()
        own_part = matmul(own_ref[...], w_own_ref[:, cols(c)])
        out_ref[:, cols(c)] = (own_part + matmul(peer_ref[...], w_peer_ref[:, cols(c)])).astype(BF16)


def conv_product(own, peer, w_own, w_peer):
    n = own.shape[0]
    return pl.pallas_call(
        pair_kernel,
        out_shape=pltpu.HBM((n, D), BF16),
        in_specs=[ONCHIP, ONCHIP, HBM, HBM],
        out_specs=pl.BlockSpec((n, D), lambda: (0, 0)),
        scratch_shapes=[
            pltpu.VMEM((C_DEV, D), BF16),
            pltpu.VMEM((C_DEV, D), BF16),
            pltpu.SemaphoreType.DMA((2, D // OUT_COLS)),
        ],
        compiler_params=grant(16),
        cost_estimate=pl.CostEstimate(flops=4 * n * D * C_DEV, transcendentals=0, bytes_accessed=12 << 20),
        name="conv_product",
    )(*onchip(own, peer), *offchip(w_own, w_peer))


def attend_blocks(blocks, kv_ref, q_ref, base, gate):
    heads = MEM_DEV // MEM_HD
    lane_head = lax.broadcasted_iota(jnp.int32, (BLOCK, MEM_DEV), 1) // MEM_HD
    scores = []
    for b in blocks:
        q = q_ref[pl.ds(base + b * BLOCK, BLOCK), :]
        spread = jnp.concatenate([jnp.where(lane_head == h, q, jnp.zeros_like(q)) for h in range(heads)], axis=0)
        scores.append(matmul_t(spread, kv_ref[2 * b : 2 * b + 2, :, :MEM_DEV].reshape(2 * PLEN, MEM_DEV)))
    expanded = [jnp.exp(s - jnp.max(s, axis=1, keepdims=True)) for s in scores]
    weights = [(e * (1.0 / jnp.sum(e, axis=1, keepdims=True))).astype(BF16) for e in expanded]
    rows = []
    for w, b in zip(weights, blocks):
        mixed = matmul(w, kv_ref[2 * b : 2 * b + 2, :, MEM_DEV:].reshape(2 * PLEN, MEM_DEV))
        attended = mixed[:BLOCK]
        for h in range(1, heads):
            attended = jnp.where(lane_head == h, mixed[h * BLOCK : (h + 1) * BLOCK], attended)
        rows.append((attended * gate).astype(BF16))
    return jnp.concatenate(rows, axis=0)


def attend_all(out_ref, kv_ref, q_ref, base, gate, arrived):
    size = ATT_GROUP * BLOCK
    for g in range(out_ref.shape[0] // size):
        arrived(g)
        blocks = range(g * ATT_GROUP, (g + 1) * ATT_GROUP)
        out_ref[pl.ds(g * size, size), :] = attend_blocks(blocks, kv_ref, q_ref, base, gate)


def attend_kernel(
    owner_ref, recv_hbm, q_ref, gate_ref, out_ref, next_kv_ref, next_q_ref, kv_ref, sem, next_sem, q_sem
):
    count = kv_ref.shape[0]
    n = next_q_ref.shape[0]
    second = lax.axis_index("tp")
    first = 1 - second
    low, high = ([owner_ref[0, h * count + i] for i in range(count)] for h in range(2))
    owners = [jnp.where(first == 0, a, b) for a, b in zip(low, high)]
    others = [jnp.where(first == 0, b, a) for a, b in zip(low, high)]
    copies = [pltpu.make_async_copy(recv_hbm.at[owners[i]], kv_ref.at[i], sem.at[i]) for i in range(count)]
    later = [
        pltpu.make_async_copy(recv_hbm.at[others[i]], next_kv_ref.at[i], next_sem.at[i])
        for i in range(count)
    ] + [pltpu.make_async_copy(q_ref.at[pl.ds(pl.multiple_of(second * n, n), n), :], next_q_ref, q_sem)]
    for c in copies:
        c.start()
    gate = jnp.tanh(wide_row(gate_ref))

    def arrived(g):
        for c in copies[2 * g * ATT_GROUP : 2 * (g + 1) * ATT_GROUP]:
            c.wait()
        if g == 0:
            for c in later:
                c.start()

    attend_all(out_ref, kv_ref, q_ref, pl.multiple_of(first * n, n), gate, arrived)
    for c in later:
        c.wait()


def attend_first(owners, received, queries, gate):
    n = queries.shape[0] // 2
    count = owners.shape[1] // 2
    return pl.pallas_call(
        attend_kernel,
        out_shape=(
            pltpu.VMEM((n, MEM_DEV), BF16),
            pltpu.VMEM((count, PLEN, 2 * MEM_DEV), BF16),
            pltpu.VMEM((n, MEM_DEV), BF16),
        ),
        in_specs=[ONCHIP, HBM, ONCHIP, ONCHIP],
        out_specs=(ONCHIP, ONCHIP, ONCHIP),
        scratch_shapes=[
            pltpu.VMEM((count, PLEN, 2 * MEM_DEV), BF16),
            pltpu.SemaphoreType.DMA((count,)),
            pltpu.SemaphoreType.DMA((count,)),
            pltpu.SemaphoreType.DMA(()),
        ],
        compiler_params=grant(8),
        cost_estimate=pl.CostEstimate(flops=n * D * 256, transcendentals=0, bytes_accessed=2 << 20),
        name="attend_first",
    )(*onchip(owners), *offchip(received), *onchip(queries, gate))


def attend_rest_kernel(kv_ref, q_ref, gate_ref, out_ref):
    attend_all(out_ref, kv_ref, q_ref, 0, jnp.tanh(wide_row(gate_ref)), lambda g: None)


def attend_rest(kv, queries, gate):
    n = queries.shape[0]
    return pl.pallas_call(
        attend_rest_kernel,
        out_shape=pltpu.VMEM((n, MEM_DEV), BF16),
        in_specs=[ONCHIP] * 3,
        out_specs=ONCHIP,
        compiler_params=grant(6),
        cost_estimate=pl.CostEstimate(flops=n * D * 256, transcendentals=0, bytes_accessed=2 << 20),
        name="attend_rest",
    )(*onchip(kv, queries, gate))


def finish_kernel(own_ref, peer_ref, w_own_ref, w_peer_ref, conv_ref, out_hbm, out_ref, out_sem):
    groups = out_ref.shape[0] // ATT_TILE
    span = lambda g: pl.ds(g * ATT_TILE, ATT_TILE)
    out_copies = [pltpu.make_async_copy(out_ref.at[span(g)], out_hbm.at[span(g)], out_sem.at[g]) for g in range(groups)]
    for g in range(groups):
        memory = matmul(own_ref[span(g), :], w_own_ref[...]) + matmul(peer_ref[span(g), :], w_peer_ref[...])
        out_ref[span(g), :] = (conv_ref[span(g), :].astype(F32) + memory).astype(BF16)
        out_copies[g].start()
    for c in out_copies:
        c.wait()


def finish(own, peer, w_own, w_peer, conv_sum):
    n = conv_sum.shape[0]
    return pl.pallas_call(
        finish_kernel,
        out_shape=pltpu.HBM((n, D), BF16),
        in_specs=[ONCHIP] * 5,
        out_specs=HBM,
        scratch_shapes=[pltpu.VMEM((n, D), BF16), pltpu.SemaphoreType.DMA((n // ATT_TILE,))],
        compiler_params=grant(12),
        cost_estimate=pl.CostEstimate(flops=4 * n * D * MEM_DEV, transcendentals=0, bytes_accessed=8 << 20),
        name="finish",
    )(*onchip(own, peer, w_own, w_peer, conv_sum))


def body(
    tokens,
    passage_ids,
    passage_store,
    norm_gain,
    conv_value_weight,
    conv_gate_weight,
    conv_weight,
    ln_gain,
    query_weight,
    query_gain,
    passage_gain,
    key_weight,
    value_weight,
    key_gain,
    memory_gate,
    conv_out_weight,
    memory_out_weight,
):
    owner_count = lax.axis_size("st")
    swap = [(0, 1), (1, 0)]
    me = lax.axis_index("tp").astype(jnp.int32).reshape(1)

    ids = lax.all_to_all(jnp.broadcast_to(passage_ids.T, (owner_count, *passage_ids.shape[::-1])), "st", 0, 0, tiled=True)
    peer_tokens = lax.ppermute(tokens, "tp", swap)
    peer_conv_weight = lax.ppermute(conv_out_weight, "tp", swap)
    peer_memory_weight = lax.ppermute(memory_out_weight, "tp", swap)

    kv = project_store(
        passage_store.reshape(-1, D),
        passage_gain.reshape(-1, LANES),
        key_weight,
        value_weight,
        key_gain.reshape(-1, LANES),
    ).reshape(PASS_DEV, PLEN, 2 * MEM_DEV)
    sent = fill_slots(ids, kv)
    received = lax.all_to_all(sent, "st", 0, 0, tiled=True)

    filtered, own_stats, queries = token_branch(
        me,
        tokens,
        peer_tokens,
        norm_gain.reshape(2, -1, LANES),
        conv_value_weight,
        conv_gate_weight,
        query_weight,
        conv_weight,
        query_gain.reshape(-1, LANES),
    )
    peer_stats = lax.ppermute(own_stats, "tp", swap)
    conv_theirs = channel_swish(1 - me, filtered, own_stats, peer_stats, ln_gain.reshape(-1, LANES))
    conv_peer = lax.ppermute(conv_theirs, "tp", swap)
    conv_mine = channel_swish(me, filtered, own_stats, peer_stats, ln_gain.reshape(-1, LANES))
    conv_sum = conv_product(conv_mine, conv_peer, conv_out_weight, peer_conv_weight)

    owners = lax.optimization_barrier((passage_ids, filtered))[0].reshape(1, -1) >> OWNER_SHIFT
    gate = memory_gate.reshape(-1, LANES)
    memory_theirs, next_kv, next_queries = attend_first(owners, received, queries, gate)
    memory_peer = lax.ppermute(memory_theirs, "tp", swap)
    memory_mine = attend_rest(next_kv, next_queries, gate)
    return finish(memory_mine, memory_peer, memory_out_weight, peer_memory_weight, conv_sum)


def solution(mesh):
    return jax.shard_map(
        body,
        mesh=mesh,
        in_specs=(
            P("st", "tp"),
            P("st", None),
            P("st", None, None),
            P(),
            P(None, "tp"),
            P(None, "tp"),
            P(None, "tp"),
            P("tp"),
            P(None, "tp"),
            P("tp"),
            P(),
            P(None, "tp"),
            P(None, "tp"),
            P("tp"),
            P("tp"),
            P("tp", None),
            P("tp", None),
        ),
        out_specs=P(("st", "tp"), None),
        check_vma=False,
    )
```
